512 devices in a mesh: sp: 128 (over z, y, core), tp: 4 (over x).
Axes of the slice: x: 4, y: 8, z: 8, core: 2. Of those that a mesh axis runs over, the one named last changes fastest.
Arguments:
- tokens: bfloat16 [65536, 2048], P('sp'), may hold values from -6 to 6
- norm_gain: bfloat16 [2048], replicated, may hold values from 0.099609375 to 1.8984375
- w_conv_value: bfloat16 [2048, 2048], P('sp', 'tp'), may hold values from -0.125 to 0.125
- w_conv_gate: bfloat16 [2048, 2048], P('sp', 'tp'), may hold values from -0.125 to 0.125
- w_query: bfloat16 [2048, 2048], P('sp', 'tp'), may hold values from -0.125 to 0.125
- w_key: bfloat16 [2048, 512], P('sp', 'tp'), may hold values from -0.125 to 0.125
- w_value: bfloat16 [2048, 512], P('sp', 'tp'), may hold values from -0.125 to 0.125
- conv_taps: float32 [31, 2048], P(None, 'tp'), as said below
- ln_gain: float32 [2048], P('tp'), may hold values from 0.1 to 1.9
- sinks: float32 [32], P('tp'), may hold values from 3 to 6
- out_conv: bfloat16 [2048, 2048], P('tp', 'sp'), may hold values from -0.125 to 0.125
- out_attn: bfloat16 [2048, 2048], P('tp', 'sp'), may hold values from -0.5 to 0.5
Outputs:
- mixed: bfloat16 [65536, 2048], P(('sp', 'tp'))
- log_sums: float32 [32, 65536], P('tp', 'sp')
The draws below stay inside these ranges and needn't reach their ends.
Inputs may be any that keep to these rules, and one draw needn't show every extreme that they name: `conv_taps`: each tap lies within 30 / sqrt(31) in magnitude.
All inputs are finite; a program needn't handle non-finite values.
Results may differ from the reference program's by a relative error of at most 0.017.
Values may be sent and summed in bfloat16 or wider, within the bound.
No kernel may reach another device: no remote copies, remote signals or barrier semaphores. Data moves between devices by JAX's collectives and lax.ppermute only.
A program may use at most 64 MiB of HBM per device.

```python
import jax
import jax.numpy as jnp
from jax import lax

D = 2048
CONV_CH = 2048
HEADS = 32
KV_HEADS = 8
HEAD_DIM = 64
CONV_K = 31
WINDOW = 128
TOKENS = 65536
SPLITS = 4


def draw_conv_taps(key, part):
    channel = jnp.arange(CONV_CH, dtype=jnp.float32)
    samples = jax.random.truncated_normal(key, -3.0, 3.0, (CONV_K, CONV_CH), jnp.float32)
    scales = 10.0 ** (channel / CONV_CH)
    return samples * scales[None, :] * CONV_K ** (-0.5)


def steps_of(own_key, extent, split, low, top_value):
    def one(position, shards_of):
        steps = jax.random.uniform(jax.random.fold_in(jax.random.fold_in(own_key, 6), position), (shards_of,), jnp.float32, low / len(split), top_value / len(split))
        return jnp.repeat(jnp.exp(steps), extent[position] // shards_of).reshape((-1,) + (1,) * (len(extent) - position - 1))

    gain = one(*split[0])
    for cut in split[1:]:
        gain = gain * one(*cut)
    return gain


def noise(rng, shape, spread, most, pieces=(), held_as=jnp.bfloat16):
    array = spread * jax.random.normal(rng, shape, jnp.float32)
    if pieces:
        array = array * steps_of(rng, shape, pieces, -0.22, 0.18)
    return jnp.clip(array, -most, most).astype(held_as)


def setup_inputs(seed: int = 0) -> dict:
    arg_keys = jax.random.split(jax.random.key(seed), 13)
    tokens = noise(arg_keys[0], (TOKENS, D), 1.0, 6.0, ((0, 128),))
    norm_gain = jnp.clip(1.0 + 0.18 * jax.random.normal(arg_keys[1], (D,), jnp.float32), 0.099609375, 1.8984375).astype(jnp.bfloat16)
    w_conv_value = noise(arg_keys[2], (D, CONV_CH), D ** -0.5, 0.125, ((0, 128), (1, 4)))
    w_conv_gate = noise(arg_keys[3], (D, CONV_CH), D ** -0.5, 0.125, ((0, 128), (1, 4)))
    w_query = noise(arg_keys[4], (D, HEADS * HEAD_DIM), D ** -0.5, 0.125, ((0, 128), (1, 4)))
    w_key = noise(arg_keys[5], (D, KV_HEADS * HEAD_DIM), D ** -0.5, 0.125, ((0, 128), (1, 4)))
    w_value = noise(arg_keys[6], (D, KV_HEADS * HEAD_DIM), D ** -0.5, 0.125, ((0, 128), (1, 4)))
    conv_taps = draw_conv_taps(jax.random.fold_in(arg_keys[12], 71), 0)
    ln_gain = jnp.clip(1.0 + 0.18 * jax.random.normal(arg_keys[8], (CONV_CH,), jnp.float32), 0.1, 1.9)
    sinks = jnp.clip(3.0 + 3.0 * jax.random.uniform(arg_keys[9], (HEADS,), jnp.float32) ** steps_of(arg_keys[9], (HEADS,), ((0, 4),), -0.2, 0.2), 3.0, 6.0)
    out_conv = noise(arg_keys[10], (CONV_CH, D), CONV_CH ** -0.5, 0.125, ((0, 4), (1, 128)))
    out_attn = noise(arg_keys[11], (HEADS * HEAD_DIM, D), (HEADS * HEAD_DIM // 16) ** -0.5, 0.5, ((0, 4), (1, 128)))
    return dict(tokens=tokens, norm_gain=norm_gain, w_conv_value=w_conv_value, w_conv_gate=w_conv_gate, w_query=w_query, w_key=w_key, w_value=w_value, conv_taps=conv_taps, ln_gain=ln_gain, sinks=sinks, out_conv=out_conv, out_attn=out_attn)


NORM_EPS = 1e-06
CHANNEL_EPS = 1e-05
ROPE_BASE = 10000.0

def rotate(heads, positions):
    half_dim = heads.shape[-1] // 2
    inverse = ROPE_BASE ** (-jnp.arange(half_dim, dtype=jnp.float32) / half_dim)
    angles = positions.astype(jnp.float32)[:, None] * inverse[None, :]
    cosine = jnp.cos(angles)[:, None, :]
    sine = jnp.sin(angles)[:, None, :]
    as_float = heads.astype(jnp.float32)
    front_part = as_float[..., :half_dim]
    back_part = as_float[..., half_dim:]
    return jnp.concatenate([front_part * cosine - back_part * sine, back_part * cosine + front_part * sine], axis=-1)

def reference(tokens, norm_gain, w_conv_value, w_conv_gate, w_query, w_key, w_value, conv_taps, ln_gain, sinks, out_conv, out_attn):
    as_float = tokens.astype(jnp.float32)
    normed = (as_float * lax.rsqrt(lax.optimization_barrier(jnp.mean(as_float * as_float, axis=-1, keepdims=True)) + NORM_EPS) * norm_gain.astype(jnp.float32)).astype(jnp.bfloat16)

    def project(weight):
        return jnp.dot(normed, weight, preferred_element_type=jnp.float32).astype(jnp.bfloat16)
    conv_value = project(w_conv_value)
    conv_gate = project(w_conv_gate)
    query_raw = project(w_query)
    key_raw = project(w_key)
    value_rows = project(w_value)
    glu = (conv_value.astype(jnp.float32) * jax.nn.sigmoid(conv_gate.astype(jnp.float32))).astype(jnp.bfloat16)
    padded = jnp.concatenate([jnp.zeros((CONV_K - 1, CONV_CH), jnp.float32), glu.astype(jnp.float32)], axis=0)
    conv_out = jnp.zeros((TOKENS, CONV_CH), jnp.float32)
    for tap in range(CONV_K):
        conv_out = conv_out + conv_taps[tap].astype(jnp.float32)[None, :] * padded[tap:tap + TOKENS]
    mean = lax.optimization_barrier(jnp.mean(conv_out, axis=-1, keepdims=True))
    var = lax.optimization_barrier(jnp.mean(conv_out * conv_out, axis=-1, keepdims=True)) - mean * mean
    conv_branch = jax.nn.silu((conv_out - mean) * lax.rsqrt(var + CHANNEL_EPS) * ln_gain.astype(jnp.float32)[None, :]).astype(jnp.bfloat16)
    positions = jnp.arange(TOKENS, dtype=jnp.int32)
    query = rotate(query_raw.reshape(TOKENS, HEADS, HEAD_DIM), positions).astype(jnp.bfloat16)
    key = rotate(key_raw.reshape(TOKENS, KV_HEADS, HEAD_DIM), positions).astype(jnp.bfloat16)
    values = value_rows.reshape(TOKENS, KV_HEADS, HEAD_DIM)
    group = HEADS // KV_HEADS
    blocks = TOKENS // WINDOW
    q_blocks = query.reshape(blocks, WINDOW, KV_HEADS, group, HEAD_DIM).astype(jnp.float32)
    leading = jnp.zeros((WINDOW, KV_HEADS, HEAD_DIM), jnp.bfloat16)
    key_blocks = jnp.concatenate([leading, key], axis=0).reshape(blocks + 1, WINDOW, KV_HEADS, HEAD_DIM)
    value_blocks = jnp.concatenate([leading, values], axis=0).reshape(blocks + 1, WINDOW, KV_HEADS, HEAD_DIM)
    key_window = jnp.concatenate([key_blocks[:-1], key_blocks[1:]], axis=1).astype(jnp.float32)
    value_window = jnp.concatenate([value_blocks[:-1], value_blocks[1:]], axis=1).astype(jnp.float32)
    scores = jnp.einsum('nqhgd,nkhd->nhgqk', q_blocks, key_window) * HEAD_DIM ** (-0.5)
    query_index = jnp.arange(WINDOW)[:, None] + WINDOW
    key_index = jnp.arange(2 * WINDOW)[None, :]
    band = (key_index <= query_index) & (query_index - key_index < WINDOW)
    block_index = jnp.arange(blocks)[:, None, None]
    allowed = band[None] & (block_index * WINDOW + key_index[None] - WINDOW >= 0)
    allowed = allowed[:, None, None]
    totals = lax.optimization_barrier(jnp.sum(jnp.where(allowed, jnp.exp(scores), 0.0), axis=-1))
    totals = totals + jnp.exp(sinks.astype(jnp.float32)).reshape(1, KV_HEADS, group, 1)
    log_total = jnp.log(totals)
    weights = jnp.where(allowed, jnp.exp(scores - log_total[..., None]), 0.0).astype(jnp.bfloat16)
    attended = jnp.einsum('nhgqk,nkhd->nqhgd', weights.astype(jnp.float32), value_window)
    attn_branch = attended.astype(jnp.bfloat16).reshape(TOKENS, HEADS * HEAD_DIM)
    log_sums = log_total.transpose(1, 2, 0, 3).reshape(HEADS, TOKENS)
    conv_width = CONV_CH // SPLITS
    attn_width = HEADS * HEAD_DIM // SPLITS
    mixed = jnp.zeros((TOKENS, D), jnp.float32)
    for index in range(SPLITS):
        part_sum = jnp.dot(conv_branch[:, index * conv_width:(index + 1) * conv_width], out_conv[index * conv_width:(index + 1) * conv_width], preferred_element_type=jnp.float32)
        part_sum = part_sum + jnp.dot(attn_branch[:, index * attn_width:(index + 1) * attn_width], out_attn[index * attn_width:(index + 1) * attn_width], preferred_element_type=jnp.float32)
        rounded = lax.optimization_barrier(part_sum.astype(jnp.bfloat16))
        mixed = mixed + rounded.astype(jnp.float32)
    return (mixed.astype(jnp.bfloat16), log_sums)
```

```python
import jax
import jax.numpy as jnp
from jax import lax
from jax.sharding import Mesh, PartitionSpec as P

CONV_CH = 2048
HEAD_DIM = 64
WINDOW = 128

NORM_EPS = 1e-06
CHANNEL_EPS = 1e-05
ROPE_BASE = 10000.0

SIDE = 8
PAIRS = SIDE // 2
CORES = 2
SP = ("chip", "core")
CHIP = ("core", "tp")


def place(z, y, core):
    return ((z % SIDE) * SIDE + y % SIDE) * CORES + core


FAR_BOTH = [
    [place(2 * i + a, 2 * j + b, c) for i in range(PAIRS) for j in range(PAIRS) for c in range(CORES)]
    for a in range(2)
    for b in range(2)
]
FAR_ONE = [
    [place(2 * i + a, 2 * j + b, c) for i in range(PAIRS) for j in range(PAIRS)]
    for a in range(2)
    for b in range(2)
    for c in range(CORES)
]
NEAR = [
    [
        place(2 * i + a if a or not c else 2 * i + 2, 2 * j + b if b or not c else 2 * j + 2, c)
        for a in range(2)
        for b in range(2)
    ]
    for c in range(CORES)
    for i in range(PAIRS)
    for j in range(PAIRS)
]
OTHER_CORE = [(i, i ^ 1) for i in range(SIDE * SIDE * CORES)]
NEXT_CHIP = [(i, i + CORES) for i in range(SIDE * SIDE * CORES - CORES)]


def exchanged(pieces, groups):
    return lax.all_to_all(pieces, SP, 0, 0, tiled=True, axis_index_groups=groups)


def repeated(shard, count):
    return jnp.broadcast_to(shard[None], (count, *shard.shape))


def rotate(heads, positions):
    half_dim = heads.shape[-1] // 2
    inverse = ROPE_BASE ** (-jnp.arange(half_dim, dtype=jnp.float32) / half_dim)
    angles = positions.astype(jnp.float32)[:, None] * inverse[None, :]
    cosine = jnp.cos(angles)[:, None, :]
    sine = jnp.sin(angles)[:, None, :]
    as_float = heads.astype(jnp.float32)
    front_part = as_float[..., :half_dim]
    back_part = as_float[..., half_dim:]
    return jnp.concatenate(
        [front_part * cosine - back_part * sine, back_part * cosine + front_part * sine], axis=-1
    )


def shards(
    tokens,
    norm_gain,
    w_conv_value,
    w_conv_gate,
    w_query,
    w_key,
    w_value,
    conv_taps,
    ln_gain,
    sinks,
    out_conv,
    out_attn,
):
    core = lax.axis_index("core")
    chip = lax.axis_index("chip")
    own_rows = tokens.shape[0]
    row_count = own_rows * CORES

    tokens_other = lax.ppermute(tokens, SP, OTHER_CORE)

    halves = jnp.stack(
        [
            jnp.concatenate(
                [
                    w[:, h * (w.shape[1] // CORES) : (h + 1) * (w.shape[1] // CORES)]
                    for w in (w_conv_value, w_conv_gate, w_query, w_key, w_value)
                ],
                axis=1,
            )
            for h in range(CORES)
        ]
    )
    depth, width = halves.shape[1:]
    sent = jnp.broadcast_to(halves[None], (PAIRS * PAIRS, *halves.shape)).reshape(-1, depth, width)
    far = exchanged(sent, FAR_BOTH)
    near = exchanged(repeated(far, 4).reshape(-1, *far.shape[1:]), NEAR)
    turned = jnp.concatenate([out_conv.T, out_attn.T], axis=1)
    turned, near = lax.optimization_barrier((turned, near))
    out_depth, out_width = turned.shape
    weights_in = (
        near.reshape(2, 2, PAIRS, PAIRS, CORES * depth, width)
        .transpose(2, 0, 3, 1, 4, 5)
        .reshape(-1, width)
    )
    out_far = exchanged(repeated(turned, PAIRS * PAIRS).reshape(-1, out_width), FAR_ONE)
    out_near = exchanged(repeated(out_far, 4).reshape(-1, out_width), NEAR)
    out_other = lax.ppermute(out_near, SP, OTHER_CORE)

    both = jnp.where(
        core == 0,
        jnp.concatenate([tokens, tokens_other], axis=0),
        jnp.concatenate([tokens_other, tokens], axis=0),
    )
    as_float = both.astype(jnp.float32)
    normed = (
        as_float
        * lax.rsqrt(jnp.mean(as_float * as_float, axis=-1, keepdims=True) + NORM_EPS)
        * norm_gain.astype(jnp.float32)
    ).astype(jnp.bfloat16)

    projected = jnp.dot(normed, weights_in, preferred_element_type=jnp.float32).astype(jnp.bfloat16)
    channels = w_conv_value.shape[1] // CORES
    q_cols = w_query.shape[1] // CORES
    conv_value = projected[:, :channels]
    conv_gate = projected[:, channels : 2 * channels]
    query_raw = projected[:, 2 * channels : 2 * channels + q_cols]
    key_raw = projected[:, 2 * channels + q_cols : 2 * channels + q_cols + HEAD_DIM]
    value_rows = projected[:, 2 * channels + q_cols + HEAD_DIM :]
    glu = (conv_value.astype(jnp.float32) * jax.nn.sigmoid(conv_gate.astype(jnp.float32))).astype(
        jnp.bfloat16
    )
    offset = chip * row_count
    positions = offset + jnp.arange(row_count, dtype=jnp.int32)
    query_heads = q_cols // HEAD_DIM
    query = rotate(query_raw.reshape(row_count, query_heads, HEAD_DIM), positions).astype(
        jnp.bfloat16
    )
    key = rotate(key_raw.reshape(row_count, 1, HEAD_DIM), positions).astype(jnp.bfloat16)[:, 0]

    reach = conv_taps.shape[0] - 1
    tail_rows = 32
    tail = glu[row_count - tail_rows :]
    packed = jnp.concatenate(
        [
            jnp.concatenate([key[row_count - WINDOW :], value_rows[row_count - WINDOW :]], axis=1),
            tail[:, : channels // 2],
            tail[:, channels // 2 :],
        ],
        axis=0,
    )
    before = lax.ppermute(packed, SP, NEXT_CHIP)
    key_before = before[:WINDOW, :HEAD_DIM]
    value_before = before[:WINDOW, HEAD_DIM:]
    glu_before = jnp.concatenate(
        [before[WINDOW : WINDOW + tail_rows], before[WINDOW + tail_rows :]], axis=1
    )[tail_rows - reach :]

    extended = jnp.concatenate([glu_before, glu], axis=0).astype(jnp.float32)
    taps = lax.dynamic_slice_in_dim(conv_taps, core * channels, channels, 1)
    conv_out = jnp.zeros((row_count, channels), jnp.float32)
    for tap in range(reach + 1):
        conv_out = conv_out + taps[tap][None, :] * extended[tap : tap + row_count]
    sums = jnp.stack([jnp.sum(conv_out, axis=-1), jnp.sum(conv_out * conv_out, axis=-1)])
    members = CORES * lax.axis_size("tp")
    totals = jnp.sum(
        lax.all_to_all(repeated(sums, members), CHIP, 0, 0, tiled=True), axis=0
    )
    mean = (totals[0] / CONV_CH)[:, None]
    var = (totals[1] / CONV_CH)[:, None] - mean * mean
    gain = lax.dynamic_slice_in_dim(ln_gain, core * channels, channels, 0)
    conv_branch = jax.nn.silu(
        (conv_out - mean) * lax.rsqrt(var + CHANNEL_EPS) * gain[None, :]
    ).astype(jnp.bfloat16)

    blocks = row_count // WINDOW
    q_blocks = query.reshape(blocks, WINDOW, query_heads, HEAD_DIM)
    key_blocks = jnp.concatenate([key_before, key], axis=0).reshape(blocks + 1, WINDOW, HEAD_DIM)
    value_blocks = jnp.concatenate([value_before, value_rows], axis=0).reshape(
        blocks + 1, WINDOW, HEAD_DIM
    )
    key_window = jnp.concatenate([key_blocks[:-1], key_blocks[1:]], axis=1)
    value_window = jnp.concatenate([value_blocks[:-1], value_blocks[1:]], axis=1)
    scores = jnp.einsum(
        "nqgd,nkd->ngqk", q_blocks, key_window, preferred_element_type=jnp.float32
    ) * HEAD_DIM ** (-0.5)
    query_index = jnp.arange(WINDOW)[:, None] + WINDOW
    key_index = jnp.arange(2 * WINDOW)[None, :]
    band = (key_index <= query_index) & (query_index - key_index < WINDOW)
    block_index = jnp.arange(blocks)[:, None, None]
    allowed = band[None] & (offset + block_index * WINDOW + key_index[None] - WINDOW >= 0)
    allowed = allowed[:, None]
    sums_exp = jnp.sum(jnp.where(allowed, jnp.exp(scores), 0.0), axis=-1)
    own_sinks = lax.dynamic_slice_in_dim(sinks, core * query_heads, query_heads, 0)
    log_total = jnp.log(sums_exp + jnp.exp(own_sinks)[None, :, None])
    weights = jnp.where(allowed, jnp.exp(scores - log_total[..., None]), 0.0).astype(jnp.bfloat16)
    attended = jnp.einsum(
        "ngqk,nkd->nqgd", weights, value_window, preferred_element_type=jnp.float32
    )
    attn_branch = attended.astype(jnp.bfloat16).reshape(row_count, q_cols)
    log_rows = log_total.transpose(1, 0, 2).reshape(query_heads, row_count)

    def swapped(value, axis):
        kept = lax.dynamic_slice_in_dim(value, core * own_rows, own_rows, axis)
        given = lax.dynamic_slice_in_dim(value, (1 - core) * own_rows, own_rows, axis)
        return kept, lax.ppermute(given, SP, OTHER_CORE)

    def joined(kept, got, axis):
        return jnp.where(
            core == 0,
            jnp.concatenate([kept, got], axis=axis),
            jnp.concatenate([got, kept], axis=axis),
        )

    log_sums = joined(*swapped(log_rows, 1), 0)
    attn_full = joined(*swapped(attn_branch, 0), 1)
    conv_full = joined(*swapped(conv_branch, 0), 1)

    split = (2, 2, PAIRS, PAIRS, out_depth, out_width)
    weights_out = joined(
        out_near.reshape(*split)[..., None, :, :], out_other.reshape(*split)[..., None, :, :], 4
    )
    weights_out = weights_out.transpose(2, 0, 3, 1, 4, 5, 6).reshape(-1, out_width)
    partial = (
        lax.dot_general(
            conv_full,
            weights_out[:, : out_width // 2],
            (((1,), (1,)), ((), ())),
            preferred_element_type=jnp.float32,
        )
        + lax.dot_general(
            attn_full,
            weights_out[:, out_width // 2 :],
            (((1,), (1,)), ((), ())),
            preferred_element_type=jnp.float32,
        )
    ).astype(jnp.bfloat16)
    peers = lax.axis_size("tp")
    arrived = lax.all_to_all(
        partial.reshape(peers, own_rows // peers, -1), "tp", split_axis=0, concat_axis=0, tiled=True
    )
    mixed = arrived.astype(jnp.float32).sum(axis=0)
    return (mixed.astype(jnp.bfloat16), log_sums)


def solution(mesh):
    split = Mesh(mesh.devices.reshape(-1, CORES, mesh.shape["tp"]), ("chip", "core", "tp"))
    in_specs = (
        P(SP, None),
        P(),
        P(SP, "tp"),
        P(SP, "tp"),
        P(SP, "tp"),
        P(SP, "tp"),
        P(SP, "tp"),
        P(None, "tp"),
        P("tp"),
        P("tp"),
        P("tp", SP),
        P("tp", SP),
    )
    out_specs = (P((*SP, "tp"), None), P("tp", SP))
    return jax.shard_map(shards, mesh=split, in_specs=in_specs, out_specs=out_specs, check_vma=False)
```

```python
import jax
import jax.numpy as jnp
from jax import lax
from jax.experimental import pallas as pl
from jax.experimental.pallas import tpu as pltpu
from jax.sharding import Mesh, PartitionSpec as P

CONV_CH = 2048
HEAD_DIM = 64
WINDOW = 128

NORM_EPS = 1e-06
CHANNEL_EPS = 1e-05
ROPE_BASE = 10000.0

SIDE = 8
PAIRS = SIDE // 2
CORES = 2
SP = ("chip", "core")
CHIP = ("core", "tp")


def place(z, y, core):
    return ((z % SIDE) * SIDE + y % SIDE) * CORES + core


FAR_BOTH = [
    [place(2 * i + a, 2 * j + b, c) for i in range(PAIRS) for j in range(PAIRS) for c in range(CORES)]
    for a in range(2)
    for b in range(2)
]
FAR_ONE = [
    [place(2 * i + a, 2 * j + b, c) for i in range(PAIRS) for j in range(PAIRS)]
    for a in range(2)
    for b in range(2)
    for c in range(CORES)
]


def beside(at, core):
    return ((at + core) ^ 1) - core


NEAR = [
    [
        (place(z, y, c), place(beside(z, c) if along_z else z, beside(y, c) if along_y else y, c))
        for z in range(SIDE)
        for y in range(SIDE)
        for c in range(CORES)
    ]
    for along_z, along_y in ((0, 1), (1, 0), (1, 1))
]
OTHER_CORE = [(i, i ^ 1) for i in range(SIDE * SIDE * CORES)]
NEXT_CHIP = [(i, i + CORES) for i in range(SIDE * SIDE * CORES - CORES)]


def exchanged(pieces, groups):
    return lax.all_to_all(pieces, SP, 0, 0, tiled=True, axis_index_groups=groups)


def repeated(shard, count):
    return jnp.broadcast_to(shard[None], (count, *shard.shape))


VMEM = pl.BlockSpec(memory_space=pltpu.VMEM)
SMEM = pl.BlockSpec(memory_space=pltpu.SMEM)
TILE = 256


def call(body, outs, scratch, flops, *operands):
    return pl.pallas_call(
        body,
        out_shape=outs,
        in_specs=[SMEM] + [VMEM] * (len(operands) - 1),
        out_specs=jax.tree.map(lambda _: VMEM, outs),
        scratch_shapes=scratch,
        compiler_params=pltpu.CompilerParams(vmem_limit_bytes=12 << 20),
        cost_estimate=pl.CostEstimate(flops=flops, bytes_accessed=1 << 20, transcendentals=0),
    )(*operands)


def put_in_order(at_ref, pieces, out_ref, rows):
    for piece, (flip_z, flip_y) in zip(pieces, ((0, 0), (0, 1), (1, 0), (1, 1))):
        odd_z = jnp.bitwise_xor(at_ref[0], flip_z)
        odd_y = jnp.bitwise_xor(at_ref[1], flip_y)
        first = (odd_z * SIDE + odd_y) * rows
        for i in range(PAIRS):
            for j in range(PAIRS):
                to = pl.multiple_of(first + (2 * i * SIDE + 2 * j) * rows, rows)
                out_ref[pl.ds(to, rows), :] = piece[pl.ds((i * PAIRS + j) * rows, rows), :]


def gated_kernel(at_ref, x_ref, a_ref, b_ref, c_ref, d_ref, out_ref, w_ref):
    put_in_order(at_ref, (a_ref, b_ref, c_ref, d_ref), w_ref, a_ref.shape[0] // PAIRS**2)
    half = out_ref.shape[1]

    @pl.loop(0, x_ref.shape[0] // TILE)
    def _(step):
        rows = pl.ds(pl.multiple_of(step * TILE, TILE), TILE)
        both = jnp.dot(x_ref[rows, :], w_ref[...], preferred_element_type=jnp.float32)
        both = both.astype(jnp.bfloat16).astype(jnp.float32)
        out_ref[rows, :] = (both[:, :half] * jax.nn.sigmoid(both[:, half:])).astype(jnp.bfloat16)


def rotated_kernel(at_ref, x_ref, cos_ref, sin_ref, a_ref, b_ref, c_ref, d_ref, out_ref, w_ref):
    put_in_order(at_ref, (a_ref, b_ref, c_ref, d_ref), w_ref, a_ref.shape[0] // PAIRS**2)
    width = out_ref.shape[1]

    @pl.loop(0, x_ref.shape[0] // TILE)
    def _(step):
        rows = pl.ds(pl.multiple_of(step * TILE, TILE), TILE)
        raw = jnp.dot(x_ref[rows, :], w_ref[...], preferred_element_type=jnp.float32)
        raw = raw.astype(jnp.bfloat16).astype(jnp.float32)
        lane = lax.broadcasted_iota(jnp.int32, (TILE, 128), 1)
        front = jnp.bitwise_and(lane, HEAD_DIM - 1) < HEAD_DIM // 2
        cosine, sine = cos_ref[rows, :], sin_ref[rows, :]
        for at in range(0, width, 128):
            part = raw[:, at : at + 128]
            other = jnp.where(
                front,
                pltpu.roll(part, 128 - HEAD_DIM // 2, 1),
                pltpu.roll(part, HEAD_DIM // 2, 1),
            )
            turned = part * cosine + other * sine
            if at + 128 == width:
                turned = jnp.where(lane < HEAD_DIM, turned, part)
            out_ref[rows, at : at + 128] = turned.astype(jnp.bfloat16)


def conv_kernel(at_ref, before_ref, glu_ref, taps_ref, out_ref, sums_ref, ext_ref):
    count, rows = taps_ref.shape[0], glu_ref.shape[0]
    lead = before_ref.shape[0]
    for part in range(2):
        lanes = pl.ds(part * 128, 128)
        ext_ref[part, pl.ds(0, lead), :] = before_ref[:, lanes].astype(jnp.float32)
        ext_ref[part, pl.ds(lead, rows), :] = glu_ref[:, lanes].astype(jnp.float32)

    @pl.loop(0, rows // 128)
    def _(step):
        base = pl.multiple_of(step * 128, 128)
        first = jnp.zeros((128, 128), jnp.float32)
        second = jnp.zeros((128, 128), jnp.float32)
        for part in range(2):
            lanes = pl.ds(part * 128, 128)
            total = jnp.zeros((128, 128), jnp.float32)
            for tap in range(count):
                rows_at = pl.ds(base + (lead - count + 1 + tap), 128)
                total = total + taps_ref[pl.ds(tap, 1), lanes] * ext_ref[part, rows_at, :]
            out_ref[pl.ds(base, 128), lanes] = total
            first = first + total
            second = second + total * total
        sums_ref[pl.ds(0, 1), pl.ds(base, 128)] = jnp.sum(first.T, axis=0, keepdims=True)
        sums_ref[pl.ds(1, 1), pl.ds(base, 128)] = jnp.sum(second.T, axis=0, keepdims=True)


def gather_kernel(at_ref, a_ref, b_ref, c_ref, d_ref, out_ref):
    put_in_order(at_ref, (a_ref, b_ref, c_ref, d_ref), out_ref, a_ref.shape[0] // PAIRS**2)


def output_kernel(at_ref, conv_ref, attn_ref, own_ref, other_ref, out_ref, w_ref):
    core = at_ref[2]
    block = own_ref.shape[0] // SIDE**2
    for source, to_core in ((own_ref, core), (other_ref, 1 - core)):
        for chip in range(SIDE**2):
            to = pl.multiple_of(chip * CORES * block + to_core * block, block)
            w_ref[pl.ds(to, block), :] = source[pl.ds(chip * block, block), :]
    half = conv_ref.shape[1]

    @pl.loop(0, out_ref.shape[1] // TILE)
    def _(step):
        cols = pl.ds(pl.multiple_of(step * TILE, TILE), TILE)
        contract = (((1,), (1,)), ((), ()))
        total = lax.dot_general(
            conv_ref[...], w_ref[cols, :half], contract, preferred_element_type=jnp.float32
        ) + lax.dot_general(
            attn_ref[...], w_ref[cols, half:], contract, preferred_element_type=jnp.float32
        )
        out_ref[:, cols] = total.astype(jnp.bfloat16)


def layer(
    tokens,
    norm_gain,
    w_conv_value,
    w_conv_gate,
    w_query,
    w_key,
    w_value,
    conv_taps,
    ln_gain,
    sinks,
    out_conv,
    out_attn,
):
    core = lax.axis_index("core")
    chip = lax.axis_index("chip")
    own_rows = tokens.shape[0]
    row_count = own_rows * CORES

    tokens_other = lax.ppermute(tokens, SP, OTHER_CORE)

    def own_half(weights):
        halves = jnp.stack(
            [
                jnp.concatenate(
                    [w[:, h * (w.shape[1] // CORES) : (h + 1) * (w.shape[1] // CORES)] for w in weights],
                    axis=1,
                )
                for h in range(CORES)
            ]
        )
        return repeated(halves, PAIRS * PAIRS).reshape(-1, *halves.shape[1:])

    at = jnp.stack([(chip // SIDE) % 2, chip % 2, core]).astype(jnp.int32)

    def from_square(far):
        own = far.reshape(-1, far.shape[-1])
        return (own, *(lax.ppermute(own, SP, pairs) for pairs in NEAR))

    far_conv = exchanged(own_half((w_conv_value, w_conv_gate)), FAR_BOTH)
    far_qkv = exchanged(own_half((w_query, w_key, w_value)), FAR_BOTH)
    near_conv = from_square(far_conv)
    turned = jnp.concatenate([out_conv.T, out_attn.T], axis=1)
    out_depth, out_width = turned.shape
    far_out = exchanged(repeated(turned, PAIRS * PAIRS).reshape(-1, out_width), FAR_ONE)
    near_qkv = from_square(far_qkv)
    near_out = from_square(far_out)
    out_own = call(
        gather_kernel,
        jax.ShapeDtypeStruct((SIDE**2 * out_depth, out_width), jnp.bfloat16),
        [],
        1 << 28,
        at,
        *near_out,
    )
    out_other = lax.ppermute(out_own, SP, OTHER_CORE)

    both = jnp.where(
        core == 0,
        jnp.concatenate([tokens, tokens_other], axis=0),
        jnp.concatenate([tokens_other, tokens], axis=0),
    )
    as_float = both.astype(jnp.float32)
    normed = (
        as_float
        * lax.rsqrt(jnp.mean(as_float * as_float, axis=-1, keepdims=True) + NORM_EPS)
        * norm_gain.astype(jnp.float32)
    ).astype(jnp.bfloat16)

    channels = w_conv_value.shape[1] // CORES
    q_cols = w_query.shape[1] // CORES
    model = normed.shape[1]
    glu = call(
        gated_kernel,
        jax.ShapeDtypeStruct((row_count, channels), jnp.bfloat16),
        [pltpu.VMEM((model, 2 * channels), jnp.bfloat16)],
        2 * row_count * model * 2 * channels,
        at,
        normed,
        *near_conv,
    )
    offset = chip * row_count
    positions = offset + jnp.arange(row_count, dtype=jnp.int32)
    half_dim = HEAD_DIM // 2
    inverse = ROPE_BASE ** (-jnp.arange(half_dim, dtype=jnp.float32) / half_dim)
    angles = positions.astype(jnp.float32)[:, None] * inverse[None, :]
    cosine, sine = jnp.cos(angles), jnp.sin(angles)
    query_heads = q_cols // HEAD_DIM
    qkv = call(
        rotated_kernel,
        jax.ShapeDtypeStruct((row_count, q_cols + 2 * HEAD_DIM), jnp.bfloat16),
        [pltpu.VMEM((model, q_cols + 2 * HEAD_DIM), jnp.bfloat16)],
        2 * row_count * model * (q_cols + 2 * HEAD_DIM),
        at,
        normed,
        jnp.concatenate([cosine] * 4, axis=1),
        jnp.concatenate([-sine, sine] * 2, axis=1),
        *near_qkv,
    )
    query = qkv[:, :q_cols].reshape(row_count, query_heads, HEAD_DIM)
    key_value = qkv[:, q_cols:]
    key = key_value[:, :HEAD_DIM]
    value_rows = key_value[:, HEAD_DIM:]

    glu_before = lax.ppermute(glu[row_count - 32 :], SP, NEXT_CHIP)
    before = lax.ppermute(key_value[row_count - WINDOW :], SP, NEXT_CHIP)
    key_before = before[:, :HEAD_DIM]
    value_before = before[:, HEAD_DIM:]

    taps = lax.dynamic_slice_in_dim(conv_taps, core * channels, channels, 1)
    conv_out, sums = call(
        conv_kernel,
        (
            jax.ShapeDtypeStruct((row_count, channels), jnp.float32),
            jax.ShapeDtypeStruct((2, row_count), jnp.float32),
        ),
        [pltpu.VMEM((2, row_count + 32, 128), jnp.float32)],
        2 * row_count * channels * 32 * 32,
        at,
        glu_before,
        glu,
        taps,
    )
    members = CORES * lax.axis_size("tp")
    everyones = lax.all_to_all(repeated(sums, members), CHIP, 0, 0, tiled=True)
    totals = jnp.sum(everyones, axis=0)
    mean = (totals[0] / CONV_CH)[:, None]
    var = (totals[1] / CONV_CH)[:, None] - mean * mean
    gain = lax.dynamic_slice_in_dim(ln_gain, core * channels, channels, 0)
    conv_branch = jax.nn.silu(
        (conv_out - mean) * lax.rsqrt(var + CHANNEL_EPS) * gain[None, :]
    ).astype(jnp.bfloat16)

    blocks = row_count // WINDOW
    q_blocks = query.reshape(blocks, WINDOW, query_heads, HEAD_DIM)
    key_blocks = jnp.concatenate([key_before, key], axis=0).reshape(blocks + 1, WINDOW, HEAD_DIM)
    value_blocks = jnp.concatenate([value_before, value_rows], axis=0).reshape(
        blocks + 1, WINDOW, HEAD_DIM
    )
    key_window = jnp.concatenate([key_blocks[:-1], key_blocks[1:]], axis=1)
    value_window = jnp.concatenate([value_blocks[:-1], value_blocks[1:]], axis=1)
    scores = jnp.einsum(
        "nqgd,nkd->ngqk", q_blocks, key_window, preferred_element_type=jnp.float32
    ) * HEAD_DIM ** (-0.5)
    query_index = jnp.arange(WINDOW)[:, None] + WINDOW
    key_index = jnp.arange(2 * WINDOW)[None, :]
    band = (key_index <= query_index) & (query_index - key_index < WINDOW)
    block_index = jnp.arange(blocks)[:, None, None]
    allowed = band[None] & (offset + block_index * WINDOW + key_index[None] - WINDOW >= 0)
    allowed = allowed[:, None]
    sums_exp = jnp.sum(jnp.where(allowed, jnp.exp(scores), 0.0), axis=-1)
    own_sinks = lax.dynamic_slice_in_dim(sinks, core * query_heads, query_heads, 0)
    log_total = jnp.log(sums_exp + jnp.exp(own_sinks)[None, :, None])
    weights = jnp.where(allowed, jnp.exp(scores - log_total[..., None]), 0.0).astype(jnp.bfloat16)
    attended = jnp.einsum(
        "ngqk,nkd->nqgd", weights, value_window, preferred_element_type=jnp.float32
    )
    attn_branch = attended.astype(jnp.bfloat16).reshape(row_count, q_cols)
    log_rows = log_total.transpose(1, 0, 2).reshape(query_heads, row_count)

    def swapped(value, axis):
        kept = lax.dynamic_slice_in_dim(value, core * own_rows, own_rows, axis)
        given = lax.dynamic_slice_in_dim(value, (1 - core) * own_rows, own_rows, axis)
        return kept, lax.ppermute(given, SP, OTHER_CORE)

    def joined(kept, got, axis):
        return jnp.where(
            core == 0,
            jnp.concatenate([kept, got], axis=axis),
            jnp.concatenate([got, kept], axis=axis),
        )

    log_sums = joined(*swapped(log_rows, 1), 0)
    attn_full = joined(*swapped(attn_branch, 0), 1)
    conv_full = joined(*swapped(conv_branch, 0), 1)

    partial = call(
        output_kernel,
        jax.ShapeDtypeStruct((own_rows, model), jnp.bfloat16),
        [pltpu.VMEM((model, out_width), jnp.bfloat16)],
        2 * own_rows * model * out_width,
        at,
        conv_full,
        attn_full,
        out_own,
        out_other,
    )
    peers = lax.axis_size("tp")
    arrived = lax.all_to_all(
        partial.reshape(peers, own_rows // peers, -1), "tp", split_axis=0, concat_axis=0, tiled=True
    )
    mixed = arrived.astype(jnp.float32).sum(axis=0)
    return (mixed.astype(jnp.bfloat16), log_sums)


def solution(mesh):
    split = Mesh(mesh.devices.reshape(-1, CORES, mesh.shape["tp"]), ("chip", "core", "tp"))
    in_specs = (
        P(SP, None),
        P(),
        P(SP, "tp"),
        P(SP, "tp"),
        P(SP, "tp"),
        P(SP, "tp"),
        P(SP, "tp"),
        P(None, "tp"),
        P("tp"),
        P("tp"),
        P("tp", SP),
        P("tp", SP),
    )
    out_specs = (P((*SP, "tp"), None), P("tp", SP))
    return jax.shard_map(layer, mesh=split, in_specs=in_specs, out_specs=out_specs, check_vma=False)
```

```python
import functools

import jax
import jax.numpy as jnp
from jax import lax
from jax.experimental import pallas as pl
from jax.experimental.pallas import tpu as pltpu
from jax.sharding import Mesh, PartitionSpec as P

CONV_CH = 2048
HEAD_DIM = 64
WINDOW = 128

NORM_EPS = 1e-06
CHANNEL_EPS = 1e-05
ROPE_BASE = 10000.0

SIDE = 8
CHIPS = SIDE * SIDE
CORES = 2
SP = ("chip", "core")
CHIP = ("core", "tp")


def place(z, y, core):
    return ((z % SIDE) * SIDE + y % SIDE) * CORES + core


def at_line(line, step, core):
    return place(line, step, core) if core == 0 else place(step, line, core)


LINES = [[at_line(i, j, c) for j in range(SIDE)] for c in range(CORES) for i in range(SIDE)]
AHEAD, BEHIND = (
    [
        (at_line(i, j, c), at_line(i + by, j, c))
        for c in range(CORES)
        for i in range(SIDE)
        for j in range(SIDE)
    ]
    for by in (1, -1)
)
OTHER_CORE = [(i, i ^ 1) for i in range(CHIPS * CORES)]
NEXT_CHIP = [(i, i + CORES) for i in range(CHIPS * CORES - CORES)]

VMEM = pl.BlockSpec(memory_space=pltpu.VMEM)
SMEM = pl.BlockSpec(memory_space=pltpu.SMEM)
ANY = pl.BlockSpec(memory_space=pl.ANY)
TILE = 256


def call(body, outs, flops, in_specs, operands, scratch=(), limit=12):
    return pl.pallas_call(
        body,
        out_shape=outs,
        in_specs=in_specs,
        out_specs=jax.tree.map(lambda _: VMEM, outs),
        scratch_shapes=list(scratch),
        compiler_params=pltpu.CompilerParams(vmem_limit_bytes=limit << 20),
        cost_estimate=pl.CostEstimate(flops=flops, bytes_accessed=1 << 20, transcendentals=0),
    )(*operands)


def shape(dims, dtype=jnp.bfloat16):
    return jax.ShapeDtypeStruct(dims, dtype)


def pack_kernel(at_ref, value_ref, gate_ref, query_ref, key_ref, v_ref, conv_ref, attn_ref, out_ref):
    core = at_ref[3]
    lane = lax.broadcasted_iota(jnp.int32, key_ref.shape, 1)
    key = key_ref[...].astype(jnp.float32)
    value = v_ref[...].astype(jnp.float32)
    both = (
        jnp.where(lane < HEAD_DIM, key, pltpu.roll(value, HEAD_DIM, 1)),
        jnp.where(lane < HEAD_DIM, pltpu.roll(key, HEAD_DIM, 1), value),
    )
    for half in range(CORES):
        to = jnp.bitwise_xor(core, half)
        at = 0
        for source in (value_ref, gate_ref, query_ref, None, conv_ref, attn_ref):
            if source is None:
                part = both[half].astype(jnp.bfloat16)
            else:
                width = source.shape[1] // CORES
                part = source[:, half * width : (half + 1) * width]
            out_ref[to, :, at : at + part.shape[1]] = part
            at += part.shape[1]


def repeat_kernel(at_ref, kept_ref, got_ref, out_ref):
    core, rows = at_ref[3], kept_ref.shape[0]
    for source, to_core in ((kept_ref, core), (got_ref, 1 - core)):
        to = pl.ds(pl.multiple_of(to_core * rows, rows), rows)
        for member in range(out_ref.shape[0]):
            out_ref[member, to, :] = source[...]


def fetch(at_ref, pieces, out_ref, sem, columns):
    block = pieces[0].shape[1]
    line, line_rows, step_rows = at_ref[0], at_ref[1], at_ref[2]
    for index, piece in enumerate(pieces):
        away = (index + 1) // 2 * (1 if index % 2 == 0 else -1)
        from_line = jnp.bitwise_and(line + away, SIDE - 1)
        count = piece.shape[0]
        first = SIDE - count if index == SIDE else 0
        for step in range(count):
            to = pl.multiple_of(from_line * line_rows + (first + step) * step_rows, block)
            pltpu.make_async_copy(
                piece.at[step, :, pl.ds(*columns)], out_ref.at[pl.ds(to, block), :], sem
            ).start()
    pltpu.make_async_copy(out_ref, out_ref, sem).wait()


def gated_kernel(columns, at_ref, x_ref, *refs):
    pieces, (out_ref, w_ref, sem) = refs[:-3], refs[-3:]
    fetch(at_ref, pieces, w_ref, sem, columns)
    half = out_ref.shape[1]

    @pl.loop(0, x_ref.shape[0] // TILE)
    def _(step):
        rows = pl.ds(pl.multiple_of(step * TILE, TILE), TILE)
        both = jnp.dot(x_ref[rows, :], w_ref[...], preferred_element_type=jnp.float32)
        both = both.astype(jnp.bfloat16).astype(jnp.float32)
        out_ref[rows, :] = (both[:, :half] * jax.nn.sigmoid(both[:, half:])).astype(jnp.bfloat16)


def rotated_kernel(columns, at_ref, x_ref, cos_ref, sin_ref, *refs):
    pieces, (out_ref, w_ref, sem) = refs[:-3], refs[-3:]
    fetch(at_ref, pieces, w_ref, sem, columns)
    width = out_ref.shape[1]

    @pl.loop(0, x_ref.shape[0] // TILE)
    def _(step):
        rows = pl.ds(pl.multiple_of(step * TILE, TILE), TILE)
        raw = jnp.dot(x_ref[rows, :], w_ref[...], preferred_element_type=jnp.float32)
        raw = raw.astype(jnp.bfloat16).astype(jnp.float32)
        lane = lax.broadcasted_iota(jnp.int32, (TILE, 128), 1)
        front = jnp.bitwise_and(lane, HEAD_DIM - 1) < HEAD_DIM // 2
        cosine, sine = cos_ref[rows, :], sin_ref[rows, :]
        for at in range(0, width, 128):
            part = raw[:, at : at + 128]
            other = jnp.where(
                front,
                pltpu.roll(part, 128 - HEAD_DIM // 2, 1),
                pltpu.roll(part, HEAD_DIM // 2, 1),
            )
            turned = part * cosine + other * sine
            if at + 128 == width:
                turned = jnp.where(lane < HEAD_DIM, turned, part)
            out_ref[rows, at : at + 128] = turned.astype(jnp.bfloat16)


def order_kernel(columns, at_ref, *refs):
    pieces, (out_ref, sem) = refs[:-2], refs[-2:]
    fetch(at_ref, pieces, out_ref, sem, columns)


def conv_kernel(before_ref, glu_ref, taps_ref, out_ref, sums_ref, ext_ref):
    count, rows = taps_ref.shape[0], glu_ref.shape[0]
    lead = before_ref.shape[0]
    for part in range(2):
        lanes = pl.ds(part * 128, 128)
        ext_ref[part, pl.ds(0, lead), :] = before_ref[:, lanes].astype(jnp.float32)
        ext_ref[part, pl.ds(lead, rows), :] = glu_ref[:, lanes].astype(jnp.float32)

    @pl.loop(0, rows // 128)
    def _(step):
        base = pl.multiple_of(step * 128, 128)
        first = jnp.zeros((128, 128), jnp.float32)
        second = jnp.zeros((128, 128), jnp.float32)
        for part in range(2):
            lanes = pl.ds(part * 128, 128)
            total = jnp.zeros((128, 128), jnp.float32)
            for tap in range(count):
                rows_at = pl.ds(base + (lead - count + 1 + tap), 128)
                total = total + taps_ref[pl.ds(tap, 1), lanes] * ext_ref[part, rows_at, :]
            out_ref[pl.ds(base, 128), lanes] = total
            first = first + total
            second = second + total * total
        sums_ref[pl.ds(0, 1), pl.ds(base, 128)] = jnp.sum(first.T, axis=0, keepdims=True)
        sums_ref[pl.ds(1, 1), pl.ds(base, 128)] = jnp.sum(second.T, axis=0, keepdims=True)


def scaled_kernel(at_ref, conv_ref, sums_ref, gain_ref, kept_ref, given_ref):
    core = at_ref[3]
    totals = sums_ref[0]
    for member in range(1, sums_ref.shape[0]):
        totals = totals + sums_ref[member]
    mean = totals[0:1] / CONV_CH
    scale = lax.rsqrt(totals[1:2] / CONV_CH - mean * mean + CHANNEL_EPS)
    half = kept_ref.shape[0]
    for base in range(0, conv_ref.shape[0], 128):
        at = slice(base, base + 128)
        mean_at = jnp.broadcast_to(mean[:, at], (128, 128)).T
        scale_at = jnp.broadcast_to(scale[:, at], (128, 128)).T
        parts = []
        for lanes in (slice(0, 128), slice(128, 256)):
            normed = (conv_ref[at, lanes] - mean_at) * scale_at * gain_ref[0:1, lanes]
            parts.append((normed * jax.nn.sigmoid(normed)).astype(jnp.bfloat16))
        out = jnp.concatenate(parts, axis=1)
        to = slice(base % half, base % half + 128)

        @pl.when(core == base // half)
        def _():
            kept_ref[to, :] = out

        @pl.when(core != base // half)
        def _():
            given_ref[to, :] = out


def attention_kernel(
    at_ref, sinks_ref, qkv_ref, before_ref, kept_ref, given_ref, logs_ref, k_lo, k_hi, v_lo, v_hi
):
    core, first_chip = at_ref[3], at_ref[4]
    cols = kept_ref.shape[1]
    lead = before_ref.shape[0]
    for source, to in ((before_ref, 0), (qkv_ref, lead)):
        both = source[:, source.shape[1] - 128 :].astype(jnp.float32)
        low = lax.broadcasted_iota(jnp.int32, both.shape, 1) < HEAD_DIM
        turned = pltpu.roll(both, HEAD_DIM, 1)
        rows = slice(to, to + both.shape[0])
        k_lo[rows, :] = jnp.where(low, both, 0.0).astype(jnp.bfloat16)
        k_hi[rows, :] = jnp.where(low, 0.0, turned).astype(jnp.bfloat16)
        v_lo[rows, :] = jnp.where(low, turned, 0.0).astype(jnp.bfloat16)
        v_hi[rows, :] = jnp.where(low, 0.0, both).astype(jnp.bfloat16)
    blocks = qkv_ref.shape[0] // WINDOW
    half_blocks = blocks // CORES
    heads = cols // HEAD_DIM

    @pl.loop(0, blocks)
    def _(block):
        base = pl.multiple_of(block * WINDOW, WINDOW)
        window = pl.ds(base, 2 * WINDOW)
        key_at = lax.broadcasted_iota(jnp.int32, (2 * WINDOW, WINDOW), 0)
        query_at = lax.broadcasted_iota(jnp.int32, (2 * WINDOW, WINDOW), 1)
        lowest = jnp.where((first_chip == 1) & (block == 0), WINDOW, 0)
        allowed = (key_at > query_at) & (key_at <= query_at + WINDOW) & (key_at >= lowest)
        outs = []
        for pair in range(heads // 2):
            query = qkv_ref[pl.ds(base, WINDOW), pair * 128 : (pair + 1) * 128]
            total = jnp.zeros((WINDOW, 128), jnp.float32)
            for which, (keys, values) in enumerate(((k_lo, v_lo), (k_hi, v_hi))):
                head = 2 * pair + which
                scores = (
                    lax.dot_general(
                        keys[window, :],
                        query,
                        (((1,), (1,)), ((), ())),
                        preferred_element_type=jnp.float32,
                    )
                    * HEAD_DIM ** (-0.5)
                )
                sums = jnp.sum(jnp.where(allowed, jnp.exp(scores), 0.0), axis=0, keepdims=True)
                sink = jnp.full((1, WINDOW), sinks_ref[core * heads + head], jnp.float32)
                log_total = jnp.log(sums + jnp.exp(sink))
                logs_ref[pl.ds(head, 1), pl.ds(base, WINDOW)] = log_total
                weights = jnp.where(allowed, jnp.exp(scores - log_total), 0.0).astype(jnp.bfloat16)
                total = total + lax.dot_general(
                    weights,
                    values[window, :],
                    (((0,), (0,)), ((), ())),
                    preferred_element_type=jnp.float32,
                )
            outs.append(total.astype(jnp.bfloat16))
        out = jnp.concatenate(outs, axis=1)
        own = block // half_blocks == core
        to = pl.ds(pl.multiple_of((block % half_blocks) * WINDOW, WINDOW), WINDOW)

        @pl.when(own)
        def _():
            kept_ref[to, :] = out

        @pl.when(jnp.logical_not(own))
        def _():
            given_ref[to, :] = out


def output_kernel(
    steps, at_ref, conv_ref, attn_ref, conv_got, attn_got, own_ref, other_ref, *out_refs
):
    member, half = at_ref[5], conv_ref.shape[1]
    peers = conv_ref.shape[0] // out_refs[0].shape[0]
    count = out_refs[0].shape[0]
    for away, out_ref in zip(steps, out_refs):
        to = jnp.bitwise_and(member + away, peers - 1)
        rows = pl.ds(pl.multiple_of(to * count, count), count)

        @pl.loop(0, out_ref.shape[1] // TILE)
        def _(step):
            cols = pl.ds(pl.multiple_of(step * TILE, TILE), TILE)
            total = jnp.zeros((count, TILE), jnp.float32)
            for left, right, at in (
                (conv_ref, own_ref, 0),
                (attn_ref, own_ref, half),
                (conv_got, other_ref, 0),
                (attn_got, other_ref, half),
            ):
                total = total + lax.dot_general(
                    left[rows, :],
                    right[cols, at : at + half],
                    (((1,), (1,)), ((), ())),
                    preferred_element_type=jnp.float32,
                )
            out_ref[:, cols] = total.astype(jnp.bfloat16)


def layer(
    tokens,
    norm_gain,
    w_conv_value,
    w_conv_gate,
    w_query,
    w_key,
    w_value,
    conv_taps,
    ln_gain,
    sinks,
    out_conv,
    out_attn,
):
    core = lax.axis_index("core")
    chip = lax.axis_index("chip")
    member = lax.axis_index("tp")
    own_rows, model = tokens.shape
    row_count = own_rows * CORES
    depth = w_conv_value.shape[0]
    channels = w_conv_value.shape[1] // CORES
    q_cols = w_query.shape[1] // CORES
    query_heads = q_cols // HEAD_DIM
    block = CORES * depth

    z, y = chip // SIDE, chip % SIDE
    at = jnp.stack(
        [
            jnp.where(core == 0, z, y),
            jnp.where(core == 0, SIDE * block, block),
            jnp.where(core == 0, block, SIDE * block),
            core,
            (chip == 0).astype(jnp.int32),
            member,
        ]
    ).astype(jnp.int32)

    conv_cols = (0, 2 * channels)
    qkv_cols = (2 * channels, q_cols + 2 * HEAD_DIM)
    out_cols = (2 * channels + q_cols + 2 * HEAD_DIM, channels + q_cols)
    width = sum(out_cols)
    halves = call(
        pack_kernel,
        shape((CORES, depth, width)),
        1 << 20,
        [SMEM] + [VMEM] * 7,
        (at, w_conv_value, w_conv_gate, w_query, w_key, w_value, out_conv.T, out_attn.T),
    )
    got = lax.ppermute(halves[1], SP, OTHER_CORE)
    sent = call(
        repeat_kernel,
        shape((SIDE, block, width)),
        1 << 20,
        [SMEM, VMEM, VMEM],
        (at, halves[0], got),
    )
    own_line = lax.all_to_all(sent, SP, 0, 0, tiled=True, axis_index_groups=LINES)
    pieces = [own_line]
    ahead = behind = own_line
    for step in range(SIDE // 2):
        if step == SIDE // 2 - 1:
            ahead, behind = ahead[: SIDE // 2], behind[SIDE // 2 :]
        ahead = lax.ppermute(ahead, SP, AHEAD)
        behind = lax.ppermute(behind, SP, BEHIND)
        pieces += [ahead, behind]

    tokens_other = lax.ppermute(tokens, SP, OTHER_CORE)
    both = jnp.where(
        core == 0,
        jnp.concatenate([tokens, tokens_other], axis=0),
        jnp.concatenate([tokens_other, tokens], axis=0),
    )
    as_float = both.astype(jnp.float32)
    normed = (
        as_float
        * lax.rsqrt(jnp.mean(as_float * as_float, axis=-1, keepdims=True) + NORM_EPS)
        * norm_gain.astype(jnp.float32)
    ).astype(jnp.bfloat16)

    positions = chip * row_count + jnp.arange(row_count, dtype=jnp.int32)
    half_dim = HEAD_DIM // 2
    inverse = ROPE_BASE ** (-jnp.arange(half_dim, dtype=jnp.float32) / half_dim)
    angles = positions.astype(jnp.float32)[:, None] * inverse[None, :]
    cosine, sine = jnp.cos(angles), jnp.sin(angles)
    cosines = jnp.concatenate([cosine] * 4, axis=1)
    sines = jnp.concatenate([-sine, sine] * 2, axis=1)

    spots = [ANY] * len(pieces)
    glu = call(
        functools.partial(gated_kernel, conv_cols),
        shape((row_count, channels)),
        2 * row_count * model * conv_cols[1],
        [SMEM, VMEM] + spots,
        (at, normed, *pieces),
        (pltpu.VMEM((model, conv_cols[1]), jnp.bfloat16), pltpu.SemaphoreType.DMA),
    )
    glu_before = lax.ppermute(glu[row_count - 32 :], SP, NEXT_CHIP)
    qkv = call(
        functools.partial(rotated_kernel, qkv_cols),
        shape((row_count, qkv_cols[1])),
        2 * row_count * model * qkv_cols[1],
        [SMEM, VMEM, VMEM, VMEM] + spots,
        (at, normed, cosines, sines, *pieces),
        (pltpu.VMEM((model, qkv_cols[1]), jnp.bfloat16), pltpu.SemaphoreType.DMA),
    )
    kv_before = lax.ppermute(qkv[row_count - WINDOW :, q_cols:], SP, NEXT_CHIP)
    out_own = call(
        functools.partial(order_kernel, out_cols),
        shape((model, out_cols[1])),
        1 << 28,
        [SMEM] + spots,
        (at, *pieces),
        (pltpu.SemaphoreType.DMA,),
    )
    out_other = lax.ppermute(out_own, SP, OTHER_CORE)

    taps = lax.dynamic_slice_in_dim(conv_taps, core * channels, channels, 1)
    conv_out, sums = call(
        conv_kernel,
        (shape((row_count, channels), jnp.float32), shape((2, row_count), jnp.float32)),
        1 << 32,
        [VMEM] * 3,
        (glu_before, glu, taps),
        (pltpu.VMEM((2, row_count + 32, 128), jnp.float32),),
    )
    members = CORES * lax.axis_size("tp")
    everyones = lax.all_to_all(
        jnp.broadcast_to(sums[None], (members, *sums.shape)), CHIP, 0, 0, tiled=True
    )
    extended = pltpu.VMEM((row_count + WINDOW, 128), jnp.bfloat16)
    attn_kept, attn_given, log_rows = call(
        attention_kernel,
        (
            shape((own_rows, q_cols)),
            shape((own_rows, q_cols)),
            shape((query_heads, row_count), jnp.float32),
        ),
        1 << 32,
        [SMEM, SMEM, VMEM, VMEM],
        (at, sinks, qkv, kv_before),
        (extended,) * 4,
    )
    attn_got = lax.ppermute(attn_given, SP, OTHER_CORE)
    gain = lax.dynamic_slice_in_dim(ln_gain, core * channels, channels, 0)
    conv_kept, conv_given = call(
        scaled_kernel,
        (shape((own_rows, channels)),) * 2,
        1 << 28,
        [SMEM, VMEM, VMEM, VMEM],
        (at, conv_out, everyones, gain[None]),
    )
    conv_got = lax.ppermute(conv_given, SP, OTHER_CORE)

    kept = lax.dynamic_slice_in_dim(log_rows, core * own_rows, own_rows, 1)
    given = lax.dynamic_slice_in_dim(log_rows, (1 - core) * own_rows, own_rows, 1)
    logs_got = lax.ppermute(given, SP, OTHER_CORE)
    log_sums = jnp.where(
        core == 0,
        jnp.concatenate([kept, logs_got], axis=0),
        jnp.concatenate([logs_got, kept], axis=0),
    )

    peers = lax.axis_size("tp")
    share = own_rows // peers

    def output(steps):
        return call(
            functools.partial(output_kernel, steps),
            (shape((share, model)),) * len(steps),
            2 * share * len(steps) * model * 2 * out_cols[1],
            [SMEM] + [VMEM] * 6,
            (at, conv_kept, attn_kept, conv_got, attn_got, out_own, out_other),
        )

    def to_member(value, away):
        return lax.ppermute(value, "tp", [(i, (i + away) % peers) for i in range(peers)])

    (far,) = output((2,))
    far = to_member(far, 2)
    up, down, mine = output((1, 3, 0))
    up, down = to_member(up, 1), to_member(down, 3)
    mixed = (
        mine.astype(jnp.float32)
        + far.astype(jnp.float32)
        + up.astype(jnp.float32)
        + down.astype(jnp.float32)
    )
    return (mixed.astype(jnp.bfloat16), log_sums)


def solution(mesh):
    split = Mesh(mesh.devices.reshape(-1, CORES, mesh.shape["tp"]), ("chip", "core", "tp"))
    in_specs = (
        P(SP, None),
        P(),
        P(SP, "tp"),
        P(SP, "tp"),
        P(SP, "tp"),
        P(SP, "tp"),
        P(SP, "tp"),
        P(None, "tp"),
        P("tp"),
        P("tp"),
        P("tp", SP),
        P("tp", SP),
    )
    out_specs = (P((*SP, "tp"), None), P("tp", SP))
    return jax.shard_map(layer, mesh=split, in_specs=in_specs, out_specs=out_specs, check_vma=False)
```

```python
import functools

import jax
import jax.numpy as jnp
from jax import lax
from jax.experimental import pallas as pl
from jax.experimental.pallas import tpu as pltpu
from jax.sharding import Mesh, PartitionSpec as P

CONV_CH = 2048
HEAD_DIM = 64
WINDOW = 128

NORM_EPS = 1e-06
CHANNEL_EPS = 1e-05
ROPE_BASE = 10000.0

SIDE = 8
CHIPS = SIDE * SIDE
CORES = 2
SP = ("chip", "core")
CHIP = ("core", "tp")


def place(z, y, core):
    return ((z % SIDE) * SIDE + y % SIDE) * CORES + core


def at_line(line, step, core):
    return place(line, step, core) if core == 0 else place(step, line, core)


LINES = [[at_line(i, j, c) for j in range(SIDE)] for c in range(CORES) for i in range(SIDE)]
AHEAD, BEHIND = (
    [
        (at_line(i, j, c), at_line(i + by, j, c))
        for c in range(CORES)
        for i in range(SIDE)
        for j in range(SIDE)
    ]
    for by in (1, -1)
)
OTHER_CORE = [(i, i ^ 1) for i in range(CHIPS * CORES)]
NEXT_CHIP = [(i, i + CORES) for i in range(CHIPS * CORES - CORES)]

VMEM = pl.BlockSpec(memory_space=pltpu.VMEM)
SMEM = pl.BlockSpec(memory_space=pltpu.SMEM)
HBM = pl.BlockSpec(memory_space=pltpu.MemorySpace.HBM)
TILE = 256


def call(body, outs, flops, in_specs, operands, scratch=(), limit=None):
    return pl.pallas_call(
        body,
        out_shape=outs,
        in_specs=in_specs,
        out_specs=jax.tree.map(lambda _: VMEM, outs),
        scratch_shapes=list(scratch),
        compiler_params=pltpu.CompilerParams(vmem_limit_bytes=limit and limit << 20),
        cost_estimate=pl.CostEstimate(flops=flops, bytes_accessed=1 << 20, transcendentals=0),
    )(*operands)


def shape(dims, dtype=jnp.bfloat16):
    return jax.ShapeDtypeStruct(dims, dtype)


def pack_kernel(at_ref, *refs):
    count = (len(refs) - 2) // 2
    shards, out_ref, held, sems = refs[:count], refs[count], refs[count + 1 : -1], refs[-1]
    copies = [
        pltpu.make_async_copy(shard, here, sems.at[index])
        for index, (shard, here) in enumerate(zip(shards, held))
    ]
    for copy in copies:
        copy.start()
    for copy in copies:
        copy.wait()
    value_ref, gate_ref, query_ref, key_ref, v_ref, conv_ref, attn_ref = held
    core = at_ref[3]
    lane = lax.broadcasted_iota(jnp.int32, key_ref.shape, 1)
    key = key_ref[...].astype(jnp.float32)
    value = v_ref[...].astype(jnp.float32)
    both = (
        jnp.where(lane < HEAD_DIM, key, pltpu.roll(value, HEAD_DIM, 1)),
        jnp.where(lane < HEAD_DIM, pltpu.roll(key, HEAD_DIM, 1), value),
    )
    for half in range(CORES):
        to = jnp.bitwise_xor(core, half)
        at = 0
        for source in (value_ref, gate_ref, query_ref, None, conv_ref, attn_ref):
            if source is None:
                part = both[half].astype(jnp.bfloat16)
            else:
                width = source.shape[1] // CORES
                part = source[:, half * width : (half + 1) * width]
            out_ref[to, :, at : at + part.shape[1]] = part
            at += part.shape[1]


def repeat_kernel(at_ref, kept_ref, got_ref, out_ref):
    core, rows = at_ref[3], kept_ref.shape[0]
    for source, to_core in ((kept_ref, core), (got_ref, 1 - core)):
        to = pl.ds(pl.multiple_of(to_core * rows, rows), rows)
        for member in range(out_ref.shape[0]):
            out_ref[member, to, :] = source[...]


def fetch(at_ref, pieces, out_ref, sem, columns):
    block = pieces[0].shape[1]
    line, line_rows, step_rows = at_ref[0], at_ref[1], at_ref[2]
    for index, piece in enumerate(pieces):
        away = (index + 1) // 2 * (1 if index % 2 == 0 else -1)
        from_line = jnp.bitwise_and(line + away, SIDE - 1)
        count = piece.shape[0]
        first = SIDE - count if index == SIDE else 0
        for step in range(count):
            to = pl.multiple_of(from_line * line_rows + (first + step) * step_rows, block)
            pltpu.make_async_copy(
                piece.at[step, :, pl.ds(*columns)], out_ref.at[pl.ds(to, block), :], sem
            ).start()
    pltpu.make_async_copy(out_ref, out_ref, sem).wait()


def rows_of(step):
    return pl.ds(pl.multiple_of(step * TILE, TILE), TILE)


def tile_copy(x_ref, x_here, sems, step):
    rows = rows_of(step)
    return pltpu.make_async_copy(x_ref.at[rows, :], x_here.at[rows, :], sems.at[step])


def gated_kernel(columns, at_ref, x_ref, *refs):
    pieces, (out_ref, w_ref, sem, x_here, x_sems) = refs[:-5], refs[-5:]
    tiles = x_ref.shape[0] // TILE
    for step in range(tiles):
        tile_copy(x_ref, x_here, x_sems, step).start()
    fetch(at_ref, pieces, w_ref, sem, columns)
    half = out_ref.shape[1]

    @pl.loop(0, tiles)
    def _(step):
        tile_copy(x_ref, x_here, x_sems, step).wait()
        rows = rows_of(step)
        both = jnp.dot(x_here[rows, :], w_ref[...], preferred_element_type=jnp.float32)
        both = both.astype(jnp.bfloat16).astype(jnp.float32)
        out_ref[rows, :] = (both[:, :half] * jax.nn.sigmoid(both[:, half:])).astype(jnp.bfloat16)


def rotated_kernel(columns, at_ref, x_ref, cos_ref, sin_ref, *refs):
    pieces, (out_ref, w_ref, sem, x_here, x_sems, cos_here, sin_here, table_sems) = (
        refs[:-8],
        refs[-8:],
    )
    tiles = x_ref.shape[0] // TILE
    for step in range(tiles):
        tile_copy(x_ref, x_here, x_sems, step).start()
    tables = (
        pltpu.make_async_copy(cos_ref, cos_here, table_sems.at[0]),
        pltpu.make_async_copy(sin_ref, sin_here, table_sems.at[1]),
    )
    for table in tables:
        table.start()
    fetch(at_ref, pieces, w_ref, sem, columns)
    for table in tables:
        table.wait()
    width = out_ref.shape[1]

    @pl.loop(0, tiles)
    def _(step):
        tile_copy(x_ref, x_here, x_sems, step).wait()
        rows = rows_of(step)
        raw = jnp.dot(x_here[rows, :], w_ref[...], preferred_element_type=jnp.float32)
        raw = raw.astype(jnp.bfloat16).astype(jnp.float32)
        lane = lax.broadcasted_iota(jnp.int32, (TILE, 128), 1)
        front = jnp.bitwise_and(lane, HEAD_DIM - 1) < HEAD_DIM // 2
        cosine, sine = cos_here[rows, :], sin_here[rows, :]
        for at in range(0, width, 128):
            part = raw[:, at : at + 128]
            other = jnp.where(
                front,
                pltpu.roll(part, 128 - HEAD_DIM // 2, 1),
                pltpu.roll(part, HEAD_DIM // 2, 1),
            )
            turned = part * cosine + other * sine
            if at + 128 == width:
                turned = jnp.where(lane < HEAD_DIM, turned, part)
            out_ref[rows, at : at + 128] = turned.astype(jnp.bfloat16)


def order_kernel(columns, at_ref, *refs):
    pieces, (out_ref, sem) = refs[:-2], refs[-2:]
    fetch(at_ref, pieces, out_ref, sem, columns)


def conv_kernel(before_ref, glu_ref, taps_ref, out_ref, sums_ref, ext_ref):
    count, rows = taps_ref.shape[0], glu_ref.shape[0]
    lead = before_ref.shape[0]
    for part in range(2):
        lanes = pl.ds(part * 128, 128)
        ext_ref[part, pl.ds(0, lead), :] = before_ref[:, lanes].astype(jnp.float32)
        ext_ref[part, pl.ds(lead, rows), :] = glu_ref[:, lanes].astype(jnp.float32)

    @pl.loop(0, rows // 128)
    def _(step):
        base = pl.multiple_of(step * 128, 128)
        first = jnp.zeros((128, 128), jnp.float32)
        second = jnp.zeros((128, 128), jnp.float32)
        for part in range(2):
            lanes = pl.ds(part * 128, 128)
            total = jnp.zeros((128, 128), jnp.float32)
            for tap in range(count):
                rows_at = pl.ds(base + (lead - count + 1 + tap), 128)
                total = total + taps_ref[pl.ds(tap, 1), lanes] * ext_ref[part, rows_at, :]
            out_ref[pl.ds(base, 128), lanes] = total
            first = first + total
            second = second + total * total
        sums_ref[pl.ds(0, 1), pl.ds(base, 128)] = jnp.sum(first.T, axis=0, keepdims=True)
        sums_ref[pl.ds(1, 1), pl.ds(base, 128)] = jnp.sum(second.T, axis=0, keepdims=True)


def scaled_kernel(at_ref, conv_ref, sums_ref, gain_ref, kept_ref, given_ref):
    core = at_ref[3]
    totals = sums_ref[0]
    for member in range(1, sums_ref.shape[0]):
        totals = totals + sums_ref[member]
    mean = totals[0:1] / CONV_CH
    scale = lax.rsqrt(totals[1:2] / CONV_CH - mean * mean + CHANNEL_EPS)
    half = kept_ref.shape[0]
    for base in range(0, conv_ref.shape[0], 128):
        at = slice(base, base + 128)
        mean_at = jnp.broadcast_to(mean[:, at], (128, 128)).T
        scale_at = jnp.broadcast_to(scale[:, at], (128, 128)).T
        parts = []
        for lanes in (slice(0, 128), slice(128, 256)):
            normed = (conv_ref[at, lanes] - mean_at) * scale_at * gain_ref[0:1, lanes]
            parts.append((normed * jax.nn.sigmoid(normed)).astype(jnp.bfloat16))
        out = jnp.concatenate(parts, axis=1)
        to = slice(base % half, base % half + 128)

        @pl.when(core == base // half)
        def _():
            kept_ref[to, :] = out

        @pl.when(core != base // half)
        def _():
            given_ref[to, :] = out


def attention_kernel(
    at_ref, sinks_ref, qkv_ref, before_ref, kept_ref, given_ref, logs_ref, k_lo, k_hi, v_lo, v_hi
):
    core, first_chip = at_ref[3], at_ref[4]
    cols = kept_ref.shape[1]
    lead = before_ref.shape[0]
    for source, to in ((before_ref, 0), (qkv_ref, lead)):
        both = source[:, source.shape[1] - 128 :].astype(jnp.float32)
        low = lax.broadcasted_iota(jnp.int32, both.shape, 1) < HEAD_DIM
        turned = pltpu.roll(both, HEAD_DIM, 1)
        rows = slice(to, to + both.shape[0])
        k_lo[rows, :] = jnp.where(low, both, 0.0).astype(jnp.bfloat16)
        k_hi[rows, :] = jnp.where(low, 0.0, turned).astype(jnp.bfloat16)
        v_lo[rows, :] = jnp.where(low, turned, 0.0).astype(jnp.bfloat16)
        v_hi[rows, :] = jnp.where(low, 0.0, both).astype(jnp.bfloat16)
    blocks = qkv_ref.shape[0] // WINDOW
    half_blocks = blocks // CORES
    heads = cols // HEAD_DIM

    @pl.loop(0, blocks)
    def _(block):
        base = pl.multiple_of(block * WINDOW, WINDOW)
        window = pl.ds(base, 2 * WINDOW)
        key_at = lax.broadcasted_iota(jnp.int32, (2 * WINDOW, WINDOW), 0)
        query_at = lax.broadcasted_iota(jnp.int32, (2 * WINDOW, WINDOW), 1)
        lowest = jnp.where((first_chip == 1) & (block == 0), WINDOW, 0)
        allowed = (key_at > query_at) & (key_at <= query_at + WINDOW) & (key_at >= lowest)
        outs = []
        for pair in range(heads // 2):
            query = qkv_ref[pl.ds(base, WINDOW), pair * 128 : (pair + 1) * 128]
            total = jnp.zeros((WINDOW, 128), jnp.float32)
            for which, (keys, values) in enumerate(((k_lo, v_lo), (k_hi, v_hi))):
                head = 2 * pair + which
                scores = (
                    lax.dot_general(
                        keys[window, :],
                        query,
                        (((1,), (1,)), ((), ())),
                        preferred_element_type=jnp.float32,
                    )
                    * HEAD_DIM ** (-0.5)
                )
                sums = jnp.sum(jnp.where(allowed, jnp.exp(scores), 0.0), axis=0, keepdims=True)
                sink = jnp.full((1, WINDOW), sinks_ref[core * heads + head], jnp.float32)
                log_total = jnp.log(sums + jnp.exp(sink))
                logs_ref[pl.ds(head, 1), pl.ds(base, WINDOW)] = log_total
                weights = jnp.where(allowed, jnp.exp(scores - log_total), 0.0).astype(jnp.bfloat16)
                total = total + lax.dot_general(
                    weights,
                    values[window, :],
                    (((0,), (0,)), ((), ())),
                    preferred_element_type=jnp.float32,
                )
            outs.append(total.astype(jnp.bfloat16))
        out = jnp.concatenate(outs, axis=1)
        own = block // half_blocks == core
        to = pl.ds(pl.multiple_of((block % half_blocks) * WINDOW, WINDOW), WINDOW)

        @pl.when(own)
        def _():
            kept_ref[to, :] = out

        @pl.when(jnp.logical_not(own))
        def _():
            given_ref[to, :] = out


def output_kernel(
    steps, at_ref, conv_ref, attn_ref, conv_got, attn_got, own_ref, other_ref, *out_refs
):
    member, half = at_ref[5], conv_ref.shape[1]
    count = out_refs[0].shape[0]
    peers = conv_ref.shape[0] // count

    @pl.loop(0, out_refs[0].shape[1] // TILE)
    def _(step):
        cols = pl.ds(pl.multiple_of(step * TILE, TILE), TILE)
        total = jnp.zeros((conv_ref.shape[0], TILE), jnp.float32)
        for left, right, at in (
            (conv_ref, own_ref, 0),
            (attn_ref, own_ref, half),
            (conv_got, other_ref, 0),
            (attn_got, other_ref, half),
        ):
            total = total + lax.dot_general(
                left[...],
                right[cols, at : at + half],
                (((1,), (1,)), ((), ())),
                preferred_element_type=jnp.float32,
            )
        for to in range(peers):
            out = total[to * count : (to + 1) * count].astype(jnp.bfloat16)
            for away, out_ref in zip(steps, out_refs):

                @pl.when(jnp.bitwise_and(to - member, peers - 1) == away)
                def _():
                    out_ref[:, cols] = out


def layer(
    tokens,
    norm_gain,
    w_conv_value,
    w_conv_gate,
    w_query,
    w_key,
    w_value,
    conv_taps,
    ln_gain,
    sinks,
    out_conv,
    out_attn,
):
    core = lax.axis_index("core")
    chip = lax.axis_index("chip")
    member = lax.axis_index("tp")
    own_rows, model = tokens.shape
    row_count = own_rows * CORES
    depth = w_conv_value.shape[0]
    channels = w_conv_value.shape[1] // CORES
    q_cols = w_query.shape[1] // CORES
    query_heads = q_cols // HEAD_DIM
    block = CORES * depth

    z, y = chip // SIDE, chip % SIDE
    at = jnp.stack(
        [
            jnp.where(core == 0, z, y),
            jnp.where(core == 0, SIDE * block, block),
            jnp.where(core == 0, block, SIDE * block),
            core,
            (chip == 0).astype(jnp.int32),
            member,
        ]
    ).astype(jnp.int32)

    conv_cols = (0, 2 * channels)
    qkv_cols = (2 * channels, q_cols + 2 * HEAD_DIM)
    out_cols = (2 * channels + q_cols + 2 * HEAD_DIM, channels + q_cols)
    width = sum(out_cols)
    shards_in = (w_conv_value, w_conv_gate, w_query, w_key, w_value, out_conv.T, out_attn.T)
    halves = call(
        pack_kernel,
        shape((CORES, depth, width)),
        1 << 20,
        [SMEM] + [HBM] * len(shards_in),
        (at, *shards_in),
        (
            *(pltpu.VMEM(w.shape, w.dtype) for w in shards_in),
            pltpu.SemaphoreType.DMA((len(shards_in),)),
        ),
    )
    got = lax.ppermute(halves[1], SP, OTHER_CORE)
    sent = call(
        repeat_kernel,
        shape((SIDE, block, width)),
        1 << 20,
        [SMEM, VMEM, VMEM],
        (at, halves[0], got),
        limit=12,
    )
    own_line = lax.all_to_all(sent, SP, 0, 0, tiled=True, axis_index_groups=LINES)
    pieces = [own_line]
    ahead = behind = own_line
    for step in range(SIDE // 2):
        if step == SIDE // 2 - 1:
            ahead, behind = ahead[: SIDE // 2], behind[SIDE // 2 :]
        ahead = lax.ppermute(ahead, SP, AHEAD)
        behind = lax.ppermute(behind, SP, BEHIND)
        pieces += [ahead, behind]

    tokens_other = lax.ppermute(tokens, SP, OTHER_CORE)
    both = jnp.where(
        core == 0,
        jnp.concatenate([tokens, tokens_other], axis=0),
        jnp.concatenate([tokens_other, tokens], axis=0),
    )
    as_float = both.astype(jnp.float32)
    normed = (
        as_float
        * lax.rsqrt(jnp.mean(as_float * as_float, axis=-1, keepdims=True) + NORM_EPS)
        * norm_gain.astype(jnp.float32)
    ).astype(jnp.bfloat16)

    positions = chip * row_count + jnp.arange(row_count, dtype=jnp.int32)
    half_dim = HEAD_DIM // 2
    inverse = ROPE_BASE ** (-jnp.arange(half_dim, dtype=jnp.float32) / half_dim)
    angles = positions.astype(jnp.float32)[:, None] * inverse[None, :]
    cosine, sine = jnp.cos(angles), jnp.sin(angles)
    cosines = jnp.concatenate([cosine] * 4, axis=1)
    sines = jnp.concatenate([-sine, sine] * 2, axis=1)

    spots = [HBM] * len(pieces)
    glu = call(
        functools.partial(gated_kernel, conv_cols),
        shape((row_count, channels)),
        2 * row_count * model * conv_cols[1],
        [SMEM, HBM] + spots,
        (at, normed, *pieces),
        (
            pltpu.VMEM((model, conv_cols[1]), jnp.bfloat16),
            pltpu.SemaphoreType.DMA,
            pltpu.VMEM(normed.shape, jnp.bfloat16),
            pltpu.SemaphoreType.DMA((row_count // TILE,)),
        ),
    )
    glu_before = lax.ppermute(glu[row_count - 32 :], SP, NEXT_CHIP)
    qkv = call(
        functools.partial(rotated_kernel, qkv_cols),
        shape((row_count, qkv_cols[1])),
        2 * row_count * model * qkv_cols[1],
        [SMEM, HBM, HBM, HBM] + spots,
        (at, normed, cosines, sines, *pieces),
        (
            pltpu.VMEM((model, qkv_cols[1]), jnp.bfloat16),
            pltpu.SemaphoreType.DMA,
            pltpu.VMEM(normed.shape, jnp.bfloat16),
            pltpu.SemaphoreType.DMA((row_count // TILE,)),
            pltpu.VMEM(cosines.shape, jnp.float32),
            pltpu.VMEM(sines.shape, jnp.float32),
            pltpu.SemaphoreType.DMA((2,)),
        ),
    )
    kv_before = lax.ppermute(qkv[row_count - WINDOW :, q_cols:], SP, NEXT_CHIP)
    out_own = call(
        functools.partial(order_kernel, out_cols),
        shape((model, out_cols[1])),
        1 << 28,
        [SMEM] + spots,
        (at, *pieces),
        (pltpu.SemaphoreType.DMA,),
    )
    out_other = lax.ppermute(out_own, SP, OTHER_CORE)

    taps = lax.dynamic_slice_in_dim(conv_taps, core * channels, channels, 1)
    conv_out, sums = call(
        conv_kernel,
        (shape((row_count, channels), jnp.float32), shape((2, row_count), jnp.float32)),
        1 << 32,
        [VMEM] * 3,
        (glu_before, glu, taps),
        (pltpu.VMEM((2, row_count + 32, 128), jnp.float32),),
        limit=12,
    )
    members = CORES * lax.axis_size("tp")
    everyones = lax.all_to_all(
        jnp.broadcast_to(sums[None], (members, *sums.shape)), CHIP, 0, 0, tiled=True
    )
    extended = pltpu.VMEM((row_count + WINDOW, 128), jnp.bfloat16)
    attn_kept, attn_given, log_rows = call(
        attention_kernel,
        (
            shape((own_rows, q_cols)),
            shape((own_rows, q_cols)),
            shape((query_heads, row_count), jnp.float32),
        ),
        1 << 32,
        [SMEM, SMEM, VMEM, VMEM],
        (at, sinks, qkv, kv_before),
        (extended,) * 4,
        limit=12,
    )
    attn_got = lax.ppermute(attn_given, SP, OTHER_CORE)
    gain = lax.dynamic_slice_in_dim(ln_gain, core * channels, channels, 0)
    conv_kept, conv_given = call(
        scaled_kernel,
        (shape((own_rows, channels)),) * 2,
        1 << 28,
        [SMEM, VMEM, VMEM, VMEM],
        (at, conv_out, everyones, gain[None]),
        limit=12,
    )
    conv_got = lax.ppermute(conv_given, SP, OTHER_CORE)

    kept = lax.dynamic_slice_in_dim(log_rows, core * own_rows, own_rows, 1)
    given = lax.dynamic_slice_in_dim(log_rows, (1 - core) * own_rows, own_rows, 1)
    logs_got = lax.ppermute(given, SP, OTHER_CORE)
    log_sums = jnp.where(
        core == 0,
        jnp.concatenate([kept, logs_got], axis=0),
        jnp.concatenate([logs_got, kept], axis=0),
    )

    peers = lax.axis_size("tp")
    share = own_rows // peers

    def output(steps):
        return call(
            functools.partial(output_kernel, steps),
            (shape((share, model)),) * len(steps),
            2 * share * len(steps) * model * 2 * out_cols[1],
            [SMEM] + [VMEM] * 6,
            (at, conv_kept, attn_kept, conv_got, attn_got, out_own, out_other),
            limit=16,
        )

    def to_member(value, away):
        return lax.ppermute(value, "tp", [(i, (i + away) % peers) for i in range(peers)])

    far, up, down, mine = output((2, 1, 3, 0))
    far = to_member(far, 2)
    up, down = to_member(up, 1), to_member(down, 3)
    mixed = (
        mine.astype(jnp.float32)
        + far.astype(jnp.float32)
        + up.astype(jnp.float32)
        + down.astype(jnp.float32)
    )
    return (mixed.astype(jnp.bfloat16), log_sums)


def solution(mesh):
    split = Mesh(mesh.devices.reshape(-1, CORES, mesh.shape["tp"]), ("chip", "core", "tp"))
    in_specs = (
        P(SP, None),
        P(),
        P(SP, "tp"),
        P(SP, "tp"),
        P(SP, "tp"),
        P(SP, "tp"),
        P(SP, "tp"),
        P(None, "tp"),
        P("tp"),
        P("tp"),
        P("tp", SP),
        P("tp", SP),
    )
    out_specs = (P((*SP, "tp"), None), P("tp", SP))
    return jax.shard_map(layer, mesh=split, in_specs=in_specs, out_specs=out_specs, check_vma=False)
```

```python
import functools

import jax
import jax.numpy as jnp
from jax import lax
from jax.experimental import pallas as pl
from jax.experimental.pallas import tpu as pltpu
from jax.sharding import Mesh, PartitionSpec as P

CONV_CH = 2048
HEAD_DIM = 64
WINDOW = 128

NORM_EPS = 1e-06
CHANNEL_EPS = 1e-05
ROPE_BASE = 10000.0

SIDE = 8
CHIPS = SIDE * SIDE
CORES = 2
SP = ("chip", "core")
CHIP = ("core", "tp")


def place(z, y, core):
    return ((z % SIDE) * SIDE + y % SIDE) * CORES + core


def at_line(line, step, core):
    return place(line, step, core) if core == 0 else place(step, line, core)


LINES = [[at_line(i, j, c) for j in range(SIDE)] for c in range(CORES) for i in range(SIDE)]
AHEAD, BEHIND = (
    [
        (at_line(i, j, c), at_line(i + by, j, c))
        for c in range(CORES)
        for i in range(SIDE)
        for j in range(SIDE)
    ]
    for by in (1, -1)
)
OTHER_CORE = [(i, i ^ 1) for i in range(CHIPS * CORES)]
NEXT_CHIP = [(i, i + CORES) for i in range(CHIPS * CORES - CORES)]

VMEM = pl.BlockSpec(memory_space=pltpu.VMEM)
SMEM = pl.BlockSpec(memory_space=pltpu.SMEM)
HBM = pl.BlockSpec(memory_space=pltpu.MemorySpace.HBM)
TILE = 256


def call(body, outs, flops, in_specs, operands, scratch=(), limit=None):
    return pl.pallas_call(
        body,
        out_shape=outs,
        in_specs=in_specs,
        out_specs=jax.tree.map(lambda _: VMEM, outs),
        scratch_shapes=list(scratch),
        compiler_params=pltpu.CompilerParams(vmem_limit_bytes=limit and limit << 20),
        cost_estimate=pl.CostEstimate(flops=flops, bytes_accessed=1 << 20, transcendentals=0),
    )(*operands)


def shape(dims, dtype=jnp.bfloat16):
    return jax.ShapeDtypeStruct(dims, dtype)


def pack_kernel(at_ref, *refs):
    count = (len(refs) - 3) // 2
    shards, held, sems = refs[:count], refs[count + 2 : -1], refs[-1]
    kept_ref, given_ref = refs[count : count + 2]
    copies = [
        pltpu.make_async_copy(shard, here, sems.at[index])
        for index, (shard, here) in enumerate(zip(shards, held))
    ]
    for copy in copies:
        copy.start()
    for copy in copies:
        copy.wait()
    value_ref, gate_ref, query_ref, key_ref, v_ref, conv_ref, attn_ref = held
    core = at_ref[3]
    lane = lax.broadcasted_iota(jnp.int32, key_ref.shape, 1)
    key = key_ref[...].astype(jnp.float32)
    value = v_ref[...].astype(jnp.float32)
    both = (
        jnp.where(lane < HEAD_DIM, key, pltpu.roll(value, HEAD_DIM, 1)),
        jnp.where(lane < HEAD_DIM, pltpu.roll(key, HEAD_DIM, 1), value),
    )
    for half in range(CORES):
        parts = []
        for source in (value_ref, gate_ref, query_ref, None, conv_ref, attn_ref):
            if source is None:
                parts.append(both[half].astype(jnp.bfloat16))
            else:
                width = source.shape[1] // CORES
                parts.append(source[:, half * width : (half + 1) * width])
        whole = jnp.concatenate(parts, axis=1)

        @pl.when(core == half)
        def _():
            kept_ref[...] = whole

        @pl.when(core != half)
        def _():
            given_ref[...] = whole


def repeat_kernel(at_ref, kept_ref, got_ref, out_ref):
    core, rows = at_ref[3], kept_ref.shape[0]
    for source, to_core in ((kept_ref, core), (got_ref, 1 - core)):
        to = pl.ds(pl.multiple_of(to_core * rows, rows), rows)
        for member in range(out_ref.shape[0]):
            out_ref[member, to, :] = source[...]


def norm_kernel(at_ref, own_ref, other_ref, gain_ref, out_ref):
    core = at_ref[3]
    count, model = own_ref.shape
    group = model // CHIPS
    tile = 32
    lane = lax.broadcasted_iota(jnp.int32, (tile, 128), 1)
    gain = gain_ref[...].astype(jnp.float32)

    @pl.loop(0, count // tile)
    def _(step):
        at = pl.multiple_of(step * tile, tile)
        for source, to_core in ((own_ref, core), (other_ref, 1 - core)):
            x = source[pl.ds(at, tile), :].astype(jnp.float32)
            scale = lax.rsqrt(jnp.mean(x * x, axis=-1, keepdims=True) + NORM_EPS)
            normed = x * scale * gain
            rows = pl.ds(pl.multiple_of(to_core * count + at, tile), tile)

            @pl.when(core == 0)
            def _():
                out_ref[rows, :] = normed.astype(jnp.bfloat16)

            @pl.when(core == 1)
            def _():
                for to in range(0, model, 128):
                    y, z = to // group // SIDE, to // group % SIDE
                    out = jnp.zeros((tile, 128), jnp.float32)
                    for part in range(128 // group):
                        start = ((z + part) * SIDE + y) * group
                        tile_at = start // 128 * 128
                        turned = pltpu.roll(
                            normed[:, tile_at : tile_at + 128],
                            (part * group - start % 128) % 128,
                            1,
                        )
                        out = jnp.where(lane // group == part, turned, out)
                    out_ref[rows, to : to + 128] = out.astype(jnp.bfloat16)


def line_of(at_ref, index):
    away = (index + 1) // 2 * (1 if index % 2 == 0 else -1)
    first = SIDE // 2 if index == SIDE else 0
    return jnp.bitwise_and(at_ref[0] + away, SIDE - 1), first


def products(at_ref, x_ref, rows, pieces, first, held_ref):
    parts = []
    for index, piece in enumerate(pieces, first):
        line, step = line_of(at_ref, index)
        block = piece.shape[1]
        size = piece.shape[0] * block
        start = pl.multiple_of(line * (SIDE * block) + step * block, 128)
        parts.append(x_ref[rows, pl.ds(start, size)])
    return jnp.dot(jnp.concatenate(parts, axis=1), held_ref[...], preferred_element_type=jnp.float32)


def hold(pieces, held_ref):
    to = 0
    for piece in pieces:
        for step in range(piece.shape[0]):
            held_ref[to : to + piece.shape[1], :] = piece[step, :, : held_ref.shape[1]]
            to += piece.shape[1]


def rows_of(step):
    return pl.ds(pl.multiple_of(step * TILE, TILE), TILE)


def early_kernel(first, count, at_ref, x_ref, *refs):
    pieces, before, (out_ref, held_ref) = refs[:count], refs[count:-2], refs[-2:]
    hold(pieces, held_ref)

    @pl.loop(0, x_ref.shape[0] // TILE)
    def _(step):
        rows = rows_of(step)
        total = products(at_ref, x_ref, rows, pieces, first, held_ref)
        for other in before:
            total = total + other[rows, :]
        out_ref[rows, :] = total


def late_kernel(
    first, at_ref, x_ref, cos_ref, sin_ref, before_ref, a_ref, b_ref, glu_ref, qkv_ref, tail_ref, held_ref
):
    pieces = (a_ref, b_ref)
    hold(pieces, held_ref)
    channels, width = glu_ref.shape[1], qkv_ref.shape[1]

    @pl.loop(0, x_ref.shape[0] // TILE)
    def _(step):
        rows = rows_of(step)
        total = products(at_ref, x_ref, rows, pieces, first, held_ref) + before_ref[rows, :]
        raw = total.astype(jnp.bfloat16).astype(jnp.float32)
        value, gate = raw[:, :channels], raw[:, channels : 2 * channels]
        glu_ref[rows, :] = (value * jax.nn.sigmoid(gate)).astype(jnp.bfloat16)
        lane = lax.broadcasted_iota(jnp.int32, (TILE, 128), 1)
        front = jnp.bitwise_and(lane, HEAD_DIM - 1) < HEAD_DIM // 2
        cosine, sine = cos_ref[rows, :], sin_ref[rows, :]
        for at in range(0, width, 128):
            part = raw[:, 2 * channels + at : 2 * channels + at + 128]
            other = jnp.where(
                front,
                pltpu.roll(part, 128 - HEAD_DIM // 2, 1),
                pltpu.roll(part, HEAD_DIM // 2, 1),
            )
            turned = part * cosine + other * sine
            if at + 128 == width:
                turned = jnp.where(lane < HEAD_DIM, turned, part)
            qkv_ref[rows, at : at + 128] = turned.astype(jnp.bfloat16)

    end = x_ref.shape[0]
    tail_ref[0:WINDOW, :] = qkv_ref[end - WINDOW : end, width - 128 : width]
    tail_ref[WINDOW : WINDOW + 32, :] = glu_ref[end - 32 : end, :128]
    tail_ref[WINDOW + 32 : WINDOW + 64, :] = glu_ref[end - 32 : end, 128:]


def join_kernel(column, at_ref, *refs):
    pieces, out_ref = refs[:-1], refs[-1]
    for index, piece in enumerate(pieces):
        line, first = line_of(at_ref, index)
        block = piece.shape[1]
        for step in range(piece.shape[0]):
            to = pl.multiple_of(line * (SIDE * block) + (first + step) * block, block)
            out_ref[pl.ds(to, block), :] = piece[step, :, column:]


def conv_kernel(before_ref, glu_ref, taps_ref, out_ref, sums_ref, ext_ref):
    count, rows = taps_ref.shape[0], glu_ref.shape[0]
    lead = 32
    for part in range(2):
        lanes = pl.ds(part * 128, 128)
        held = pl.ds(WINDOW + part * lead, lead)
        ext_ref[part, pl.ds(0, lead), :] = before_ref[held, :].astype(jnp.float32)
        ext_ref[part, pl.ds(lead, rows), :] = glu_ref[:, lanes].astype(jnp.float32)

    @pl.loop(0, rows // 128)
    def _(step):
        base = pl.multiple_of(step * 128, 128)
        first = jnp.zeros((128, 128), jnp.float32)
        second = jnp.zeros((128, 128), jnp.float32)
        for part in range(2):
            lanes = pl.ds(part * 128, 128)
            total = jnp.zeros((128, 128), jnp.float32)
            for tap in range(count):
                rows_at = pl.ds(base + (lead - count + 1 + tap), 128)
                total = total + taps_ref[pl.ds(tap, 1), lanes] * ext_ref[part, rows_at, :]
            out_ref[pl.ds(base, 128), lanes] = total
            first = first + total
            second = second + total * total
        first = jnp.sum(first.T, axis=0, keepdims=True)
        second = jnp.sum(second.T, axis=0, keepdims=True)
        for member in range(sums_ref.shape[0]):
            sums_ref[member, pl.ds(0, 1), pl.ds(base, 128)] = first
            sums_ref[member, pl.ds(1, 1), pl.ds(base, 128)] = second


def scaled_kernel(at_ref, conv_ref, sums_ref, gain_ref, attn_ref, kept_ref, given_ref):
    core = at_ref[3]
    totals = sums_ref[0]
    for member in range(1, sums_ref.shape[0]):
        totals = totals + sums_ref[member]
    mean = totals[0:1] / CONV_CH
    scale = lax.rsqrt(totals[1:2] / CONV_CH - mean * mean + CHANNEL_EPS)
    half, channels = kept_ref.shape
    given_ref[:, channels:] = attn_ref[...]
    for base in range(0, conv_ref.shape[0], 128):
        at = slice(base, base + 128)
        mean_at = jnp.broadcast_to(mean[:, at], (128, 128)).T
        scale_at = jnp.broadcast_to(scale[:, at], (128, 128)).T
        parts = []
        for lanes in (slice(0, 128), slice(128, 256)):
            normed = (conv_ref[at, lanes] - mean_at) * scale_at * gain_ref[0:1, lanes]
            parts.append((normed * jax.nn.sigmoid(normed)).astype(jnp.bfloat16))
        out = jnp.concatenate(parts, axis=1)
        to = slice(base % half, base % half + 128)

        @pl.when(core == base // half)
        def _():
            kept_ref[to, :] = out

        @pl.when(core != base // half)
        def _():
            given_ref[to, :channels] = out


def attention_kernel(
    at_ref, sinks_ref, qkv_ref, before_ref, kept_ref, given_ref, logs_ref, k_lo, k_hi, v_lo, v_hi
):
    core, first_chip = at_ref[3], at_ref[4]
    cols = kept_ref.shape[1]
    for source, to, count in ((before_ref, 0, WINDOW), (qkv_ref, WINDOW, qkv_ref.shape[0])):
        both = source[:count, source.shape[1] - 128 :].astype(jnp.float32)
        low = lax.broadcasted_iota(jnp.int32, both.shape, 1) < HEAD_DIM
        turned = pltpu.roll(both, HEAD_DIM, 1)
        rows = slice(to, to + both.shape[0])
        k_lo[rows, :] = jnp.where(low, both, 0.0).astype(jnp.bfloat16)
        k_hi[rows, :] = jnp.where(low, 0.0, turned).astype(jnp.bfloat16)
        v_lo[rows, :] = jnp.where(low, turned, 0.0).astype(jnp.bfloat16)
        v_hi[rows, :] = jnp.where(low, 0.0, both).astype(jnp.bfloat16)
    blocks = qkv_ref.shape[0] // WINDOW
    half_blocks = blocks // CORES
    heads = cols // HEAD_DIM

    @pl.loop(0, blocks)
    def _(block):
        base = pl.multiple_of(block * WINDOW, WINDOW)
        window = pl.ds(base, 2 * WINDOW)
        key_at = lax.broadcasted_iota(jnp.int32, (2 * WINDOW, WINDOW), 0)
        query_at = lax.broadcasted_iota(jnp.int32, (2 * WINDOW, WINDOW), 1)
        lowest = jnp.where((first_chip == 1) & (block == 0), WINDOW, 0)
        allowed = (key_at > query_at) & (key_at <= query_at + WINDOW) & (key_at >= lowest)
        outs = []
        for pair in range(heads // 2):
            query = qkv_ref[pl.ds(base, WINDOW), pair * 128 : (pair + 1) * 128]
            total = jnp.zeros((WINDOW, 128), jnp.float32)
            for which, (keys, values) in enumerate(((k_lo, v_lo), (k_hi, v_hi))):
                head = 2 * pair + which
                scores = (
                    lax.dot_general(
                        keys[window, :],
                        query,
                        (((1,), (1,)), ((), ())),
                        preferred_element_type=jnp.float32,
                    )
                    * HEAD_DIM ** (-0.5)
                )
                sums = jnp.sum(jnp.where(allowed, jnp.exp(scores), 0.0), axis=0, keepdims=True)
                sink = jnp.full((1, WINDOW), sinks_ref[core * heads + head], jnp.float32)
                log_total = jnp.log(sums + jnp.exp(sink))
                logs_ref[pl.ds(head, 1), pl.ds(base, WINDOW)] = log_total
                weights = jnp.where(allowed, jnp.exp(scores - log_total), 0.0).astype(jnp.bfloat16)
                total = total + lax.dot_general(
                    weights,
                    values[window, :],
                    (((0,), (0,)), ((), ())),
                    preferred_element_type=jnp.float32,
                )
            outs.append(total.astype(jnp.bfloat16))
        out = jnp.concatenate(outs, axis=1)
        own = block // half_blocks == core
        to = pl.ds(pl.multiple_of((block % half_blocks) * WINDOW, WINDOW), WINDOW)

        @pl.when(own)
        def _():
            kept_ref[to, :] = out

        @pl.when(jnp.logical_not(own))
        def _():
            given_ref[to, :] = out


def output_kernel(
    steps, at_ref, conv_ref, attn_ref, got_ref, own_ref, other_ref, *rest
):
    out_refs, w_ref = rest[:-1], rest[-1]
    core, member, half = at_ref[3], at_ref[5], conv_ref.shape[1]
    count = out_refs[0].shape[0]
    peers = conv_ref.shape[0] // count
    block = own_ref.shape[0] // CHIPS
    width = own_ref.shape[1]

    @pl.loop(0, SIDE)
    def _(z):
        cols = pl.ds(pl.multiple_of(z * SIDE * block, TILE), SIDE * block)
        by_z, by_y = z * SIDE * block, z * block
        for source, at, along_z in ((own_ref, 0, core == 0), (other_ref, width, core == 1)):
            first = jnp.where(along_z, by_z, by_y)
            stride = jnp.where(along_z, block, SIDE * block)
            for y in range(SIDE):
                start = pl.multiple_of(first + y * stride, block)
                w_ref[y * block : (y + 1) * block, at : at + width] = source[pl.ds(start, block), :]
        total = jnp.zeros((conv_ref.shape[0], SIDE * block), jnp.float32)
        for left, at in ((conv_ref, 0), (attn_ref, half), (got_ref, width)):
            total = total + lax.dot_general(
                left[...],
                w_ref[:, at : at + left.shape[1]],
                (((1,), (1,)), ((), ())),
                preferred_element_type=jnp.float32,
            )
        for to in range(peers):
            out = total[to * count : (to + 1) * count].astype(jnp.bfloat16)
            for away, out_ref in zip(steps, out_refs):

                @pl.when(jnp.bitwise_and(to - member, peers - 1) == away)
                def _():
                    out_ref[:, cols] = out


def layer(
    tokens,
    norm_gain,
    w_conv_value,
    w_conv_gate,
    w_query,
    w_key,
    w_value,
    conv_taps,
    ln_gain,
    sinks,
    out_conv,
    out_attn,
):
    core = lax.axis_index("core")
    chip = lax.axis_index("chip")
    member = lax.axis_index("tp")
    own_rows, model = tokens.shape
    row_count = own_rows * CORES
    depth = w_conv_value.shape[0]
    channels = w_conv_value.shape[1] // CORES
    q_cols = w_query.shape[1] // CORES
    query_heads = q_cols // HEAD_DIM
    block = CORES * depth

    z, y = chip // SIDE, chip % SIDE
    at = jnp.stack(
        [
            jnp.where(core == 0, z, y),
            jnp.where(core == 0, SIDE * block, block),
            jnp.where(core == 0, block, SIDE * block),
            core,
            (chip == 0).astype(jnp.int32),
            member,
        ]
    ).astype(jnp.int32)

    conv_cols = (0, 2 * channels)
    qkv_cols = (2 * channels, q_cols + 2 * HEAD_DIM)
    out_cols = (2 * channels + q_cols + 2 * HEAD_DIM, channels + q_cols)
    width = sum(out_cols)
    shards_in = (w_conv_value, w_conv_gate, w_query, w_key, w_value, out_conv.T, out_attn.T)
    kept, given = call(
        pack_kernel,
        (shape((depth, width)),) * 2,
        1 << 20,
        [SMEM] + [HBM] * len(shards_in),
        (at, *shards_in),
        (
            *(pltpu.VMEM(w.shape, w.dtype) for w in shards_in),
            pltpu.SemaphoreType.DMA((len(shards_in),)),
        ),
    )
    got = lax.ppermute(given, SP, OTHER_CORE)
    sent = call(
        repeat_kernel,
        shape((SIDE, block, width)),
        1 << 20,
        [SMEM, VMEM, VMEM],
        (at, kept, got),
        limit=12,
    )
    own_line = lax.all_to_all(sent, SP, 0, 0, tiled=True, axis_index_groups=LINES)
    pieces = [own_line]
    ahead = behind = own_line
    for step in range(SIDE // 2):
        if step == SIDE // 2 - 1:
            ahead, behind = ahead[: SIDE // 2], behind[SIDE // 2 :]
        ahead = lax.ppermute(ahead, SP, AHEAD)
        behind = lax.ppermute(behind, SP, BEHIND)
        pieces += [ahead, behind]

    tokens_other = lax.ppermute(tokens, SP, OTHER_CORE)
    normed = call(
        norm_kernel,
        shape((row_count, model)),
        1 << 30,
        [SMEM, VMEM, VMEM, VMEM],
        (at, tokens, tokens_other, norm_gain[None]),
        limit=16,
    )

    positions = chip * row_count + jnp.arange(row_count, dtype=jnp.int32)
    half_dim = HEAD_DIM // 2
    inverse = ROPE_BASE ** (-jnp.arange(half_dim, dtype=jnp.float32) / half_dim)
    angles = positions.astype(jnp.float32)[:, None] * inverse[None, :]
    cosine, sine = jnp.cos(angles), jnp.sin(angles)
    cosines = jnp.concatenate([cosine] * 4, axis=1)
    sines = jnp.concatenate([-sine, sine] * 2, axis=1)

    in_cols = conv_cols[1] + qkv_cols[1]
    lines = SIDE * block

    def early(first, last, before):
        held = pieces[first:last]
        return call(
            functools.partial(early_kernel, first, len(held)),
            shape((row_count, in_cols), jnp.float32),
            2 * row_count * lines * len(held) * in_cols,
            [SMEM] + [VMEM] * (1 + len(held) + len(before)),
            (at, normed, *held, *before),
            (pltpu.VMEM((lines * len(held), in_cols), jnp.bfloat16),),
            limit=16,
        )

    total = early(0, 5, ())
    total = early(5, 7, (total,))
    glu, qkv, tail = call(
        functools.partial(late_kernel, 7),
        (shape((row_count, channels)), shape((row_count, qkv_cols[1])), shape((WINDOW + 64, 128))),
        2 * row_count * lines * in_cols,
        [SMEM] + [VMEM] * 6,
        (at, normed, cosines, sines, total, *pieces[7:]),
        (pltpu.VMEM((lines, in_cols), jnp.bfloat16),),
        limit=16,
    )
    before = lax.ppermute(tail, SP, NEXT_CHIP)
    out_own = call(
        functools.partial(join_kernel, out_cols[0]),
        shape((model, out_cols[1])),
        1 << 28,
        [SMEM] + [VMEM] * len(pieces),
        (at, *pieces),
        limit=12,
    )
    out_other = lax.ppermute(out_own, SP, OTHER_CORE)

    taps = lax.dynamic_slice_in_dim(conv_taps, core * channels, channels, 1)
    members = CORES * lax.axis_size("tp")
    conv_out, sums = call(
        conv_kernel,
        (shape((row_count, channels), jnp.float32), shape((members, 2, row_count), jnp.float32)),
        1 << 32,
        [VMEM] * 3,
        (before, glu, taps),
        (pltpu.VMEM((2, row_count + 32, 128), jnp.float32),),
        limit=12,
    )
    everyones = lax.all_to_all(sums, CHIP, 0, 0, tiled=True)
    extended = pltpu.VMEM((row_count + WINDOW, 128), jnp.bfloat16)
    attn_kept, attn_given, log_rows = call(
        attention_kernel,
        (
            shape((own_rows, q_cols)),
            shape((own_rows, q_cols)),
            shape((query_heads, row_count), jnp.float32),
        ),
        1 << 32,
        [SMEM, SMEM, VMEM, VMEM],
        (at, sinks, qkv, before),
        (extended,) * 4,
        limit=12,
    )
    gain = lax.dynamic_slice_in_dim(ln_gain, core * channels, channels, 0)
    conv_kept, given = call(
        scaled_kernel,
        (shape((own_rows, channels)), shape((own_rows, channels + q_cols))),
        1 << 28,
        [SMEM] + [VMEM] * 4,
        (at, conv_out, everyones, gain[None], attn_given),
        limit=12,
    )
    rows_got = lax.ppermute(given, SP, OTHER_CORE)

    kept = lax.dynamic_slice_in_dim(log_rows, core * own_rows, own_rows, 1)
    given = lax.dynamic_slice_in_dim(log_rows, (1 - core) * own_rows, own_rows, 1)
    logs_got = lax.ppermute(given, SP, OTHER_CORE)
    log_sums = jnp.where(
        core == 0,
        jnp.concatenate([kept, logs_got], axis=0),
        jnp.concatenate([logs_got, kept], axis=0),
    )

    peers = lax.axis_size("tp")
    share = own_rows // peers

    def output(steps):
        return call(
            functools.partial(output_kernel, steps),
            (shape((share, model)),) * len(steps),
            2 * share * len(steps) * model * 2 * out_cols[1],
            [SMEM] + [VMEM] * 5,
            (at, conv_kept, attn_kept, rows_got, out_own, out_other),
            (pltpu.VMEM((TILE, 2 * out_cols[1]), jnp.bfloat16),),
            limit=16,
        )

    def to_member(value, away):
        return lax.ppermute(value, "tp", [(i, (i + away) % peers) for i in range(peers)])

    far, up, down, mine = output((2, 1, 3, 0))
    far = to_member(far, 2)
    up, down = to_member(up, 1), to_member(down, 3)
    mixed = (
        mine.astype(jnp.float32)
        + far.astype(jnp.float32)
        + up.astype(jnp.float32)
        + down.astype(jnp.float32)
    )
    return (mixed.astype(jnp.bfloat16), log_sums)


def solution(mesh):
    split = Mesh(mesh.devices.reshape(-1, CORES, mesh.shape["tp"]), ("chip", "core", "tp"))
    in_specs = (
        P(SP, None),
        P(),
        P(SP, "tp"),
        P(SP, "tp"),
        P(SP, "tp"),
        P(SP, "tp"),
        P(SP, "tp"),
        P(None, "tp"),
        P("tp"),
        P("tp"),
        P("tp", SP),
        P("tp", SP),
    )
    out_specs = (P((*SP, "tp"), None), P("tp", SP))
    return jax.shard_map(layer, mesh=split, in_specs=in_specs, out_specs=out_specs, check_vma=False)
```

```python
import functools

import jax
import jax.numpy as jnp
from jax import lax
from jax.experimental import pallas as pl
from jax.experimental.pallas import tpu as pltpu
from jax.sharding import Mesh, PartitionSpec as P

CONV_CH = 2048
HEAD_DIM = 64
WINDOW = 128

NORM_EPS = 1e-06
CHANNEL_EPS = 1e-05
ROPE_BASE = 10000.0

SIDE = 8
CHIPS = SIDE * SIDE
CORES = 2
SP = ("chip", "core")
CHIP = ("core", "tp")


def place(z, y, core):
    return ((z % SIDE) * SIDE + y % SIDE) * CORES + core


def at_line(line, step, core):
    return place(line, step, core) if core == 0 else place(step, line, core)


LINES = [[at_line(i, j, c) for j in range(SIDE)] for c in range(CORES) for i in range(SIDE)]
AHEAD, BEHIND = (
    [
        (at_line(i, j, c), at_line(i + by, j, c))
        for c in range(CORES)
        for i in range(SIDE)
        for j in range(SIDE)
    ]
    for by in (1, -1)
)
OTHER_CORE = [(i, i ^ 1) for i in range(CHIPS * CORES)]
NEXT_CHIP = [(i, i + CORES) for i in range(CHIPS * CORES - CORES)]

VMEM = pl.BlockSpec(memory_space=pltpu.VMEM)
SMEM = pl.BlockSpec(memory_space=pltpu.SMEM)
HBM = pl.BlockSpec(memory_space=pltpu.MemorySpace.HBM)
TILE = 256


def call(body, outs, flops, in_specs, operands, scratch=(), limit=None):
    return pl.pallas_call(
        body,
        out_shape=outs,
        in_specs=in_specs,
        out_specs=jax.tree.map(lambda _: VMEM, outs),
        scratch_shapes=list(scratch),
        compiler_params=pltpu.CompilerParams(vmem_limit_bytes=limit and limit << 20),
        cost_estimate=pl.CostEstimate(flops=flops, bytes_accessed=1 << 20, transcendentals=0),
    )(*operands)


def shape(dims, dtype=jnp.bfloat16):
    return jax.ShapeDtypeStruct(dims, dtype)


def pack_kernel(*refs):
    count = (len(refs) - 3) // 2
    shards, held, sems = refs[:count], refs[count + 2 : -1], refs[-1]
    kept_ref, given_ref = refs[count : count + 2]
    copies = [
        pltpu.make_async_copy(shard, here, sems.at[index])
        for index, (shard, here) in enumerate(zip(shards, held))
    ]
    for copy in copies:
        copy.start()
    for copy in copies:
        copy.wait()
    value_ref, gate_ref, query_ref, key_ref, v_ref, conv_ref, attn_ref = held
    core = lax.axis_index("core")
    lane = lax.broadcasted_iota(jnp.int32, key_ref.shape, 1)
    key = key_ref[...].astype(jnp.float32)
    value = v_ref[...].astype(jnp.float32)
    both = (
        jnp.where(lane < HEAD_DIM, key, pltpu.roll(value, HEAD_DIM, 1)),
        jnp.where(lane < HEAD_DIM, pltpu.roll(key, HEAD_DIM, 1), value),
    )
    for half in range(CORES):
        parts = []
        for source in (value_ref, gate_ref, query_ref, None, conv_ref, attn_ref):
            if source is None:
                parts.append(both[half].astype(jnp.bfloat16))
            else:
                width = source.shape[1] // CORES
                parts.append(source[:, half * width : (half + 1) * width])
        whole = jnp.concatenate(parts, axis=1)

        @pl.when(core == half)
        def _():
            kept_ref[...] = whole

        @pl.when(core != half)
        def _():
            given_ref[...] = whole


def repeat_kernel(kept_ref, got_ref, out_ref):
    core, rows = lax.axis_index("core"), kept_ref.shape[0]
    for source, to_core in ((kept_ref, core), (got_ref, 1 - core)):
        to = pl.ds(pl.multiple_of(to_core * rows, rows), rows)
        for member in range(out_ref.shape[0]):
            out_ref[member, to, :] = source[...]


def norm_kernel(own_ref, other_ref, gain_ref, out_ref):
    core = lax.axis_index("core")
    count, model = own_ref.shape
    group = model // CHIPS
    tile = 32
    lane = lax.broadcasted_iota(jnp.int32, (tile, 128), 1)
    gain = gain_ref[...].astype(jnp.float32)

    @pl.loop(0, count // tile)
    def _(step):
        at = pl.multiple_of(step * tile, tile)
        for source, to_core in ((own_ref, core), (other_ref, 1 - core)):
            x = source[pl.ds(at, tile), :].astype(jnp.float32)
            scale = lax.rsqrt(jnp.mean(x * x, axis=-1, keepdims=True) + NORM_EPS)
            normed = x * scale * gain
            rows = pl.ds(pl.multiple_of(to_core * count + at, tile), tile)

            @pl.when(core == 0)
            def _():
                out_ref[rows, :] = normed.astype(jnp.bfloat16)

            @pl.when(core == 1)
            def _():
                for to in range(0, model, 128):
                    y, z = to // group // SIDE, to // group % SIDE
                    out = jnp.zeros((tile, 128), jnp.float32)
                    for part in range(128 // group):
                        start = ((z + part) * SIDE + y) * group
                        tile_at = start // 128 * 128
                        turned = pltpu.roll(
                            normed[:, tile_at : tile_at + 128],
                            (part * group - start % 128) % 128,
                            1,
                        )
                        out = jnp.where(lane // group == part, turned, out)
                    out_ref[rows, to : to + 128] = out.astype(jnp.bfloat16)


def line_of(index):
    away = (index + 1) // 2 * (1 if index % 2 == 0 else -1)
    first = SIDE // 2 if index == SIDE else 0
    chip = lax.axis_index("chip")
    line = jnp.where(lax.axis_index("core") == 0, chip // SIDE, chip % SIDE)
    return jnp.bitwise_and(line + away, SIDE - 1), first


def products(x_ref, rows, pieces, first, held_ref):
    parts = []
    for index, piece in enumerate(pieces, first):
        line, step = line_of(index)
        block = piece.shape[1]
        size = piece.shape[0] * block
        start = pl.multiple_of(line * (SIDE * block) + step * block, 128)
        parts.append(x_ref[rows, pl.ds(start, size)])
    return jnp.dot(jnp.concatenate(parts, axis=1), held_ref[...], preferred_element_type=jnp.float32)


def hold(pieces, held_ref):
    to = 0
    for piece in pieces:
        for step in range(piece.shape[0]):
            held_ref[to : to + piece.shape[1], :] = piece[step, :, : held_ref.shape[1]]
            to += piece.shape[1]


def rows_of(step):
    return pl.ds(pl.multiple_of(step * TILE, TILE), TILE)


def early_kernel(first, count, x_ref, *refs):
    pieces, before, (out_ref, held_ref) = refs[:count], refs[count:-2], refs[-2:]
    hold(pieces, held_ref)

    @pl.loop(0, x_ref.shape[0] // TILE)
    def _(step):
        rows = rows_of(step)
        total = products(x_ref, rows, pieces, first, held_ref)
        for other in before:
            total = total + other[rows, :]
        out_ref[rows, :] = total


def late_kernel(
    first, x_ref, cos_ref, sin_ref, before_ref, a_ref, b_ref, glu_ref, qkv_ref, tail_ref, held_ref
):
    pieces = (a_ref, b_ref)
    hold(pieces, held_ref)
    channels, width = glu_ref.shape[1], qkv_ref.shape[1]

    @pl.loop(0, x_ref.shape[0] // TILE)
    def _(step):
        rows = rows_of(step)
        total = products(x_ref, rows, pieces, first, held_ref) + before_ref[rows, :]
        raw = total.astype(jnp.bfloat16).astype(jnp.float32)
        value, gate = raw[:, :channels], raw[:, channels : 2 * channels]
        glu_ref[rows, :] = (value * jax.nn.sigmoid(gate)).astype(jnp.bfloat16)
        lane = lax.broadcasted_iota(jnp.int32, (TILE, 128), 1)
        front = jnp.bitwise_and(lane, HEAD_DIM - 1) < HEAD_DIM // 2
        cosine, sine = cos_ref[rows, :], sin_ref[rows, :]
        for at in range(0, width, 128):
            part = raw[:, 2 * channels + at : 2 * channels + at + 128]
            other = jnp.where(
                front,
                pltpu.roll(part, 128 - HEAD_DIM // 2, 1),
                pltpu.roll(part, HEAD_DIM // 2, 1),
            )
            turned = part * cosine + other * sine
            if at + 128 == width:
                turned = jnp.where(lane < HEAD_DIM, turned, part)
            qkv_ref[rows, at : at + 128] = turned.astype(jnp.bfloat16)

    end = x_ref.shape[0]
    tail_ref[0:WINDOW, :] = qkv_ref[end - WINDOW : end, width - 128 : width]
    tail_ref[WINDOW : WINDOW + 32, :] = glu_ref[end - 32 : end, :128]
    tail_ref[WINDOW + 32 : WINDOW + 64, :] = glu_ref[end - 32 : end, 128:]


def join_kernel(column, *refs):
    pieces, out_ref = refs[:-1], refs[-1]
    for index, piece in enumerate(pieces):
        line, first = line_of(index)
        block = piece.shape[1]
        for step in range(piece.shape[0]):
            to = pl.multiple_of(line * (SIDE * block) + (first + step) * block, block)
            out_ref[pl.ds(to, block), :] = piece[step, :, column:]


def conv_kernel(before_ref, glu_ref, taps_ref, out_ref, sums_ref, ext_ref):
    count, (rows, channels) = taps_ref.shape[0], glu_ref.shape
    first_channel = lax.axis_index("core") * channels
    lead = 32
    for part in range(2):
        lanes = pl.ds(part * 128, 128)
        held = pl.ds(WINDOW + part * lead, lead)
        ext_ref[part, pl.ds(0, lead), :] = before_ref[held, :].astype(jnp.float32)
        ext_ref[part, pl.ds(lead, rows), :] = glu_ref[:, lanes].astype(jnp.float32)

    @pl.loop(0, rows // 128)
    def _(step):
        base = pl.multiple_of(step * 128, 128)
        first = jnp.zeros((128, 128), jnp.float32)
        second = jnp.zeros((128, 128), jnp.float32)
        for part in range(2):
            lanes = pl.ds(part * 128, 128)
            own = pl.ds(pl.multiple_of(first_channel + part * 128, 128), 128)
            total = jnp.zeros((128, 128), jnp.float32)
            for tap in range(count):
                rows_at = pl.ds(base + (lead - count + 1 + tap), 128)
                total = total + taps_ref[pl.ds(tap, 1), own] * ext_ref[part, rows_at, :]
            out_ref[pl.ds(base, 128), lanes] = total
            first = first + total
            second = second + total * total
        first = jnp.sum(first.T, axis=0, keepdims=True)
        second = jnp.sum(second.T, axis=0, keepdims=True)
        for member in range(sums_ref.shape[0]):
            sums_ref[member, pl.ds(0, 1), pl.ds(base, 128)] = first
            sums_ref[member, pl.ds(1, 1), pl.ds(base, 128)] = second


def scaled_kernel(conv_ref, sums_ref, gain_ref, attn_ref, kept_ref, given_ref):
    core = lax.axis_index("core")
    totals = sums_ref[0]
    for member in range(1, sums_ref.shape[0]):
        totals = totals + sums_ref[member]
    mean = totals[0:1] / CONV_CH
    scale = lax.rsqrt(totals[1:2] / CONV_CH - mean * mean + CHANNEL_EPS)
    half, channels = kept_ref.shape
    given_ref[:, channels:] = attn_ref[...]
    for base in range(0, conv_ref.shape[0], 128):
        at = slice(base, base + 128)
        mean_at = jnp.broadcast_to(mean[:, at], (128, 128)).T
        scale_at = jnp.broadcast_to(scale[:, at], (128, 128)).T
        parts = []
        for lane in range(0, channels, 128):
            own = pl.ds(pl.multiple_of(core * channels + lane, 128), 128)
            normed = (conv_ref[at, lane : lane + 128] - mean_at) * scale_at * gain_ref[0:1, own]
            parts.append((normed * jax.nn.sigmoid(normed)).astype(jnp.bfloat16))
        out = jnp.concatenate(parts, axis=1)
        to = slice(base % half, base % half + 128)

        @pl.when(core == base // half)
        def _():
            kept_ref[to, :] = out

        @pl.when(core != base // half)
        def _():
            given_ref[to, :channels] = out


def attention_kernel(
    sinks_ref, qkv_ref, before_ref, kept_ref, given_ref, logs_ref, k_lo, k_hi, v_lo, v_hi
):
    core, chip = lax.axis_index("core"), lax.axis_index("chip")
    cols = kept_ref.shape[1]
    for source, to, count in ((before_ref, 0, WINDOW), (qkv_ref, WINDOW, qkv_ref.shape[0])):
        both = source[:count, source.shape[1] - 128 :].astype(jnp.float32)
        low = lax.broadcasted_iota(jnp.int32, both.shape, 1) < HEAD_DIM
        turned = pltpu.roll(both, HEAD_DIM, 1)
        rows = slice(to, to + both.shape[0])
        k_lo[rows, :] = jnp.where(low, both, 0.0).astype(jnp.bfloat16)
        k_hi[rows, :] = jnp.where(low, 0.0, turned).astype(jnp.bfloat16)
        v_lo[rows, :] = jnp.where(low, turned, 0.0).astype(jnp.bfloat16)
        v_hi[rows, :] = jnp.where(low, 0.0, both).astype(jnp.bfloat16)
    blocks = qkv_ref.shape[0] // WINDOW
    half_blocks = blocks // CORES
    heads = cols // HEAD_DIM

    @pl.loop(0, blocks)
    def _(block):
        base = pl.multiple_of(block * WINDOW, WINDOW)
        window = pl.ds(base, 2 * WINDOW)
        key_at = lax.broadcasted_iota(jnp.int32, (2 * WINDOW, WINDOW), 0)
        query_at = lax.broadcasted_iota(jnp.int32, (2 * WINDOW, WINDOW), 1)
        lowest = jnp.where((chip == 0) & (block == 0), WINDOW, 0)
        allowed = (key_at > query_at) & (key_at <= query_at + WINDOW) & (key_at >= lowest)
        outs = []
        for pair in range(heads // 2):
            query = qkv_ref[pl.ds(base, WINDOW), pair * 128 : (pair + 1) * 128]
            total = jnp.zeros((WINDOW, 128), jnp.float32)
            for which, (keys, values) in enumerate(((k_lo, v_lo), (k_hi, v_hi))):
                head = 2 * pair + which
                scores = (
                    lax.dot_general(
                        keys[window, :],
                        query,
                        (((1,), (1,)), ((), ())),
                        preferred_element_type=jnp.float32,
                    )
                    * HEAD_DIM ** (-0.5)
                )
                sums = jnp.sum(jnp.where(allowed, jnp.exp(scores), 0.0), axis=0, keepdims=True)
                sink = jnp.full((1, WINDOW), sinks_ref[core * heads + head], jnp.float32)
                log_total = jnp.log(sums + jnp.exp(sink))
                logs_ref[pl.ds(head, 1), pl.ds(base, WINDOW)] = log_total
                weights = jnp.where(allowed, jnp.exp(scores - log_total), 0.0).astype(jnp.bfloat16)
                total = total + lax.dot_general(
                    weights,
                    values[window, :],
                    (((0,), (0,)), ((), ())),
                    preferred_element_type=jnp.float32,
                )
            outs.append(total.astype(jnp.bfloat16))
        out = jnp.concatenate(outs, axis=1)
        own = block // half_blocks == core
        to = pl.ds(pl.multiple_of((block % half_blocks) * WINDOW, WINDOW), WINDOW)

        @pl.when(own)
        def _():
            kept_ref[to, :] = out

        @pl.when(jnp.logical_not(own))
        def _():
            given_ref[to, :] = out


def output_kernel(steps, conv_ref, attn_ref, got_ref, own_ref, other_ref, *rest):
    out_refs, (x_ref, w_ref) = rest[:-2], rest[-2:]
    core, member = lax.axis_index("core"), lax.axis_index("tp")
    count = out_refs[0].shape[0]
    peers = conv_ref.shape[0] // count
    block = own_ref.shape[0] // CHIPS
    width = own_ref.shape[1]
    for index, away in enumerate(steps):
        to = jnp.bitwise_and(member + away, peers - 1)
        rows = pl.ds(pl.multiple_of(to * count, count), count)
        x_ref[index * count : (index + 1) * count, :] = jnp.concatenate(
            [conv_ref[rows, :], attn_ref[rows, :], got_ref[rows, :]], axis=1
        )

    @pl.loop(0, SIDE)
    def _(z):
        cols = pl.ds(pl.multiple_of(z * SIDE * block, TILE), SIDE * block)
        by_z, by_y = z * SIDE * block, z * block
        for source, at, along_z in ((own_ref, 0, core == 0), (other_ref, width, core == 1)):
            first = jnp.where(along_z, by_z, by_y)
            stride = jnp.where(along_z, block, SIDE * block)
            for y in range(SIDE):
                start = pl.multiple_of(first + y * stride, block)
                w_ref[y * block : (y + 1) * block, at : at + width] = source[pl.ds(start, block), :]
        total = lax.dot_general(
            x_ref[...], w_ref[...], (((1,), (1,)), ((), ())), preferred_element_type=jnp.float32
        )
        for index, out_ref in enumerate(out_refs):
            out_ref[:, cols] = total[index * count : (index + 1) * count].astype(jnp.bfloat16)


def layer(
    tokens,
    norm_gain,
    w_conv_value,
    w_conv_gate,
    w_query,
    w_key,
    w_value,
    conv_taps,
    ln_gain,
    sinks,
    out_conv,
    out_attn,
):
    core = lax.axis_index("core")
    chip = lax.axis_index("chip")
    own_rows, model = tokens.shape
    row_count = own_rows * CORES
    depth = w_conv_value.shape[0]
    channels = w_conv_value.shape[1] // CORES
    q_cols = w_query.shape[1] // CORES
    query_heads = q_cols // HEAD_DIM
    block = CORES * depth

    conv_cols = (0, 2 * channels)
    qkv_cols = (2 * channels, q_cols + 2 * HEAD_DIM)
    out_cols = (2 * channels + q_cols + 2 * HEAD_DIM, channels + q_cols)
    width = sum(out_cols)
    shards_in = (w_conv_value, w_conv_gate, w_query, w_key, w_value, out_conv.T, out_attn.T)
    kept, given = call(
        pack_kernel,
        (shape((depth, width)),) * 2,
        1 << 20,
        [HBM] * len(shards_in),
        shards_in,
        (
            *(pltpu.VMEM(w.shape, w.dtype) for w in shards_in),
            pltpu.SemaphoreType.DMA((len(shards_in),)),
        ),
    )
    got = lax.ppermute(given, SP, OTHER_CORE)
    sent = call(repeat_kernel, shape((SIDE, block, width)), 1 << 20, [VMEM, VMEM], (kept, got))
    own_line = lax.all_to_all(sent, SP, 0, 0, tiled=True, axis_index_groups=LINES)
    pieces = [own_line]
    ahead = behind = own_line
    for step in range(SIDE // 2):
        if step == SIDE // 2 - 1:
            ahead, behind = ahead[: SIDE // 2], behind[SIDE // 2 :]
        ahead = lax.ppermute(ahead, SP, AHEAD)
        behind = lax.ppermute(behind, SP, BEHIND)
        pieces += [ahead, behind]

    tokens_other = lax.ppermute(tokens, SP, OTHER_CORE)
    normed = call(
        norm_kernel,
        shape((row_count, model)),
        1 << 30,
        [VMEM, VMEM, VMEM],
        (tokens, tokens_other, norm_gain[None]),
        limit=16,
    )

    positions = chip * row_count + jnp.arange(row_count, dtype=jnp.int32)
    half_dim = HEAD_DIM // 2
    inverse = ROPE_BASE ** (-jnp.arange(half_dim, dtype=jnp.float32) / half_dim)
    angles = positions.astype(jnp.float32)[:, None] * inverse[None, :]
    cosine, sine = jnp.cos(angles), jnp.sin(angles)
    cosines = jnp.concatenate([cosine] * 4, axis=1)
    sines = jnp.concatenate([-sine, sine] * 2, axis=1)

    in_cols = conv_cols[1] + qkv_cols[1]
    lines = SIDE * block

    def early(first, last, before):
        held = pieces[first:last]
        return call(
            functools.partial(early_kernel, first, len(held)),
            shape((row_count, in_cols), jnp.float32),
            2 * row_count * lines * len(held) * in_cols,
            [VMEM] * (1 + len(held) + len(before)),
            (normed, *held, *before),
            (pltpu.VMEM((lines * len(held), in_cols), jnp.bfloat16),),
            limit=16,
        )

    total = early(0, 5, ())
    total = early(5, 7, (total,))
    glu, qkv, tail = call(
        functools.partial(late_kernel, 7),
        (shape((row_count, channels)), shape((row_count, qkv_cols[1])), shape((WINDOW + 64, 128))),
        2 * row_count * lines * in_cols,
        [VMEM] * 6,
        (normed, cosines, sines, total, *pieces[7:]),
        (pltpu.VMEM((lines, in_cols), jnp.bfloat16),),
        limit=16,
    )
    before = lax.ppermute(tail, SP, NEXT_CHIP)
    out_own = call(
        functools.partial(join_kernel, out_cols[0]),
        shape((model, out_cols[1])),
        1 << 28,
        [VMEM] * len(pieces),
        pieces,
        limit=12,
    )
    out_other = lax.ppermute(out_own, SP, OTHER_CORE)

    members = CORES * lax.axis_size("tp")
    conv_out, sums = call(
        conv_kernel,
        (shape((row_count, channels), jnp.float32), shape((members, 2, row_count), jnp.float32)),
        1 << 32,
        [VMEM] * 3,
        (before, glu, conv_taps),
        (pltpu.VMEM((2, row_count + 32, 128), jnp.float32),),
        limit=12,
    )
    everyones = lax.all_to_all(sums, CHIP, 0, 0, tiled=True)
    extended = pltpu.VMEM((row_count + WINDOW, 128), jnp.bfloat16)
    attn_kept, attn_given, log_rows = call(
        attention_kernel,
        (
            shape((own_rows, q_cols)),
            shape((own_rows, q_cols)),
            shape((query_heads, row_count), jnp.float32),
        ),
        1 << 32,
        [SMEM, VMEM, VMEM],
        (sinks, qkv, before),
        (extended,) * 4,
        limit=12,
    )
    conv_kept, given = call(
        scaled_kernel,
        (shape((own_rows, channels)), shape((own_rows, channels + q_cols))),
        1 << 28,
        [VMEM] * 4,
        (conv_out, everyones, ln_gain[None], attn_given),
        limit=12,
    )
    rows_got = lax.ppermute(given, SP, OTHER_CORE)

    kept = lax.dynamic_slice_in_dim(log_rows, core * own_rows, own_rows, 1)
    given = lax.dynamic_slice_in_dim(log_rows, (1 - core) * own_rows, own_rows, 1)
    logs_got = lax.ppermute(given, SP, OTHER_CORE)
    log_sums = jnp.where(
        core == 0,
        jnp.concatenate([kept, logs_got], axis=0),
        jnp.concatenate([logs_got, kept], axis=0),
    )

    peers = lax.axis_size("tp")
    share = own_rows // peers

    def output(steps):
        return call(
            functools.partial(output_kernel, steps),
            (shape((share, model)),) * len(steps),
            2 * share * len(steps) * model * 2 * out_cols[1],
            [VMEM] * 5,
            (conv_kept, attn_kept, rows_got, out_own, out_other),
            (
                pltpu.VMEM((share * len(steps), 2 * out_cols[1]), jnp.bfloat16),
                pltpu.VMEM((TILE, 2 * out_cols[1]), jnp.bfloat16),
            ),
            limit=12,
        )

    def to_member(value, away):
        return lax.ppermute(value, "tp", [(i, (i + away) % peers) for i in range(peers)])

    far, up = output((2, 1))
    far, up = to_member(far, 2), to_member(up, 1)
    down, mine = output((3, 0))
    down = to_member(down, 3)
    mixed = (
        mine.astype(jnp.float32)
        + far.astype(jnp.float32)
        + up.astype(jnp.float32)
        + down.astype(jnp.float32)
    )
    return (mixed.astype(jnp.bfloat16), log_sums)


def solution(mesh):
    split = Mesh(mesh.devices.reshape(-1, CORES, mesh.shape["tp"]), ("chip", "core", "tp"))
    in_specs = (
        P(SP, None),
        P(),
        P(SP, "tp"),
        P(SP, "tp"),
        P(SP, "tp"),
        P(SP, "tp"),
        P(SP, "tp"),
        P(None, "tp"),
        P("tp"),
        P("tp"),
        P("tp", SP),
        P("tp", SP),
    )
    out_specs = (P((*SP, "tp"), None), P("tp", SP))
    return jax.shard_map(layer, mesh=split, in_specs=in_specs, out_specs=out_specs, check_vma=False)
```

```python
import functools

import jax
import jax.numpy as jnp
from jax import lax
from jax.experimental import pallas as pl
from jax.experimental.pallas import tpu as pltpu
from jax.sharding import Mesh, PartitionSpec as P

CONV_CH = 2048
HEAD_DIM = 64
WINDOW = 128

NORM_EPS = 1e-06
CHANNEL_EPS = 1e-05
ROPE_BASE = 10000.0

SIDE = 8
CHIPS = SIDE * SIDE
CORES = 2
SP = ("chip", "core")
CHIP = ("core", "tp")


def place(z, y, core):
    return ((z % SIDE) * SIDE + y % SIDE) * CORES + core


def at_line(line, step, core):
    return place(line, step, core) if core == 0 else place(step, line, core)


LINES = [[at_line(i, j, c) for j in range(SIDE)] for c in range(CORES) for i in range(SIDE)]
AHEAD, BEHIND = (
    [
        (at_line(i, j, c), at_line(i + by, j, c))
        for c in range(CORES)
        for i in range(SIDE)
        for j in range(SIDE)
    ]
    for by in (1, -1)
)
OTHER_CORE = [(i, i ^ 1) for i in range(CHIPS * CORES)]
NEXT_CHIP = [(i, i + CORES) for i in range(CHIPS * CORES - CORES)]

VMEM = pl.BlockSpec(memory_space=pltpu.VMEM)
SMEM = pl.BlockSpec(memory_space=pltpu.SMEM)
HBM = pl.BlockSpec(memory_space=pltpu.MemorySpace.HBM)
TILE = 256


def call(body, outs, flops, in_specs, operands, scratch=(), limit=None):
    return pl.pallas_call(
        body,
        out_shape=outs,
        in_specs=in_specs,
        out_specs=jax.tree.map(lambda _: VMEM, outs),
        scratch_shapes=list(scratch),
        compiler_params=pltpu.CompilerParams(vmem_limit_bytes=limit and limit << 20),
        cost_estimate=pl.CostEstimate(flops=flops, bytes_accessed=1 << 20, transcendentals=0),
    )(*operands)


def shape(dims, dtype=jnp.bfloat16):
    return jax.ShapeDtypeStruct(dims, dtype)


def pack_kernel(*refs):
    count = (len(refs) - 3) // 2
    shards, held, sems = refs[:count], refs[count + 2 : -1], refs[-1]
    kept_ref, given_ref = refs[count : count + 2]
    copies = [
        pltpu.make_async_copy(shard, here, sems.at[index])
        for index, (shard, here) in enumerate(zip(shards, held))
    ]
    for copy in copies:
        copy.start()
    for copy in copies:
        copy.wait()
    value_ref, gate_ref, query_ref, key_ref, v_ref, conv_ref, attn_ref = held
    core = lax.axis_index("core")
    lane = lax.broadcasted_iota(jnp.int32, key_ref.shape, 1)
    key = key_ref[...].astype(jnp.float32)
    value = v_ref[...].astype(jnp.float32)
    both = (
        jnp.where(lane < HEAD_DIM, key, pltpu.roll(value, HEAD_DIM, 1)),
        jnp.where(lane < HEAD_DIM, pltpu.roll(key, HEAD_DIM, 1), value),
    )
    for half in range(CORES):
        parts = []
        for source in (value_ref, gate_ref, query_ref, None, conv_ref, attn_ref):
            if source is None:
                parts.append(both[half].astype(jnp.bfloat16))
            else:
                width = source.shape[1] // CORES
                parts.append(source[:, half * width : (half + 1) * width])
        whole = jnp.concatenate(parts, axis=1)

        @pl.when(core == half)
        def _():
            kept_ref[...] = whole

        @pl.when(core != half)
        def _():
            given_ref[...] = whole


def repeat_kernel(kept_ref, got_ref, out_ref):
    core, rows = lax.axis_index("core"), kept_ref.shape[0]
    for source, to_core in ((kept_ref, core), (got_ref, 1 - core)):
        to = pl.ds(pl.multiple_of(to_core * rows, rows), rows)
        for member in range(out_ref.shape[0]):
            out_ref[member, to, :] = source[...]


def norm_kernel(own_ref, other_ref, gain_ref, out_ref):
    core = lax.axis_index("core")
    count, _ = own_ref.shape
    group = 128 // 4
    tile = 32
    lane = lax.broadcasted_iota(jnp.int32, (tile, 128), 1)
    gain = gain_ref[...].astype(jnp.float32)

    @pl.loop(0, count // tile)
    def _(step):
        at = pl.multiple_of(step * tile, tile)
        for source, to_core in ((own_ref, core), (other_ref, 1 - core)):
            x = source[pl.ds(at, tile), :].astype(jnp.float32)
            scale = lax.rsqrt(jnp.mean(x * x, axis=-1, keepdims=True) + NORM_EPS)
            normed = x * scale * gain
            rows = pl.ds(pl.multiple_of(to_core * count + at, tile), tile)

            @pl.when(core == 0)
            def _():
                out_ref[rows, :] = normed.astype(jnp.bfloat16)

            @pl.when(core == 1)
            def _():
                for z in range(0, SIDE, 4):
                    for y in range(0, SIDE, 4):
                        tiles = []
                        for part in range(4):
                            start = ((z + part) * SIDE + y) * group
                            tiles.append(normed[:, start : start + 128])
                        for away in (2, 1):
                            low = jnp.bitwise_and(lane // group, away) == 0
                            tiles = [
                                jnp.where(low, tiles[i], pltpu.roll(tiles[i + away], away * group, 1))
                                if i & away == 0
                                else jnp.where(
                                    low, pltpu.roll(tiles[i - away], 128 - away * group, 1), tiles[i]
                                )
                                for i in range(4)
                            ]
                        for part in range(4):
                            to = ((y + part) * SIDE + z) * group
                            out_ref[rows, to : to + 128] = tiles[part].astype(jnp.bfloat16)


def line_of(index):
    away = (index + 1) // 2 * (1 if index % 2 == 0 else -1)
    first = SIDE // 2 if index == SIDE else 0
    chip = lax.axis_index("chip")
    line = jnp.where(lax.axis_index("core") == 0, chip // SIDE, chip % SIDE)
    return jnp.bitwise_and(line + away, SIDE - 1), first


def products(x_ref, rows, pieces, first, held_ref):
    parts = []
    for index, piece in enumerate(pieces, first):
        line, step = line_of(index)
        block = piece.shape[1]
        size = piece.shape[0] * block
        start = pl.multiple_of(line * (SIDE * block) + step * block, 128)
        parts.append(x_ref[rows, pl.ds(start, size)])
    return jnp.dot(jnp.concatenate(parts, axis=1), held_ref[...], preferred_element_type=jnp.float32)


def hold(pieces, held_ref):
    to = 0
    for piece in pieces:
        for step in range(piece.shape[0]):
            held_ref[to : to + piece.shape[1], :] = piece[step, :, : held_ref.shape[1]]
            to += piece.shape[1]


def rows_of(step):
    return pl.ds(pl.multiple_of(step * TILE, TILE), TILE)


def early_kernel(first, count, x_ref, *refs):
    pieces, before, (out_ref, held_ref) = refs[:count], refs[count:-2], refs[-2:]
    hold(pieces, held_ref)

    @pl.loop(0, x_ref.shape[0] // TILE)
    def _(step):
        rows = rows_of(step)
        total = products(x_ref, rows, pieces, first, held_ref)
        for other in before:
            total = total + other[rows, :]
        out_ref[rows, :] = total


def late_kernel(
    first, x_ref, cos_ref, sin_ref, before_ref, a_ref, b_ref, glu_ref, qkv_ref, tail_ref, held_ref
):
    pieces = (a_ref, b_ref)
    hold(pieces, held_ref)
    channels, width = glu_ref.shape[1], qkv_ref.shape[1]

    @pl.loop(0, x_ref.shape[0] // TILE)
    def _(step):
        rows = rows_of(step)
        total = products(x_ref, rows, pieces, first, held_ref) + before_ref[rows, :]
        raw = total.astype(jnp.bfloat16).astype(jnp.float32)
        value, gate = raw[:, :channels], raw[:, channels : 2 * channels]
        glu_ref[rows, :] = (value * jax.nn.sigmoid(gate)).astype(jnp.bfloat16)
        lane = lax.broadcasted_iota(jnp.int32, (TILE, 128), 1)
        front = jnp.bitwise_and(lane, HEAD_DIM - 1) < HEAD_DIM // 2
        cosine, sine = cos_ref[rows, :], sin_ref[rows, :]
        for at in range(0, width, 128):
            part = raw[:, 2 * channels + at : 2 * channels + at + 128]
            other = jnp.where(
                front,
                pltpu.roll(part, 128 - HEAD_DIM // 2, 1),
                pltpu.roll(part, HEAD_DIM // 2, 1),
            )
            turned = part * cosine + other * sine
            if at + 128 == width:
                turned = jnp.where(lane < HEAD_DIM, turned, part)
            qkv_ref[rows, at : at + 128] = turned.astype(jnp.bfloat16)

    end = x_ref.shape[0]
    tail_ref[0:WINDOW, :] = qkv_ref[end - WINDOW : end, width - 128 : width]
    tail_ref[WINDOW : WINDOW + 32, :] = glu_ref[end - 32 : end, :128]
    tail_ref[WINDOW + 32 : WINDOW + 64, :] = glu_ref[end - 32 : end, 128:]


def join_kernel(column, *refs):
    pieces, out_ref = refs[:-1], refs[-1]
    for index, piece in enumerate(pieces):
        line, first = line_of(index)
        block = piece.shape[1]
        for step in range(piece.shape[0]):
            to = pl.multiple_of(line * (SIDE * block) + (first + step) * block, block)
            out_ref[pl.ds(to, block), :] = piece[step, :, column:]


def conv_kernel(before_ref, glu_ref, taps_ref, out_ref, sums_ref, ext_ref):
    count, (rows, channels) = taps_ref.shape[0], glu_ref.shape
    first_channel = lax.axis_index("core") * channels
    lead = 32
    for part in range(2):
        lanes = pl.ds(part * 128, 128)
        held = pl.ds(WINDOW + part * lead, lead)
        ext_ref[part, pl.ds(0, lead), :] = before_ref[held, :].astype(jnp.float32)
        ext_ref[part, pl.ds(lead, rows), :] = glu_ref[:, lanes].astype(jnp.float32)

    @pl.loop(0, rows // 128)
    def _(step):
        base = pl.multiple_of(step * 128, 128)
        first = jnp.zeros((128, 128), jnp.float32)
        second = jnp.zeros((128, 128), jnp.float32)
        for part in range(2):
            lanes = pl.ds(part * 128, 128)
            own = pl.ds(pl.multiple_of(first_channel + part * 128, 128), 128)
            total = jnp.zeros((128, 128), jnp.float32)
            for tap in range(count):
                rows_at = pl.ds(base + (lead - count + 1 + tap), 128)
                total = total + taps_ref[pl.ds(tap, 1), own] * ext_ref[part, rows_at, :]
            out_ref[pl.ds(base, 128), lanes] = total
            first = first + total
            second = second + total * total
        first = jnp.sum(first.T, axis=0, keepdims=True)
        second = jnp.sum(second.T, axis=0, keepdims=True)
        for member in range(sums_ref.shape[0]):
            sums_ref[member, pl.ds(0, 1), pl.ds(base, 128)] = first
            sums_ref[member, pl.ds(1, 1), pl.ds(base, 128)] = second


def scaled_kernel(conv_ref, sums_ref, gain_ref, attn_ref, kept_ref, given_ref):
    core = lax.axis_index("core")
    totals = sums_ref[0]
    for member in range(1, sums_ref.shape[0]):
        totals = totals + sums_ref[member]
    mean = totals[0:1] / CONV_CH
    scale = lax.rsqrt(totals[1:2] / CONV_CH - mean * mean + CHANNEL_EPS)
    half, channels = kept_ref.shape
    given_ref[:, channels:] = attn_ref[...]
    for base in range(0, conv_ref.shape[0], 128):
        at = slice(base, base + 128)
        mean_at = jnp.broadcast_to(mean[:, at], (128, 128)).T
        scale_at = jnp.broadcast_to(scale[:, at], (128, 128)).T
        parts = []
        for lane in range(0, channels, 128):
            own = pl.ds(pl.multiple_of(core * channels + lane, 128), 128)
            normed = (conv_ref[at, lane : lane + 128] - mean_at) * scale_at * gain_ref[0:1, own]
            parts.append((normed * jax.nn.sigmoid(normed)).astype(jnp.bfloat16))
        out = jnp.concatenate(parts, axis=1)
        to = slice(base % half, base % half + 128)

        @pl.when(core == base // half)
        def _():
            kept_ref[to, :] = out

        @pl.when(core != base // half)
        def _():
            given_ref[to, :channels] = out


def attention_kernel(
    sinks_ref, qkv_ref, before_ref, kept_ref, given_ref, logs_ref, k_lo, k_hi, v_lo, v_hi
):
    core, chip = lax.axis_index("core"), lax.axis_index("chip")
    cols = kept_ref.shape[1]
    for source, to, count in ((before_ref, 0, WINDOW), (qkv_ref, WINDOW, qkv_ref.shape[0])):
        both = source[:count, source.shape[1] - 128 :].astype(jnp.float32)
        low = lax.broadcasted_iota(jnp.int32, both.shape, 1) < HEAD_DIM
        turned = pltpu.roll(both, HEAD_DIM, 1)
        rows = slice(to, to + both.shape[0])
        k_lo[rows, :] = jnp.where(low, both, 0.0).astype(jnp.bfloat16)
        k_hi[rows, :] = jnp.where(low, 0.0, turned).astype(jnp.bfloat16)
        v_lo[rows, :] = jnp.where(low, turned, 0.0).astype(jnp.bfloat16)
        v_hi[rows, :] = jnp.where(low, 0.0, both).astype(jnp.bfloat16)
    blocks = qkv_ref.shape[0] // WINDOW
    half_blocks = blocks // CORES
    heads = cols // HEAD_DIM

    @pl.loop(0, blocks, unroll=2)
    def _(block):
        base = pl.multiple_of(block * WINDOW, WINDOW)
        window = pl.ds(base, 2 * WINDOW)
        key_at = lax.broadcasted_iota(jnp.int32, (2 * WINDOW, WINDOW), 0)
        query_at = lax.broadcasted_iota(jnp.int32, (2 * WINDOW, WINDOW), 1)
        lowest = jnp.where((chip == 0) & (block == 0), WINDOW, 0)
        allowed = (key_at > query_at) & (key_at <= query_at + WINDOW) & (key_at >= lowest)
        outs = []
        for pair in range(heads // 2):
            query = qkv_ref[pl.ds(base, WINDOW), pair * 128 : (pair + 1) * 128] * HEAD_DIM ** (-0.5)
            total = jnp.zeros((WINDOW, 128), jnp.float32)
            for which, (keys, values) in enumerate(((k_lo, v_lo), (k_hi, v_hi))):
                head = 2 * pair + which
                scores = lax.dot_general(
                    keys[window, :],
                    query,
                    (((1,), (1,)), ((), ())),
                    preferred_element_type=jnp.float32,
                )
                scores = jnp.where(allowed, scores, -jnp.inf)
                sums = jnp.sum(jnp.exp(scores), axis=0, keepdims=True)
                sink = jnp.full((1, WINDOW), sinks_ref[core * heads + head], jnp.float32)
                log_total = jnp.log(sums + jnp.exp(sink))
                logs_ref[pl.ds(head, 1), pl.ds(base, WINDOW)] = log_total
                weights = jnp.exp(scores - log_total).astype(jnp.bfloat16)
                total = total + lax.dot_general(
                    weights,
                    values[window, :],
                    (((0,), (0,)), ((), ())),
                    preferred_element_type=jnp.float32,
                )
            outs.append(total.astype(jnp.bfloat16))
        out = jnp.concatenate(outs, axis=1)
        own = block // half_blocks == core
        to = pl.ds(pl.multiple_of((block % half_blocks) * WINDOW, WINDOW), WINDOW)

        @pl.when(own)
        def _():
            kept_ref[to, :] = out

        @pl.when(jnp.logical_not(own))
        def _():
            given_ref[to, :] = out


def output_kernel(steps, conv_ref, attn_ref, got_ref, own_ref, other_ref, *rest):
    out_refs, (x_ref, w_ref) = rest[:-2], rest[-2:]
    core, member = lax.axis_index("core"), lax.axis_index("tp")
    count = out_refs[0].shape[0]
    peers = conv_ref.shape[0] // count
    block = own_ref.shape[0] // CHIPS
    width = own_ref.shape[1]
    for index, away in enumerate(steps):
        to = jnp.bitwise_and(member + away, peers - 1)
        rows = pl.ds(pl.multiple_of(to * count, count), count)
        x_ref[index * count : (index + 1) * count, :] = jnp.concatenate(
            [conv_ref[rows, :], attn_ref[rows, :], got_ref[rows, :]], axis=1
        )

    @pl.loop(0, SIDE, unroll=4)
    def _(z):
        cols = pl.ds(pl.multiple_of(z * SIDE * block, TILE), SIDE * block)
        by_z, by_y = z * SIDE * block, z * block
        for source, at, along_z in ((own_ref, 0, core == 0), (other_ref, width, core == 1)):
            first = jnp.where(along_z, by_z, by_y)
            stride = jnp.where(along_z, block, SIDE * block)
            for y in range(SIDE):
                start = pl.multiple_of(first + y * stride, block)
                w_ref[y * block : (y + 1) * block, at : at + width] = source[pl.ds(start, block), :]
        total = lax.dot_general(
            x_ref[...], w_ref[...], (((1,), (1,)), ((), ())), preferred_element_type=jnp.float32
        )
        for index, out_ref in enumerate(out_refs):
            out_ref[:, cols] = total[index * count : (index + 1) * count].astype(jnp.bfloat16)


def layer(
    tokens,
    norm_gain,
    w_conv_value,
    w_conv_gate,
    w_query,
    w_key,
    w_value,
    conv_taps,
    ln_gain,
    sinks,
    out_conv,
    out_attn,
):
    core = lax.axis_index("core")
    chip = lax.axis_index("chip")
    own_rows, model = tokens.shape
    row_count = own_rows * CORES
    depth = w_conv_value.shape[0]
    channels = w_conv_value.shape[1] // CORES
    q_cols = w_query.shape[1] // CORES
    query_heads = q_cols // HEAD_DIM
    block = CORES * depth

    conv_cols = (0, 2 * channels)
    qkv_cols = (2 * channels, q_cols + 2 * HEAD_DIM)
    out_cols = (2 * channels + q_cols + 2 * HEAD_DIM, channels + q_cols)
    width = sum(out_cols)
    shards_in = (w_conv_value, w_conv_gate, w_query, w_key, w_value, out_conv.T, out_attn.T)
    kept, given = call(
        pack_kernel,
        (shape((depth, width)),) * 2,
        1 << 20,
        [HBM] * len(shards_in),
        shards_in,
        (
            *(pltpu.VMEM(w.shape, w.dtype) for w in shards_in),
            pltpu.SemaphoreType.DMA((len(shards_in),)),
        ),
    )
    got = lax.ppermute(given, SP, OTHER_CORE)
    sent = call(repeat_kernel, shape((SIDE, block, width)), 1 << 20, [VMEM, VMEM], (kept, got))
    own_line = lax.all_to_all(sent, SP, 0, 0, tiled=True, axis_index_groups=LINES)
    pieces = [own_line]
    ahead = behind = own_line
    for step in range(SIDE // 2):
        if step == SIDE // 2 - 1:
            ahead, behind = ahead[: SIDE // 2], behind[SIDE // 2 :]
        ahead = lax.ppermute(ahead, SP, AHEAD)
        behind = lax.ppermute(behind, SP, BEHIND)
        pieces += [ahead, behind]

    tokens_other = lax.ppermute(tokens, SP, OTHER_CORE)
    normed = call(
        norm_kernel,
        shape((row_count, model)),
        1 << 30,
        [VMEM, VMEM, VMEM],
        (tokens, tokens_other, norm_gain[None]),
        limit=16,
    )

    positions = chip * row_count + jnp.arange(row_count, dtype=jnp.int32)
    half_dim = HEAD_DIM // 2
    inverse = ROPE_BASE ** (-jnp.arange(half_dim, dtype=jnp.float32) / half_dim)
    angles = positions.astype(jnp.float32)[:, None] * inverse[None, :]
    cosine, sine = jnp.cos(angles), jnp.sin(angles)
    cosines = jnp.concatenate([cosine] * 4, axis=1)
    sines = jnp.concatenate([-sine, sine] * 2, axis=1)

    in_cols = conv_cols[1] + qkv_cols[1]
    lines = SIDE * block

    def early(first, last, before):
        held = pieces[first:last]
        return call(
            functools.partial(early_kernel, first, len(held)),
            shape((row_count, in_cols), jnp.float32),
            2 * row_count * lines * len(held) * in_cols,
            [VMEM] * (1 + len(held) + len(before)),
            (normed, *held, *before),
            (pltpu.VMEM((lines * len(held), in_cols), jnp.bfloat16),),
            limit=16,
        )

    total = early(0, 5, ())
    total = early(5, 7, (total,))
    glu, qkv, tail = call(
        functools.partial(late_kernel, 7),
        (shape((row_count, channels)), shape((row_count, qkv_cols[1])), shape((WINDOW + 64, 128))),
        2 * row_count * lines * in_cols,
        [VMEM] * 6,
        (normed, cosines, sines, total, *pieces[7:]),
        (pltpu.VMEM((lines, in_cols), jnp.bfloat16),),
        limit=16,
    )
    before = lax.ppermute(tail, SP, NEXT_CHIP)
    out_own = call(
        functools.partial(join_kernel, out_cols[0]),
        shape((model, out_cols[1])),
        1 << 28,
        [VMEM] * len(pieces),
        pieces,
        limit=12,
    )
    out_other = lax.ppermute(out_own, SP, OTHER_CORE)

    members = CORES * lax.axis_size("tp")
    conv_out, sums = call(
        conv_kernel,
        (shape((row_count, channels), jnp.float32), shape((members, 2, row_count), jnp.float32)),
        1 << 32,
        [VMEM] * 3,
        (before, glu, conv_taps),
        (pltpu.VMEM((2, row_count + 32, 128), jnp.float32),),
        limit=12,
    )
    everyones = lax.all_to_all(sums, CHIP, 0, 0, tiled=True)
    extended = pltpu.VMEM((row_count + WINDOW, 128), jnp.bfloat16)
    attn_kept, attn_given, log_rows = call(
        attention_kernel,
        (
            shape((own_rows, q_cols)),
            shape((own_rows, q_cols)),
            shape((query_heads, row_count), jnp.float32),
        ),
        1 << 32,
        [SMEM, VMEM, VMEM],
        (sinks, qkv, before),
        (extended,) * 4,
        limit=12,
    )
    conv_kept, given = call(
        scaled_kernel,
        (shape((own_rows, channels)), shape((own_rows, channels + q_cols))),
        1 << 28,
        [VMEM] * 4,
        (conv_out, everyones, ln_gain[None], attn_given),
        limit=12,
    )
    rows_got = lax.ppermute(given, SP, OTHER_CORE)

    kept = lax.dynamic_slice_in_dim(log_rows, core * own_rows, own_rows, 1)
    given = lax.dynamic_slice_in_dim(log_rows, (1 - core) * own_rows, own_rows, 1)
    logs_got = lax.ppermute(given, SP, OTHER_CORE)
    log_sums = jnp.where(
        core == 0,
        jnp.concatenate([kept, logs_got], axis=0),
        jnp.concatenate([logs_got, kept], axis=0),
    )

    peers = lax.axis_size("tp")
    share = own_rows // peers

    def output(steps):
        return call(
            functools.partial(output_kernel, steps),
            (shape((share, model)),) * len(steps),
            2 * share * len(steps) * model * 2 * out_cols[1],
            [VMEM] * 5,
            (conv_kept, attn_kept, rows_got, out_own, out_other),
            (
                pltpu.VMEM((share * len(steps), 2 * out_cols[1]), jnp.bfloat16),
                pltpu.VMEM((TILE, 2 * out_cols[1]), jnp.bfloat16),
            ),
            limit=12,
        )

    def to_member(value, away):
        return lax.ppermute(value, "tp", [(i, (i + away) % peers) for i in range(peers)])

    far, up = output((2, 1))
    far, up = to_member(far, 2), to_member(up, 1)
    down, mine = output((3, 0))
    down = to_member(down, 3)
    mixed = (
        mine.astype(jnp.float32)
        + far.astype(jnp.float32)
        + up.astype(jnp.float32)
        + down.astype(jnp.float32)
    )
    return (mixed.astype(jnp.bfloat16), log_sums)


def solution(mesh):
    split = Mesh(mesh.devices.reshape(-1, CORES, mesh.shape["tp"]), ("chip", "core", "tp"))
    in_specs = (
        P(SP, None),
        P(),
        P(SP, "tp"),
        P(SP, "tp"),
        P(SP, "tp"),
        P(SP, "tp"),
        P(SP, "tp"),
        P(None, "tp"),
        P("tp"),
        P("tp"),
        P("tp", SP),
        P("tp", SP),
    )
    out_specs = (P((*SP, "tp"), None), P("tp", SP))
    return jax.shard_map(layer, mesh=split, in_specs=in_specs, out_specs=out_specs, check_vma=False)
```

```python
import functools

import jax
import jax.numpy as jnp
from jax import lax
from jax.experimental import pallas as pl
from jax.experimental.pallas import tpu as pltpu
from jax.sharding import Mesh, PartitionSpec as P

CONV_CH = 2048
HEAD_DIM = 64
WINDOW = 128

NORM_EPS = 1e-06
CHANNEL_EPS = 1e-05
ROPE_BASE = 10000.0

SIDE = 8
CHIPS = SIDE * SIDE
CORES = 2
SP = ("chip", "core")
CHIP = ("core", "tp")


def place(z, y, core):
    return ((z % SIDE) * SIDE + y % SIDE) * CORES + core


def at_line(line, step, core):
    return place(line, step, core) if core == 0 else place(step, line, core)


LINES = [[at_line(i, j, c) for j in range(SIDE)] for c in range(CORES) for i in range(SIDE)]
AHEAD, BEHIND = (
    [
        (at_line(i, j, c), at_line(i + by, j, c))
        for c in range(CORES)
        for i in range(SIDE)
        for j in range(SIDE)
    ]
    for by in (1, -1)
)
OTHER_CORE = [(i, i ^ 1) for i in range(CHIPS * CORES)]
NEXT_CHIP = [(i, i + CORES) for i in range(CHIPS * CORES - CORES)]

VMEM = pl.BlockSpec(memory_space=pltpu.VMEM)
SMEM = pl.BlockSpec(memory_space=pltpu.SMEM)
HBM = pl.BlockSpec(memory_space=pltpu.MemorySpace.HBM)
TILE = 256


def call(body, outs, flops, in_specs, operands, scratch=(), limit=None):
    return pl.pallas_call(
        body,
        out_shape=outs,
        in_specs=in_specs,
        out_specs=jax.tree.map(lambda _: VMEM, outs),
        scratch_shapes=list(scratch),
        compiler_params=pltpu.CompilerParams(vmem_limit_bytes=limit and limit << 20),
        cost_estimate=pl.CostEstimate(flops=flops, bytes_accessed=1 << 20, transcendentals=0),
    )(*operands)


def shape(dims, dtype=jnp.bfloat16):
    return jax.ShapeDtypeStruct(dims, dtype)


def pack_kernel(*refs):
    count = (len(refs) - 3) // 2
    shards, held, sems = refs[:count], refs[count + 2 : -1], refs[-1]
    kept_ref, given_ref = refs[count : count + 2]
    copies = [
        pltpu.make_async_copy(shard, here, sems.at[index])
        for index, (shard, here) in enumerate(zip(shards, held))
    ]
    for copy in copies:
        copy.start()
    for copy in copies:
        copy.wait()
    value_ref, gate_ref, query_ref, key_ref, v_ref, conv_ref, attn_ref = held
    core = lax.axis_index("core")
    lane = lax.broadcasted_iota(jnp.int32, key_ref.shape, 1)
    key = key_ref[...].astype(jnp.float32)
    value = v_ref[...].astype(jnp.float32)
    both = (
        jnp.where(lane < HEAD_DIM, key, pltpu.roll(value, HEAD_DIM, 1)),
        jnp.where(lane < HEAD_DIM, pltpu.roll(key, HEAD_DIM, 1), value),
    )
    for half in range(CORES):
        parts = []
        for source in (value_ref, gate_ref, query_ref, None, conv_ref, attn_ref):
            if source is None:
                parts.append(both[half].astype(jnp.bfloat16))
            else:
                width = source.shape[1] // CORES
                parts.append(source[:, half * width : (half + 1) * width])
        whole = jnp.concatenate(parts, axis=1)

        @pl.when(core == half)
        def _():
            kept_ref[...] = whole

        @pl.when(core != half)
        def _():
            given_ref[...] = whole


def repeat_kernel(kept_ref, got_ref, out_ref):
    core, rows = lax.axis_index("core"), kept_ref.shape[0]
    for source, to_core in ((kept_ref, core), (got_ref, 1 - core)):
        to = pl.ds(pl.multiple_of(to_core * rows, rows), rows)
        for member in range(out_ref.shape[0]):
            out_ref[member, to, :] = source[...]


def norm_kernel(x_ref, gain_ref, out_ref):
    core = lax.axis_index("core")
    count, _ = x_ref.shape
    group = 128 // 4
    tile = 32
    lane = lax.broadcasted_iota(jnp.int32, (tile, 128), 1)
    gain = gain_ref[...].astype(jnp.float32)

    @pl.loop(0, count // tile)
    def _(step):
        rows = pl.ds(pl.multiple_of(step * tile, tile), tile)
        x = x_ref[rows, :].astype(jnp.float32)
        scale = lax.rsqrt(jnp.mean(x * x, axis=-1, keepdims=True) + NORM_EPS)
        normed = x * scale * gain

        @pl.when(core == 0)
        def _():
            out_ref[rows, :] = normed.astype(jnp.bfloat16)

        @pl.when(core == 1)
        def _():
            for z in range(0, SIDE, 4):
                for y in range(0, SIDE, 4):
                    tiles = []
                    for part in range(4):
                        start = ((z + part) * SIDE + y) * group
                        tiles.append(normed[:, start : start + 128])
                    for away in (2, 1):
                        low = jnp.bitwise_and(lane // group, away) == 0
                        tiles = [
                            jnp.where(low, tiles[i], pltpu.roll(tiles[i + away], away * group, 1))
                            if i & away == 0
                            else jnp.where(
                                low, pltpu.roll(tiles[i - away], 128 - away * group, 1), tiles[i]
                            )
                            for i in range(4)
                        ]
                    for part in range(4):
                        to = ((y + part) * SIDE + z) * group
                        out_ref[rows, to : to + 128] = tiles[part].astype(jnp.bfloat16)


def line_of(index):
    away = (index + 1) // 2 * (1 if index % 2 == 0 else -1)
    first = SIDE // 2 if index == SIDE else 0
    chip = lax.axis_index("chip")
    line = jnp.where(lax.axis_index("core") == 0, chip // SIDE, chip % SIDE)
    return jnp.bitwise_and(line + away, SIDE - 1), first


def products(x_ref, rows, pieces, first, held_ref):
    parts = []
    for index, piece in enumerate(pieces, first):
        line, step = line_of(index)
        block = piece.shape[1]
        size = piece.shape[0] * block
        start = pl.multiple_of(line * (SIDE * block) + step * block, 128)
        parts.append(x_ref[rows, pl.ds(start, size)])
    return jnp.dot(jnp.concatenate(parts, axis=1), held_ref[...], preferred_element_type=jnp.float32)


def hold(pieces, held_ref):
    to = 0
    for piece in pieces:
        for step in range(piece.shape[0]):
            held_ref[to : to + piece.shape[1], :] = piece[step, :, : held_ref.shape[1]]
            to += piece.shape[1]


def row_tiles(own_ref, other_ref, body):
    core, count = lax.axis_index("core"), own_ref.shape[0]
    for x_ref, of_core in ((own_ref, core), (other_ref, 1 - core)):

        @pl.loop(0, count // TILE)
        def _(step):
            here = pl.multiple_of(step * TILE, TILE)
            there = pl.multiple_of(of_core * count + step * TILE, TILE)
            body(x_ref, pl.ds(here, TILE), pl.ds(there, TILE))


def early_kernel(first, count, own_ref, other_ref, *refs):
    pieces, before, (out_ref, held_ref) = refs[:count], refs[count:-2], refs[-2:]
    hold(pieces, held_ref)

    def body(x_ref, here, rows):
        total = products(x_ref, here, pieces, first, held_ref)
        for other in before:
            total = total + other[rows, :]
        out_ref[rows, :] = total

    row_tiles(own_ref, other_ref, body)


def late_kernel(
    first, own_ref, other_ref, cos_ref, sin_ref, before_ref, a_ref, b_ref, glu_ref, qkv_ref, tail_ref, held_ref
):
    pieces = (a_ref, b_ref)
    hold(pieces, held_ref)
    channels, width = glu_ref.shape[1], qkv_ref.shape[1]

    def body(x_ref, here, rows):
        total = products(x_ref, here, pieces, first, held_ref) + before_ref[rows, :]
        raw = total.astype(jnp.bfloat16).astype(jnp.float32)
        value, gate = raw[:, :channels], raw[:, channels : 2 * channels]
        glu_ref[rows, :] = (value * jax.nn.sigmoid(gate)).astype(jnp.bfloat16)
        lane = lax.broadcasted_iota(jnp.int32, (TILE, 128), 1)
        front = jnp.bitwise_and(lane, HEAD_DIM - 1) < HEAD_DIM // 2
        cosine, sine = cos_ref[rows, :], sin_ref[rows, :]
        for at in range(0, width, 128):
            part = raw[:, 2 * channels + at : 2 * channels + at + 128]
            other = jnp.where(
                front,
                pltpu.roll(part, 128 - HEAD_DIM // 2, 1),
                pltpu.roll(part, HEAD_DIM // 2, 1),
            )
            turned = part * cosine + other * sine
            if at + 128 == width:
                turned = jnp.where(lane < HEAD_DIM, turned, part)
            qkv_ref[rows, at : at + 128] = turned.astype(jnp.bfloat16)

    row_tiles(own_ref, other_ref, body)
    end = glu_ref.shape[0]
    tail_ref[0:WINDOW, :] = qkv_ref[end - WINDOW : end, width - 128 : width]
    tail_ref[WINDOW : WINDOW + 32, :] = glu_ref[end - 32 : end, :128]
    tail_ref[WINDOW + 32 : WINDOW + 64, :] = glu_ref[end - 32 : end, 128:]


def join_kernel(column, *refs):
    pieces, out_ref = refs[:-1], refs[-1]
    for index, piece in enumerate(pieces):
        line, first = line_of(index)
        block = piece.shape[1]
        for step in range(piece.shape[0]):
            to = pl.multiple_of(line * (SIDE * block) + (first + step) * block, block)
            out_ref[pl.ds(to, block), :] = piece[step, :, column:]


def conv_kernel(before_ref, glu_ref, taps_ref, out_ref, sums_ref, ext_ref, pair_ref):
    count, (rows, channels) = taps_ref.shape[0], glu_ref.shape
    first_channel = lax.axis_index("core") * channels
    lead = 32
    for part in range(2):
        lanes = pl.ds(part * 128, 128)
        held = pl.ds(WINDOW + part * lead, lead)
        ext_ref[part, pl.ds(0, lead), :] = before_ref[held, :].astype(jnp.float32)
        ext_ref[part, pl.ds(lead, rows), :] = glu_ref[:, lanes].astype(jnp.float32)

    @pl.loop(0, rows // 128)
    def _(step):
        base = pl.multiple_of(step * 128, 128)
        for half in range(0, 128, 64):
            first = jnp.zeros((64, 128), jnp.float32)
            second = jnp.zeros((64, 128), jnp.float32)
            for part in range(2):
                own = pl.ds(pl.multiple_of(first_channel + part * 128, 128), 128)
                total = jnp.zeros((64, 128), jnp.float32)
                for tap in range(count):
                    rows_at = pl.ds(base + (half + lead - count + 1 + tap), 64)
                    total = total + taps_ref[pl.ds(tap, 1), own] * ext_ref[part, rows_at, :]
                out_ref[pl.ds(base + half, 64), pl.ds(part * 128, 128)] = total
                first = first + total
                second = second + total * total
            pair_ref[0, half : half + 64, :] = first
            pair_ref[1, half : half + 64, :] = second
        first = jnp.sum(pair_ref[0].T, axis=0, keepdims=True)
        second = jnp.sum(pair_ref[1].T, axis=0, keepdims=True)
        for member in range(sums_ref.shape[0]):
            sums_ref[member, pl.ds(0, 1), pl.ds(base, 128)] = first
            sums_ref[member, pl.ds(1, 1), pl.ds(base, 128)] = second


def scaled_kernel(conv_ref, sums_ref, gain_ref, attn_ref, kept_ref, given_ref):
    core = lax.axis_index("core")
    totals = sums_ref[0]
    for member in range(1, sums_ref.shape[0]):
        totals = totals + sums_ref[member]
    mean = totals[0:1] / CONV_CH
    scale = lax.rsqrt(totals[1:2] / CONV_CH - mean * mean + CHANNEL_EPS)
    half, channels = kept_ref.shape
    given_ref[:, channels:] = attn_ref[...]
    for base in range(0, conv_ref.shape[0], 128):
        at = slice(base, base + 128)
        mean_at = jnp.broadcast_to(mean[:, at], (128, 128)).T
        scale_at = jnp.broadcast_to(scale[:, at], (128, 128)).T
        parts = []
        for lane in range(0, channels, 128):
            own = pl.ds(pl.multiple_of(core * channels + lane, 128), 128)
            normed = (conv_ref[at, lane : lane + 128] - mean_at) * scale_at * gain_ref[0:1, own]
            parts.append((normed * jax.nn.sigmoid(normed)).astype(jnp.bfloat16))
        out = jnp.concatenate(parts, axis=1)
        to = slice(base % half, base % half + 128)

        @pl.when(core == base // half)
        def _():
            kept_ref[to, :] = out

        @pl.when(core != base // half)
        def _():
            given_ref[to, :channels] = out


def attention_kernel(
    sinks_ref, qkv_ref, before_ref, kept_ref, given_ref, logs_ref, k_lo, k_hi, v_lo, v_hi
):
    core, chip = lax.axis_index("core"), lax.axis_index("chip")
    cols = kept_ref.shape[1]
    for source, to, count in ((before_ref, 0, WINDOW), (qkv_ref, WINDOW, qkv_ref.shape[0])):
        both = source[:count, source.shape[1] - 128 :].astype(jnp.float32)
        low = lax.broadcasted_iota(jnp.int32, both.shape, 1) < HEAD_DIM
        turned = pltpu.roll(both, HEAD_DIM, 1)
        rows = slice(to, to + both.shape[0])
        k_lo[rows, :] = jnp.where(low, both, 0.0).astype(jnp.bfloat16)
        k_hi[rows, :] = jnp.where(low, 0.0, turned).astype(jnp.bfloat16)
        v_lo[rows, :] = jnp.where(low, turned, 0.0).astype(jnp.bfloat16)
        v_hi[rows, :] = jnp.where(low, 0.0, both).astype(jnp.bfloat16)
    blocks = qkv_ref.shape[0] // WINDOW
    half_blocks = blocks // CORES
    heads = cols // HEAD_DIM

    @pl.loop(0, blocks, unroll=2)
    def _(block):
        base = pl.multiple_of(block * WINDOW, WINDOW)
        window = pl.ds(base, 2 * WINDOW)
        key_at = lax.broadcasted_iota(jnp.int32, (2 * WINDOW, WINDOW), 0)
        query_at = lax.broadcasted_iota(jnp.int32, (2 * WINDOW, WINDOW), 1)
        lowest = jnp.where((chip == 0) & (block == 0), WINDOW, 0)
        allowed = (key_at > query_at) & (key_at <= query_at + WINDOW) & (key_at >= lowest)
        outs = []
        for pair in range(heads // 2):
            query = qkv_ref[pl.ds(base, WINDOW), pair * 128 : (pair + 1) * 128] * HEAD_DIM ** (-0.5)
            total = jnp.zeros((WINDOW, 128), jnp.float32)
            for which, (keys, values) in enumerate(((k_lo, v_lo), (k_hi, v_hi))):
                head = 2 * pair + which
                scores = lax.dot_general(
                    keys[window, :],
                    query,
                    (((1,), (1,)), ((), ())),
                    preferred_element_type=jnp.float32,
                )
                scores = jnp.where(allowed, scores, -jnp.inf)
                sums = jnp.sum(jnp.exp(scores), axis=0, keepdims=True)
                sink = jnp.full((1, WINDOW), sinks_ref[core * heads + head], jnp.float32)
                log_total = jnp.log(sums + jnp.exp(sink))
                logs_ref[pl.ds(head, 1), pl.ds(base, WINDOW)] = log_total
                weights = jnp.exp(scores - log_total).astype(jnp.bfloat16)
                total = total + lax.dot_general(
                    weights,
                    values[window, :],
                    (((0,), (0,)), ((), ())),
                    preferred_element_type=jnp.float32,
                )
            outs.append(total.astype(jnp.bfloat16))
        out = jnp.concatenate(outs, axis=1)
        own = block // half_blocks == core
        to = pl.ds(pl.multiple_of((block % half_blocks) * WINDOW, WINDOW), WINDOW)

        @pl.when(own)
        def _():
            kept_ref[to, :] = out

        @pl.when(jnp.logical_not(own))
        def _():
            given_ref[to, :] = out


def output_kernel(steps, conv_ref, attn_ref, got_ref, own_ref, other_ref, *rest):
    out_refs, (x_ref, w_ref) = rest[:-2], rest[-2:]
    core, member = lax.axis_index("core"), lax.axis_index("tp")
    count = out_refs[0].shape[0]
    peers = conv_ref.shape[0] // count
    block = own_ref.shape[0] // CHIPS
    width = own_ref.shape[1]
    for index, away in enumerate(steps):
        to = jnp.bitwise_and(member + away, peers - 1)
        rows = pl.ds(pl.multiple_of(to * count, count), count)
        x_ref[index * count : (index + 1) * count, :] = jnp.concatenate(
            [conv_ref[rows, :], attn_ref[rows, :], got_ref[rows, :]], axis=1
        )

    @pl.loop(0, SIDE, unroll=4)
    def _(z):
        cols = pl.ds(pl.multiple_of(z * SIDE * block, TILE), SIDE * block)
        by_z, by_y = z * SIDE * block, z * block
        for source, at, along_z in ((own_ref, 0, core == 0), (other_ref, width, core == 1)):
            first = jnp.where(along_z, by_z, by_y)
            stride = jnp.where(along_z, block, SIDE * block)
            for y in range(SIDE):
                start = pl.multiple_of(first + y * stride, block)
                w_ref[y * block : (y + 1) * block, at : at + width] = source[pl.ds(start, block), :]
        total = lax.dot_general(
            x_ref[...], w_ref[...], (((1,), (1,)), ((), ())), preferred_element_type=jnp.float32
        )
        for index, out_ref in enumerate(out_refs):
            out_ref[:, cols] = total[index * count : (index + 1) * count].astype(jnp.bfloat16)


def layer(
    tokens,
    norm_gain,
    w_conv_value,
    w_conv_gate,
    w_query,
    w_key,
    w_value,
    conv_taps,
    ln_gain,
    sinks,
    out_conv,
    out_attn,
):
    core = lax.axis_index("core")
    chip = lax.axis_index("chip")
    own_rows, model = tokens.shape
    row_count = own_rows * CORES
    depth = w_conv_value.shape[0]
    channels = w_conv_value.shape[1] // CORES
    q_cols = w_query.shape[1] // CORES
    query_heads = q_cols // HEAD_DIM
    block = CORES * depth

    conv_cols = (0, 2 * channels)
    qkv_cols = (2 * channels, q_cols + 2 * HEAD_DIM)
    out_cols = (2 * channels + q_cols + 2 * HEAD_DIM, channels + q_cols)
    width = sum(out_cols)
    shards_in = (w_conv_value, w_conv_gate, w_query, w_key, w_value, out_conv.T, out_attn.T)
    kept, given = call(
        pack_kernel,
        (shape((depth, width)),) * 2,
        1 << 20,
        [HBM] * len(shards_in),
        shards_in,
        (
            *(pltpu.VMEM(w.shape, w.dtype) for w in shards_in),
            pltpu.SemaphoreType.DMA((len(shards_in),)),
        ),
    )
    got = lax.ppermute(given, SP, OTHER_CORE)
    sent = call(repeat_kernel, shape((SIDE, block, width)), 1 << 20, [VMEM, VMEM], (kept, got))
    own_line = lax.all_to_all(sent, SP, 0, 0, tiled=True, axis_index_groups=LINES)
    pieces = [own_line]
    ahead = behind = own_line
    for step in range(SIDE // 2):
        if step == SIDE // 2 - 1:
            ahead, behind = ahead[: SIDE // 2], behind[SIDE // 2 :]
        ahead = lax.ppermute(ahead, SP, AHEAD)
        behind = lax.ppermute(behind, SP, BEHIND)
        pieces += [ahead, behind]

    tokens_other = lax.ppermute(tokens, SP, OTHER_CORE)

    def rms_normed(rows):
        return call(
            norm_kernel, shape(rows.shape), 1 << 30, [VMEM, VMEM], (rows, norm_gain[None]), limit=12
        )

    normed = (rms_normed(tokens), rms_normed(tokens_other))

    positions = chip * row_count + jnp.arange(row_count, dtype=jnp.int32)
    half_dim = HEAD_DIM // 2
    inverse = ROPE_BASE ** (-jnp.arange(half_dim, dtype=jnp.float32) / half_dim)
    angles = positions.astype(jnp.float32)[:, None] * inverse[None, :]
    cosine, sine = jnp.cos(angles), jnp.sin(angles)
    cosines = jnp.concatenate([cosine] * 4, axis=1)
    sines = jnp.concatenate([-sine, sine] * 2, axis=1)

    in_cols = conv_cols[1] + qkv_cols[1]
    lines = SIDE * block

    def early(first, last, before):
        held = pieces[first:last]
        return call(
            functools.partial(early_kernel, first, len(held)),
            shape((row_count, in_cols), jnp.float32),
            2 * row_count * lines * len(held) * in_cols,
            [VMEM] * (2 + len(held) + len(before)),
            (*normed, *held, *before),
            (pltpu.VMEM((lines * len(held), in_cols), jnp.bfloat16),),
            limit=16,
        )

    total = early(0, 5, ())
    total = early(5, 7, (total,))
    glu, qkv, tail = call(
        functools.partial(late_kernel, 7),
        (shape((row_count, channels)), shape((row_count, qkv_cols[1])), shape((WINDOW + 64, 128))),
        2 * row_count * lines * in_cols,
        [VMEM] * 7,
        (*normed, cosines, sines, total, *pieces[7:]),
        (pltpu.VMEM((lines, in_cols), jnp.bfloat16),),
        limit=16,
    )
    before = lax.ppermute(tail, SP, NEXT_CHIP)
    out_own = call(
        functools.partial(join_kernel, out_cols[0]),
        shape((model, out_cols[1])),
        1 << 28,
        [VMEM] * len(pieces),
        pieces,
        limit=12,
    )
    out_other = lax.ppermute(out_own, SP, OTHER_CORE)

    members = CORES * lax.axis_size("tp")
    conv_out, sums = call(
        conv_kernel,
        (shape((row_count, channels), jnp.float32), shape((members, 2, row_count), jnp.float32)),
        1 << 32,
        [VMEM] * 3,
        (before, glu, conv_taps),
        (pltpu.VMEM((2, row_count + 32, 128), jnp.float32), pltpu.VMEM((2, 128, 128), jnp.float32)),
        limit=12,
    )
    everyones = lax.all_to_all(sums, CHIP, 0, 0, tiled=True)
    extended = pltpu.VMEM((row_count + WINDOW, 128), jnp.bfloat16)
    attn_kept, attn_given, log_rows = call(
        attention_kernel,
        (
            shape((own_rows, q_cols)),
            shape((own_rows, q_cols)),
            shape((query_heads, row_count), jnp.float32),
        ),
        1 << 32,
        [SMEM, VMEM, VMEM],
        (sinks, qkv, before),
        (extended,) * 4,
        limit=12,
    )
    conv_kept, given = call(
        scaled_kernel,
        (shape((own_rows, channels)), shape((own_rows, channels + q_cols))),
        1 << 28,
        [VMEM] * 4,
        (conv_out, everyones, ln_gain[None], attn_given),
        limit=12,
    )
    rows_got = lax.ppermute(given, SP, OTHER_CORE)

    kept = lax.dynamic_slice_in_dim(log_rows, core * own_rows, own_rows, 1)
    given = lax.dynamic_slice_in_dim(log_rows, (1 - core) * own_rows, own_rows, 1)
    logs_got = lax.ppermute(given, SP, OTHER_CORE)
    log_sums = jnp.where(
        core == 0,
        jnp.concatenate([kept, logs_got], axis=0),
        jnp.concatenate([logs_got, kept], axis=0),
    )

    peers = lax.axis_size("tp")
    share = own_rows // peers

    def output(steps):
        return call(
            functools.partial(output_kernel, steps),
            (shape((share, model)),) * len(steps),
            2 * share * len(steps) * model * 2 * out_cols[1],
            [VMEM] * 5,
            (conv_kept, attn_kept, rows_got, out_own, out_other),
            (
                pltpu.VMEM((share * len(steps), 2 * out_cols[1]), jnp.bfloat16),
                pltpu.VMEM((TILE, 2 * out_cols[1]), jnp.bfloat16),
            ),
            limit=12,
        )

    def to_member(value, away):
        return lax.ppermute(value, "tp", [(i, (i + away) % peers) for i in range(peers)])

    far, up, down, mine = output((2, 1, 3, 0))
    far, up = to_member(far, 2), to_member(up, 1)
    down = to_member(down, 3)
    mixed = (
        mine.astype(jnp.float32)
        + far.astype(jnp.float32)
        + up.astype(jnp.float32)
        + down.astype(jnp.float32)
    )
    return (mixed.astype(jnp.bfloat16), log_sums)


def solution(mesh):
    split = Mesh(mesh.devices.reshape(-1, CORES, mesh.shape["tp"]), ("chip", "core", "tp"))
    in_specs = (
        P(SP, None),
        P(),
        P(SP, "tp"),
        P(SP, "tp"),
        P(SP, "tp"),
        P(SP, "tp"),
        P(SP, "tp"),
        P(None, "tp"),
        P("tp"),
        P("tp"),
        P("tp", SP),
        P("tp", SP),
    )
    out_specs = (P((*SP, "tp"), None), P("tp", SP))
    return jax.shard_map(layer, mesh=split, in_specs=in_specs, out_specs=out_specs, check_vma=False)
```

```python
import functools

import jax
import jax.numpy as jnp
from jax import lax
from jax.experimental import pallas as pl
from jax.experimental.pallas import tpu as pltpu
from jax.sharding import Mesh, PartitionSpec as P

CONV_CH = 2048
HEAD_DIM = 64
WINDOW = 128

NORM_EPS = 1e-06
CHANNEL_EPS = 1e-05
ROPE_BASE = 10000.0

SIDE = 8
CHIPS = SIDE * SIDE
CORES = 2
SP = ("chip", "core")
CHIP = ("core", "tp")


def place(z, y, core):
    return ((z % SIDE) * SIDE + y % SIDE) * CORES + core


def at_line(line, step, core):
    return place(line, step, core) if core == 0 else place(step, line, core)


LINES = [[at_line(i, j, c) for j in range(SIDE)] for c in range(CORES) for i in range(SIDE)]
AHEAD, BEHIND = (
    [
        (at_line(i, j, c), at_line(i + by, j, c))
        for c in range(CORES)
        for i in range(SIDE)
        for j in range(SIDE)
    ]
    for by in (1, -1)
)
OTHER_CORE = [(i, i ^ 1) for i in range(CHIPS * CORES)]
NEXT_CHIP = [(i, i + CORES) for i in range(CHIPS * CORES - CORES)]

VMEM = pl.BlockSpec(memory_space=pltpu.VMEM)
SMEM = pl.BlockSpec(memory_space=pltpu.SMEM)
HBM = pl.BlockSpec(memory_space=pltpu.MemorySpace.HBM)
TILE = 256


def call(body, outs, flops, in_specs, operands, scratch=(), limit=None):
    return pl.pallas_call(
        body,
        out_shape=outs,
        in_specs=in_specs,
        out_specs=jax.tree.map(lambda _: VMEM, outs),
        scratch_shapes=list(scratch),
        compiler_params=pltpu.CompilerParams(vmem_limit_bytes=limit and limit << 20),
        cost_estimate=pl.CostEstimate(flops=flops, bytes_accessed=1 << 20, transcendentals=0),
    )(*operands)


def shape(dims, dtype=jnp.bfloat16):
    return jax.ShapeDtypeStruct(dims, dtype)


def pack_kernel(*refs):
    count = (len(refs) - 3) // 2
    shards, held, sems = refs[:count], refs[count + 2 : -1], refs[-1]
    kept_ref, given_ref = refs[count : count + 2]
    copies = [
        pltpu.make_async_copy(shard, here, sems.at[index])
        for index, (shard, here) in enumerate(zip(shards, held))
    ]
    for copy in copies:
        copy.start()
    for copy in copies:
        copy.wait()
    value_ref, gate_ref, query_ref, key_ref, v_ref, conv_ref, attn_ref = held
    core = lax.axis_index("core")
    lane = lax.broadcasted_iota(jnp.int32, key_ref.shape, 1)
    key = key_ref[...].astype(jnp.float32)
    value = v_ref[...].astype(jnp.float32)
    both = (
        jnp.where(lane < HEAD_DIM, key, pltpu.roll(value, HEAD_DIM, 1)),
        jnp.where(lane < HEAD_DIM, pltpu.roll(key, HEAD_DIM, 1), value),
    )
    for half in range(CORES):
        parts = []
        for source in (value_ref, gate_ref, query_ref, None, conv_ref, attn_ref):
            if source is None:
                parts.append(both[half].astype(jnp.bfloat16))
            else:
                width = source.shape[1] // CORES
                parts.append(source[:, half * width : (half + 1) * width])
        whole = jnp.concatenate(parts, axis=1)

        @pl.when(core == half)
        def _():
            kept_ref[...] = whole

        @pl.when(core != half)
        def _():
            given_ref[...] = whole


def repeat_kernel(kept_ref, got_ref, out_ref):
    core, rows = lax.axis_index("core"), kept_ref.shape[0]
    for source, to_core in ((kept_ref, core), (got_ref, 1 - core)):
        to = pl.ds(pl.multiple_of(to_core * rows, rows), rows)
        for member in range(out_ref.shape[0]):
            out_ref[member, to, :] = source[...]


def norm_kernel(x_ref, gain_ref, out_ref):
    core = lax.axis_index("core")
    count, _ = x_ref.shape
    group = 128 // 4
    tile = 32
    lane = lax.broadcasted_iota(jnp.int32, (tile, 128), 1)
    gain = gain_ref[...].astype(jnp.float32)

    @pl.loop(0, count // tile)
    def _(step):
        rows = pl.ds(pl.multiple_of(step * tile, tile), tile)
        x = x_ref[rows, :].astype(jnp.float32)
        scale = lax.rsqrt(jnp.mean(x * x, axis=-1, keepdims=True) + NORM_EPS)
        normed = x * scale * gain

        @pl.when(core == 0)
        def _():
            out_ref[rows, :] = normed.astype(jnp.bfloat16)

        @pl.when(core == 1)
        def _():
            for z in range(0, SIDE, 4):
                for y in range(0, SIDE, 4):
                    tiles = []
                    for part in range(4):
                        start = ((z + part) * SIDE + y) * group
                        tiles.append(normed[:, start : start + 128])
                    for away in (2, 1):
                        low = jnp.bitwise_and(lane // group, away) == 0
                        tiles = [
                            jnp.where(low, tiles[i], pltpu.roll(tiles[i + away], away * group, 1))
                            if i & away == 0
                            else jnp.where(
                                low, pltpu.roll(tiles[i - away], 128 - away * group, 1), tiles[i]
                            )
                            for i in range(4)
                        ]
                    for part in range(4):
                        to = ((y + part) * SIDE + z) * group
                        out_ref[rows, to : to + 128] = tiles[part].astype(jnp.bfloat16)


def line_of(index):
    away = (index + 1) // 2 * (1 if index % 2 == 0 else -1)
    first = SIDE // 2 if index == SIDE else 0
    chip = lax.axis_index("chip")
    line = jnp.where(lax.axis_index("core") == 0, chip // SIDE, chip % SIDE)
    return jnp.bitwise_and(line + away, SIDE - 1), first


def products(x_ref, rows, pieces, first, held_ref):
    parts = []
    for index, piece in enumerate(pieces, first):
        line, step = line_of(index)
        block = piece.shape[1]
        size = piece.shape[0] * block
        start = pl.multiple_of(line * (SIDE * block) + step * block, 128)
        parts.append(x_ref[rows, pl.ds(start, size)])
    return jnp.dot(jnp.concatenate(parts, axis=1), held_ref[...], preferred_element_type=jnp.float32)


def hold(pieces, held_ref):
    to = 0
    for piece in pieces:
        for step in range(piece.shape[0]):
            held_ref[to : to + piece.shape[1], :] = piece[step, :, : held_ref.shape[1]]
            to += piece.shape[1]


def row_tiles(own_ref, other_ref, body):
    core, count = lax.axis_index("core"), own_ref.shape[0]
    for x_ref, of_core in ((own_ref, core), (other_ref, 1 - core)):

        @pl.loop(0, count // TILE)
        def _(step):
            here = pl.multiple_of(step * TILE, TILE)
            there = pl.multiple_of(of_core * count + step * TILE, TILE)
            body(x_ref, pl.ds(here, TILE), pl.ds(there, TILE))


def early_kernel(first, count, own_ref, other_ref, *refs):
    pieces, before, (out_ref, held_ref) = refs[:count], refs[count:-2], refs[-2:]
    hold(pieces, held_ref)

    def body(x_ref, here, rows):
        total = products(x_ref, here, pieces, first, held_ref)
        for other in before:
            total = total + other[rows, :]
        out_ref[rows, :] = total

    row_tiles(own_ref, other_ref, body)


def late_kernel(
    first, own_ref, other_ref, cos_ref, sin_ref, before_ref, a_ref, b_ref, glu_ref, qkv_ref, tail_ref, held_ref
):
    pieces = (a_ref, b_ref)
    hold(pieces, held_ref)
    channels, width = glu_ref.shape[1], qkv_ref.shape[1]

    def body(x_ref, here, rows):
        total = products(x_ref, here, pieces, first, held_ref) + before_ref[rows, :]
        raw = total.astype(jnp.bfloat16).astype(jnp.float32)
        value, gate = raw[:, :channels], raw[:, channels : 2 * channels]
        glu_ref[rows, :] = (value * jax.nn.sigmoid(gate)).astype(jnp.bfloat16)
        lane = lax.broadcasted_iota(jnp.int32, (TILE, 128), 1)
        front = jnp.bitwise_and(lane, HEAD_DIM - 1) < HEAD_DIM // 2
        cosine, sine = cos_ref[rows, :], sin_ref[rows, :]
        for at in range(0, width, 128):
            part = raw[:, 2 * channels + at : 2 * channels + at + 128]
            other = jnp.where(
                front,
                pltpu.roll(part, 128 - HEAD_DIM // 2, 1),
                pltpu.roll(part, HEAD_DIM // 2, 1),
            )
            turned = part * cosine + other * sine
            if at + 128 == width:
                turned = jnp.where(lane < HEAD_DIM, turned, part)
            qkv_ref[rows, at : at + 128] = turned.astype(jnp.bfloat16)

    row_tiles(own_ref, other_ref, body)
    end = glu_ref.shape[0]
    tail_ref[0:WINDOW, :] = qkv_ref[end - WINDOW : end, width - 128 : width]
    tail_ref[WINDOW : WINDOW + 32, :] = glu_ref[end - 32 : end, :128]
    tail_ref[WINDOW + 32 : WINDOW + 64, :] = glu_ref[end - 32 : end, 128:]


def join_kernel(column, *refs):
    pieces, out_ref = refs[:-1], refs[-1]
    for index, piece in enumerate(pieces):
        line, first = line_of(index)
        block = piece.shape[1]
        for step in range(piece.shape[0]):
            to = pl.multiple_of(line * (SIDE * block) + (first + step) * block, block)
            out_ref[pl.ds(to, block), :] = piece[step, :, column:]


def conv_kernel(before_ref, glu_ref, taps_ref, out_ref, sums_ref, ext_ref, pair_ref):
    count, (rows, channels) = taps_ref.shape[0], glu_ref.shape
    first_channel = lax.axis_index("core") * channels
    lead = 32
    for part in range(2):
        lanes = pl.ds(part * 128, 128)
        held = pl.ds(WINDOW + part * lead, lead)
        ext_ref[part, pl.ds(0, lead), :] = before_ref[held, :].astype(jnp.float32)
        ext_ref[part, pl.ds(lead, rows), :] = glu_ref[:, lanes].astype(jnp.float32)

    @pl.loop(0, rows // 128)
    def _(step):
        base = pl.multiple_of(step * 128, 128)
        for half in range(0, 128, 64):
            first = jnp.zeros((64, 128), jnp.float32)
            second = jnp.zeros((64, 128), jnp.float32)
            for part in range(2):
                own = pl.ds(pl.multiple_of(first_channel + part * 128, 128), 128)
                total = jnp.zeros((64, 128), jnp.float32)
                for tap in range(count):
                    rows_at = pl.ds(base + (half + lead - count + 1 + tap), 64)
                    total = total + taps_ref[pl.ds(tap, 1), own] * ext_ref[part, rows_at, :]
                out_ref[pl.ds(base + half, 64), pl.ds(part * 128, 128)] = total
                first = first + total
                second = second + total * total
            pair_ref[0, half : half + 64, :] = first
            pair_ref[1, half : half + 64, :] = second
        first = jnp.sum(pair_ref[0].T, axis=0, keepdims=True)
        second = jnp.sum(pair_ref[1].T, axis=0, keepdims=True)
        for member in range(sums_ref.shape[0]):
            sums_ref[member, pl.ds(0, 1), pl.ds(base, 128)] = first
            sums_ref[member, pl.ds(1, 1), pl.ds(base, 128)] = second


def scaled_kernel(conv_ref, sums_ref, gain_ref, attn_ref, kept_ref, given_ref):
    core = lax.axis_index("core")
    totals = sums_ref[0]
    for member in range(1, sums_ref.shape[0]):
        totals = totals + sums_ref[member]
    mean = totals[0:1] / CONV_CH
    scale = lax.rsqrt(totals[1:2] / CONV_CH - mean * mean + CHANNEL_EPS)
    half, channels = kept_ref.shape
    given_ref[:, channels:] = attn_ref[...]
    for base in range(0, conv_ref.shape[0], 128):
        at = slice(base, base + 128)
        mean_at = jnp.broadcast_to(mean[:, at], (128, 128)).T
        scale_at = jnp.broadcast_to(scale[:, at], (128, 128)).T
        parts = []
        for lane in range(0, channels, 128):
            own = pl.ds(pl.multiple_of(core * channels + lane, 128), 128)
            normed = (conv_ref[at, lane : lane + 128] - mean_at) * scale_at * gain_ref[0:1, own]
            parts.append((normed * jax.nn.sigmoid(normed)).astype(jnp.bfloat16))
        out = jnp.concatenate(parts, axis=1)
        to = slice(base % half, base % half + 128)

        @pl.when(core == base // half)
        def _():
            kept_ref[to, :] = out

        @pl.when(core != base // half)
        def _():
            given_ref[to, :channels] = out


def attention_kernel(
    sinks_ref, qkv_ref, before_ref, kept_ref, given_ref, logs_ref, k_lo, k_hi, v_lo, v_hi
):
    core, chip = lax.axis_index("core"), lax.axis_index("chip")
    cols = kept_ref.shape[1]
    for source, to, count in ((before_ref, 0, WINDOW), (qkv_ref, WINDOW, qkv_ref.shape[0])):
        both = source[:count, source.shape[1] - 128 :].astype(jnp.float32)
        low = lax.broadcasted_iota(jnp.int32, both.shape, 1) < HEAD_DIM
        turned = pltpu.roll(both, HEAD_DIM, 1)
        rows = slice(to, to + both.shape[0])
        k_lo[rows, :] = jnp.where(low, both, 0.0).astype(jnp.bfloat16)
        k_hi[rows, :] = jnp.where(low, 0.0, turned).astype(jnp.bfloat16)
        v_lo[rows, :] = jnp.where(low, turned, 0.0).astype(jnp.bfloat16)
        v_hi[rows, :] = jnp.where(low, 0.0, both).astype(jnp.bfloat16)
    blocks = qkv_ref.shape[0] // WINDOW
    half_blocks = blocks // CORES
    heads = cols // HEAD_DIM

    @pl.loop(0, blocks, unroll=2)
    def _(block):
        base = pl.multiple_of(block * WINDOW, WINDOW)
        window = pl.ds(base, 2 * WINDOW)
        query_at = lax.broadcasted_iota(jnp.int32, (WINDOW, 2 * WINDOW), 0)
        key_at = lax.broadcasted_iota(jnp.int32, (WINDOW, 2 * WINDOW), 1)
        head_at = lax.broadcasted_iota(jnp.int32, (WINDOW, 128), 1)
        logs = jnp.zeros((WINDOW, 128), jnp.float32)
        lowest = jnp.where((chip == 0) & (block == 0), WINDOW, 0)
        allowed = (key_at > query_at) & (key_at <= query_at + WINDOW) & (key_at >= lowest)
        outs = []
        for pair in range(heads // 2):
            query = qkv_ref[pl.ds(base, WINDOW), pair * 128 : (pair + 1) * 128] * HEAD_DIM ** (-0.5)
            total = jnp.zeros((WINDOW, 128), jnp.float32)
            for which, (keys, values) in enumerate(((k_lo, v_lo), (k_hi, v_hi))):
                head = 2 * pair + which
                scores = lax.dot_general(
                    query,
                    keys[window, :],
                    (((1,), (1,)), ((), ())),
                    preferred_element_type=jnp.float32,
                )
                scores = jnp.where(allowed, scores, -jnp.inf)
                sums = jnp.sum(jnp.exp(scores), axis=1, keepdims=True)
                sink = jnp.full((WINDOW, 1), sinks_ref[core * heads + head], jnp.float32)
                log_total = jnp.log(sums + jnp.exp(sink))
                logs = jnp.where(head_at == head, log_total, logs)
                weights = jnp.exp(scores - log_total).astype(jnp.bfloat16)
                total = total + jnp.dot(
                    weights, values[window, :], preferred_element_type=jnp.float32
                )
            outs.append(total.astype(jnp.bfloat16))
        out = jnp.concatenate(outs, axis=1)
        logs_ref[:, pl.ds(base, WINDOW)] = logs.T[:heads]
        own = block // half_blocks == core
        to = pl.ds(pl.multiple_of((block % half_blocks) * WINDOW, WINDOW), WINDOW)

        @pl.when(own)
        def _():
            kept_ref[to, :] = out

        @pl.when(jnp.logical_not(own))
        def _():
            given_ref[to, :] = out


def output_kernel(steps, conv_ref, attn_ref, got_ref, own_ref, other_ref, *rest):
    out_refs, (x_ref, w_ref) = rest[:-2], rest[-2:]
    core, member = lax.axis_index("core"), lax.axis_index("tp")
    count = out_refs[0].shape[0]
    peers = conv_ref.shape[0] // count
    block = own_ref.shape[0] // CHIPS
    width = own_ref.shape[1]
    for index, away in enumerate(steps):
        to = jnp.bitwise_and(member + away, peers - 1)
        rows = pl.ds(pl.multiple_of(to * count, count), count)
        x_ref[index * count : (index + 1) * count, :] = jnp.concatenate(
            [conv_ref[rows, :], attn_ref[rows, :], got_ref[rows, :]], axis=1
        )

    @pl.loop(0, SIDE, unroll=4)
    def _(z):
        cols = pl.ds(pl.multiple_of(z * SIDE * block, TILE), SIDE * block)
        by_z, by_y = z * SIDE * block, z * block
        for source, at, along_z in ((own_ref, 0, core == 0), (other_ref, width, core == 1)):
            first = jnp.where(along_z, by_z, by_y)
            stride = jnp.where(along_z, block, SIDE * block)
            for y in range(SIDE):
                start = pl.multiple_of(first + y * stride, block)
                w_ref[y * block : (y + 1) * block, at : at + width] = source[pl.ds(start, block), :]
        total = lax.dot_general(
            x_ref[...], w_ref[...], (((1,), (1,)), ((), ())), preferred_element_type=jnp.float32
        )
        for index, out_ref in enumerate(out_refs):
            out_ref[:, cols] = total[index * count : (index + 1) * count].astype(jnp.bfloat16)


def layer(
    tokens,
    norm_gain,
    w_conv_value,
    w_conv_gate,
    w_query,
    w_key,
    w_value,
    conv_taps,
    ln_gain,
    sinks,
    out_conv,
    out_attn,
):
    core = lax.axis_index("core")
    chip = lax.axis_index("chip")
    own_rows, model = tokens.shape
    row_count = own_rows * CORES
    depth = w_conv_value.shape[0]
    channels = w_conv_value.shape[1] // CORES
    q_cols = w_query.shape[1] // CORES
    query_heads = q_cols // HEAD_DIM
    block = CORES * depth

    conv_cols = (0, 2 * channels)
    qkv_cols = (2 * channels, q_cols + 2 * HEAD_DIM)
    out_cols = (2 * channels + q_cols + 2 * HEAD_DIM, channels + q_cols)
    width = sum(out_cols)
    shards_in = (w_conv_value, w_conv_gate, w_query, w_key, w_value, out_conv.T, out_attn.T)
    kept, given = call(
        pack_kernel,
        (shape((depth, width)),) * 2,
        1 << 20,
        [HBM] * len(shards_in),
        shards_in,
        (
            *(pltpu.VMEM(w.shape, w.dtype) for w in shards_in),
            pltpu.SemaphoreType.DMA((len(shards_in),)),
        ),
    )
    got = lax.ppermute(given, SP, OTHER_CORE)
    sent = call(repeat_kernel, shape((SIDE, block, width)), 1 << 20, [VMEM, VMEM], (kept, got))
    own_line = lax.all_to_all(sent, SP, 0, 0, tiled=True, axis_index_groups=LINES)
    pieces = [own_line]
    ahead = behind = own_line
    for step in range(SIDE // 2):
        if step == SIDE // 2 - 1:
            ahead, behind = ahead[: SIDE // 2], behind[SIDE // 2 :]
        ahead = lax.ppermute(ahead, SP, AHEAD)
        behind = lax.ppermute(behind, SP, BEHIND)
        pieces += [ahead, behind]

    tokens_other = lax.ppermute(tokens, SP, OTHER_CORE)

    def rms_normed(rows):
        return call(
            norm_kernel, shape(rows.shape), 1 << 30, [VMEM, VMEM], (rows, norm_gain[None]), limit=12
        )

    normed = (rms_normed(tokens), rms_normed(tokens_other))

    positions = chip * row_count + jnp.arange(row_count, dtype=jnp.int32)
    half_dim = HEAD_DIM // 2
    inverse = ROPE_BASE ** (-jnp.arange(half_dim, dtype=jnp.float32) / half_dim)
    angles = positions.astype(jnp.float32)[:, None] * inverse[None, :]
    cosine, sine = jnp.cos(angles), jnp.sin(angles)
    cosines = jnp.concatenate([cosine] * 4, axis=1)
    sines = jnp.concatenate([-sine, sine] * 2, axis=1)

    in_cols = conv_cols[1] + qkv_cols[1]
    lines = SIDE * block

    def early(first, last, before):
        held = pieces[first:last]
        return call(
            functools.partial(early_kernel, first, len(held)),
            shape((row_count, in_cols), jnp.float32),
            2 * row_count * lines * len(held) * in_cols,
            [VMEM] * (2 + len(held) + len(before)),
            (*normed, *held, *before),
            (pltpu.VMEM((lines * len(held), in_cols), jnp.bfloat16),),
            limit=16,
        )

    total = early(0, 5, ())
    total = early(5, 7, (total,))
    glu, qkv, tail = call(
        functools.partial(late_kernel, 7),
        (shape((row_count, channels)), shape((row_count, qkv_cols[1])), shape((WINDOW + 64, 128))),
        2 * row_count * lines * in_cols,
        [VMEM] * 7,
        (*normed, cosines, sines, total, *pieces[7:]),
        (pltpu.VMEM((lines, in_cols), jnp.bfloat16),),
        limit=16,
    )
    before = lax.ppermute(tail, SP, NEXT_CHIP)
    out_own = call(
        functools.partial(join_kernel, out_cols[0]),
        shape((model, out_cols[1])),
        1 << 28,
        [VMEM] * len(pieces),
        pieces,
        limit=12,
    )
    out_other = lax.ppermute(out_own, SP, OTHER_CORE)

    members = CORES * lax.axis_size("tp")
    conv_out, sums = call(
        conv_kernel,
        (shape((row_count, channels), jnp.float32), shape((members, 2, row_count), jnp.float32)),
        1 << 32,
        [VMEM] * 3,
        (before, glu, conv_taps),
        (pltpu.VMEM((2, row_count + 32, 128), jnp.float32), pltpu.VMEM((2, 128, 128), jnp.float32)),
        limit=12,
    )
    everyones = lax.all_to_all(sums, CHIP, 0, 0, tiled=True)
    extended = pltpu.VMEM((row_count + WINDOW, 128), jnp.bfloat16)
    attn_kept, attn_given, log_rows = call(
        attention_kernel,
        (
            shape((own_rows, q_cols)),
            shape((own_rows, q_cols)),
            shape((query_heads, row_count), jnp.float32),
        ),
        1 << 32,
        [SMEM, VMEM, VMEM],
        (sinks, qkv, before),
        (extended,) * 4,
    )
    conv_kept, given = call(
        scaled_kernel,
        (shape((own_rows, channels)), shape((own_rows, channels + q_cols))),
        1 << 28,
        [VMEM] * 4,
        (conv_out, everyones, ln_gain[None], attn_given),
        limit=12,
    )
    rows_got = lax.ppermute(given, SP, OTHER_CORE)

    kept = lax.dynamic_slice_in_dim(log_rows, core * own_rows, own_rows, 1)
    given = lax.dynamic_slice_in_dim(log_rows, (1 - core) * own_rows, own_rows, 1)
    logs_got = lax.ppermute(given, SP, OTHER_CORE)
    log_sums = jnp.where(
        core == 0,
        jnp.concatenate([kept, logs_got], axis=0),
        jnp.concatenate([logs_got, kept], axis=0),
    )

    peers = lax.axis_size("tp")
    share = own_rows // peers

    def output(steps):
        return call(
            functools.partial(output_kernel, steps),
            (shape((share, model)),) * len(steps),
            2 * share * len(steps) * model * 2 * out_cols[1],
            [VMEM] * 5,
            (conv_kept, attn_kept, rows_got, out_own, out_other),
            (
                pltpu.VMEM((share * len(steps), 2 * out_cols[1]), jnp.bfloat16),
                pltpu.VMEM((TILE, 2 * out_cols[1]), jnp.bfloat16),
            ),
            limit=12,
        )

    def to_member(value, away):
        return lax.ppermute(value, "tp", [(i, (i + away) % peers) for i in range(peers)])

    far, up, down, mine = output((2, 1, 3, 0))
    far, up = to_member(far, 2), to_member(up, 1)
    down = to_member(down, 3)
    mixed = (
        mine.astype(jnp.float32)
        + far.astype(jnp.float32)
        + up.astype(jnp.float32)
        + down.astype(jnp.float32)
    )
    return (mixed.astype(jnp.bfloat16), log_sums)


def solution(mesh):
    split = Mesh(mesh.devices.reshape(-1, CORES, mesh.shape["tp"]), ("chip", "core", "tp"))
    in_specs = (
        P(SP, None),
        P(),
        P(SP, "tp"),
        P(SP, "tp"),
        P(SP, "tp"),
        P(SP, "tp"),
        P(SP, "tp"),
        P(None, "tp"),
        P("tp"),
        P("tp"),
        P("tp", SP),
        P("tp", SP),
    )
    out_specs = (P((*SP, "tp"), None), P("tp", SP))
    return jax.shard_map(layer, mesh=split, in_specs=in_specs, out_specs=out_specs, check_vma=False)
```

```python
import functools

import jax
import jax.numpy as jnp
from jax import lax
from jax.experimental import pallas as pl
from jax.experimental.pallas import tpu as pltpu
from jax.sharding import Mesh, PartitionSpec as P

CONV_CH = 2048
HEAD_DIM = 64
WINDOW = 128

NORM_EPS = 1e-06
CHANNEL_EPS = 1e-05
ROPE_BASE = 10000.0

SIDE = 8
CHIPS = SIDE * SIDE
CORES = 2
SP = ("chip", "core")
CHIP = ("core", "tp")


def place(z, y, core):
    return ((z % SIDE) * SIDE + y % SIDE) * CORES + core


def at_line(line, step, core):
    return place(line, step, core) if core == 0 else place(step, line, core)


LINES = [[at_line(i, j, c) for j in range(SIDE)] for c in range(CORES) for i in range(SIDE)]
AHEAD, BEHIND = (
    [
        (at_line(i, j, c), at_line(i + by, j, c))
        for c in range(CORES)
        for i in range(SIDE)
        for j in range(SIDE)
    ]
    for by in (1, -1)
)
OTHER_CORE = [(i, i ^ 1) for i in range(CHIPS * CORES)]
NEXT_CHIP = [(i, i + CORES) for i in range(CHIPS * CORES - CORES)]

VMEM = pl.BlockSpec(memory_space=pltpu.VMEM)
SMEM = pl.BlockSpec(memory_space=pltpu.SMEM)
HBM = pl.BlockSpec(memory_space=pltpu.MemorySpace.HBM)
TILE = 256


def call(body, outs, flops, in_specs, operands, scratch=(), limit=None):
    return pl.pallas_call(
        body,
        out_shape=outs,
        in_specs=in_specs,
        out_specs=jax.tree.map(lambda _: VMEM, outs),
        scratch_shapes=list(scratch),
        compiler_params=pltpu.CompilerParams(vmem_limit_bytes=limit and limit << 20),
        cost_estimate=pl.CostEstimate(flops=flops, bytes_accessed=1 << 20, transcendentals=0),
    )(*operands)


def shape(dims, dtype=jnp.bfloat16):
    return jax.ShapeDtypeStruct(dims, dtype)


def pack_kernel(*refs):
    count = (len(refs) - 3) // 2
    shards, held, sems = refs[:count], refs[count + 2 : -1], refs[-1]
    kept_ref, given_ref = refs[count : count + 2]
    copies = [
        pltpu.make_async_copy(shard, here, sems.at[index])
        for index, (shard, here) in enumerate(zip(shards, held))
    ]
    for copy in copies:
        copy.start()
    for copy in copies:
        copy.wait()
    value_ref, gate_ref, query_ref, key_ref, v_ref, conv_ref, attn_ref = held
    core = lax.axis_index("core")
    lane = lax.broadcasted_iota(jnp.int32, key_ref.shape, 1)
    key = key_ref[...].astype(jnp.float32)
    value = v_ref[...].astype(jnp.float32)
    both = (
        jnp.where(lane < HEAD_DIM, key, pltpu.roll(value, HEAD_DIM, 1)),
        jnp.where(lane < HEAD_DIM, pltpu.roll(key, HEAD_DIM, 1), value),
    )
    for half in range(CORES):
        parts = []
        for source in (value_ref, gate_ref, query_ref, None, conv_ref, attn_ref):
            if source is None:
                parts.append(both[half].astype(jnp.bfloat16))
            else:
                width = source.shape[1] // CORES
                parts.append(source[:, half * width : (half + 1) * width])
        whole = jnp.concatenate(parts, axis=1)

        @pl.when(core == half)
        def _():
            kept_ref[...] = whole

        @pl.when(core != half)
        def _():
            given_ref[...] = whole


def repeat_kernel(kept_ref, got_ref, out_ref):
    core, rows = lax.axis_index("core"), kept_ref.shape[0]
    for source, to_core in ((kept_ref, core), (got_ref, 1 - core)):
        to = pl.ds(pl.multiple_of(to_core * rows, rows), rows)
        for member in range(out_ref.shape[0]):
            out_ref[member, to, :] = source[...]


def norm_kernel(x_ref, gain_ref, out_ref):
    core = lax.axis_index("core")
    count, _ = x_ref.shape
    group = 128 // 4
    tile = 32
    lane = lax.broadcasted_iota(jnp.int32, (tile, 128), 1)
    gain = gain_ref[...].astype(jnp.float32)

    @pl.loop(0, count // tile)
    def _(step):
        rows = pl.ds(pl.multiple_of(step * tile, tile), tile)
        x = x_ref[rows, :].astype(jnp.float32)
        scale = lax.rsqrt(jnp.mean(x * x, axis=-1, keepdims=True) + NORM_EPS)
        normed = x * scale * gain

        @pl.when(core == 0)
        def _():
            out_ref[rows, :] = normed.astype(jnp.bfloat16)

        @pl.when(core == 1)
        def _():
            for z in range(0, SIDE, 4):
                for y in range(0, SIDE, 4):
                    tiles = []
                    for part in range(4):
                        start = ((z + part) * SIDE + y) * group
                        tiles.append(normed[:, start : start + 128])
                    for away in (2, 1):
                        low = jnp.bitwise_and(lane // group, away) == 0
                        tiles = [
                            jnp.where(low, tiles[i], pltpu.roll(tiles[i + away], away * group, 1))
                            if i & away == 0
                            else jnp.where(
                                low, pltpu.roll(tiles[i - away], 128 - away * group, 1), tiles[i]
                            )
                            for i in range(4)
                        ]
                    for part in range(4):
                        to = ((y + part) * SIDE + z) * group
                        out_ref[rows, to : to + 128] = tiles[part].astype(jnp.bfloat16)


def line_of(index):
    away = (index + 1) // 2 * (1 if index % 2 == 0 else -1)
    first = SIDE // 2 if index == SIDE else 0
    chip = lax.axis_index("chip")
    line = jnp.where(lax.axis_index("core") == 0, chip // SIDE, chip % SIDE)
    return jnp.bitwise_and(line + away, SIDE - 1), first


def products(x_ref, rows, pieces, first, held_ref):
    parts = []
    for index, piece in enumerate(pieces, first):
        line, step = line_of(index)
        block = piece.shape[1]
        size = piece.shape[0] * block
        start = pl.multiple_of(line * (SIDE * block) + step * block, 128)
        parts.append(x_ref[rows, pl.ds(start, size)])
    return jnp.dot(jnp.concatenate(parts, axis=1), held_ref[...], preferred_element_type=jnp.float32)


def hold(pieces, held_ref):
    to = 0
    for piece in pieces:
        for step in range(piece.shape[0]):
            held_ref[to : to + piece.shape[1], :] = piece[step, :, : held_ref.shape[1]]
            to += piece.shape[1]


def row_tiles(own_ref, other_ref, body):
    core, count = lax.axis_index("core"), own_ref.shape[0]
    for x_ref, of_core in ((own_ref, core), (other_ref, 1 - core)):

        @pl.loop(0, count // TILE)
        def _(step):
            here = pl.multiple_of(step * TILE, TILE)
            there = pl.multiple_of(of_core * count + step * TILE, TILE)
            body(x_ref, pl.ds(here, TILE), pl.ds(there, TILE))


def early_kernel(first, count, own_ref, other_ref, *refs):
    pieces, before, (out_ref, held_ref) = refs[:count], refs[count:-2], refs[-2:]
    hold(pieces, held_ref)

    def body(x_ref, here, rows):
        total = products(x_ref, here, pieces, first, held_ref)
        for other in before:
            total = total + other[rows, :]
        out_ref[rows, :] = total

    row_tiles(own_ref, other_ref, body)


def late_kernel(
    first, own_ref, other_ref, cos_ref, sin_ref, before_ref, a_ref, b_ref, glu_ref, qkv_ref, tail_ref, held_ref
):
    pieces = (a_ref, b_ref)
    hold(pieces, held_ref)
    channels, width = glu_ref.shape[1], qkv_ref.shape[1]

    def body(x_ref, here, rows):
        total = products(x_ref, here, pieces, first, held_ref) + before_ref[rows, :]
        raw = total.astype(jnp.bfloat16).astype(jnp.float32)
        value, gate = raw[:, :channels], raw[:, channels : 2 * channels]
        glu_ref[rows, :] = (value * jax.nn.sigmoid(gate)).astype(jnp.bfloat16)
        lane = lax.broadcasted_iota(jnp.int32, (TILE, 128), 1)
        front = jnp.bitwise_and(lane, HEAD_DIM - 1) < HEAD_DIM // 2
        cosine, sine = cos_ref[rows, :], sin_ref[rows, :]
        for at in range(0, width, 128):
            part = raw[:, 2 * channels + at : 2 * channels + at + 128]
            other = jnp.where(
                front,
                pltpu.roll(part, 128 - HEAD_DIM // 2, 1),
                pltpu.roll(part, HEAD_DIM // 2, 1),
            )
            turned = part * cosine + other * sine
            if at + 128 == width:
                turned = jnp.where(lane < HEAD_DIM, turned, part)
            qkv_ref[rows, at : at + 128] = turned.astype(jnp.bfloat16)

    row_tiles(own_ref, other_ref, body)
    end = glu_ref.shape[0]
    tail_ref[0:WINDOW, :] = qkv_ref[end - WINDOW : end, width - 128 : width]
    tail_ref[WINDOW : WINDOW + 32, :] = glu_ref[end - 32 : end, :128]
    tail_ref[WINDOW + 32 : WINDOW + 64, :] = glu_ref[end - 32 : end, 128:]


def join_kernel(column, *refs):
    pieces, out_ref = refs[:-1], refs[-1]
    for index, piece in enumerate(pieces):
        line, first = line_of(index)
        block = piece.shape[1]
        for step in range(piece.shape[0]):
            to = pl.multiple_of(line * (SIDE * block) + (first + step) * block, block)
            out_ref[pl.ds(to, block), :] = piece[step, :, column:]


def conv_kernel(before_ref, glu_ref, taps_ref, out_ref, sums_ref, ext_ref, pair_ref):
    count, (rows, channels) = taps_ref.shape[0], glu_ref.shape
    first_channel = lax.axis_index("core") * channels
    lead = 32
    for part in range(2):
        lanes = pl.ds(part * 128, 128)
        held = pl.ds(WINDOW + part * lead, lead)
        ext_ref[part, pl.ds(0, lead), :] = before_ref[held, :].astype(jnp.float32)
        ext_ref[part, pl.ds(lead, rows), :] = glu_ref[:, lanes].astype(jnp.float32)

    @pl.loop(0, rows // 128)
    def _(step):
        base = pl.multiple_of(step * 128, 128)
        for half in range(0, 128, 64):
            first = jnp.zeros((64, 128), jnp.float32)
            second = jnp.zeros((64, 128), jnp.float32)
            for part in range(2):
                own = pl.ds(pl.multiple_of(first_channel + part * 128, 128), 128)
                total = jnp.zeros((64, 128), jnp.float32)
                for tap in range(count):
                    rows_at = pl.ds(base + (half + lead - count + 1 + tap), 64)
                    total = total + taps_ref[pl.ds(tap, 1), own] * ext_ref[part, rows_at, :]
                out_ref[pl.ds(base + half, 64), pl.ds(part * 128, 128)] = total
                first = first + total
                second = second + total * total
            pair_ref[0, half : half + 64, :] = first
            pair_ref[1, half : half + 64, :] = second
        first = jnp.sum(pair_ref[0].T, axis=0, keepdims=True)
        second = jnp.sum(pair_ref[1].T, axis=0, keepdims=True)
        for member in range(sums_ref.shape[0]):
            sums_ref[member, pl.ds(0, 1), pl.ds(base, 128)] = first
            sums_ref[member, pl.ds(1, 1), pl.ds(base, 128)] = second


def scaled_kernel(conv_ref, sums_ref, gain_ref, attn_ref, kept_ref, given_ref):
    core = lax.axis_index("core")
    totals = sums_ref[0]
    for member in range(1, sums_ref.shape[0]):
        totals = totals + sums_ref[member]
    mean = totals[0:1] / CONV_CH
    scale = lax.rsqrt(totals[1:2] / CONV_CH - mean * mean + CHANNEL_EPS)
    half, channels = kept_ref.shape
    given_ref[:, channels:] = attn_ref[...]
    for base in range(0, conv_ref.shape[0], 128):
        at = slice(base, base + 128)
        mean_at = jnp.broadcast_to(mean[:, at], (128, 128)).T
        scale_at = jnp.broadcast_to(scale[:, at], (128, 128)).T
        parts = []
        for lane in range(0, channels, 128):
            own = pl.ds(pl.multiple_of(core * channels + lane, 128), 128)
            normed = (conv_ref[at, lane : lane + 128] - mean_at) * scale_at * gain_ref[0:1, own]
            parts.append((normed * jax.nn.sigmoid(normed)).astype(jnp.bfloat16))
        out = jnp.concatenate(parts, axis=1)
        to = slice(base % half, base % half + 128)

        @pl.when(core == base // half)
        def _():
            kept_ref[to, :] = out

        @pl.when(core != base // half)
        def _():
            given_ref[to, :channels] = out


def attention_kernel(sinks_ref, qkv_ref, before_ref, kept_ref, given_ref, logs_ref, keys, values):
    core, chip = lax.axis_index("core"), lax.axis_index("chip")
    cols = kept_ref.shape[1]
    for source, to, count in ((before_ref, 0, WINDOW), (qkv_ref, WINDOW, qkv_ref.shape[0])):
        both = source[:count, source.shape[1] - 128 :].astype(jnp.float32)
        low = lax.broadcasted_iota(jnp.int32, both.shape, 1) < HEAD_DIM
        turned = pltpu.roll(both, HEAD_DIM, 1)
        rows = slice(to, to + both.shape[0])
        keys[rows, :] = jnp.where(low, both, turned).astype(jnp.bfloat16)
        values[rows, :] = jnp.where(low, turned, both).astype(jnp.bfloat16)
    blocks = qkv_ref.shape[0] // WINDOW
    half_blocks = blocks // CORES
    heads = cols // HEAD_DIM

    @pl.loop(0, blocks, unroll=2)
    def _(block):
        base = pl.multiple_of(block * WINDOW, WINDOW)
        window = pl.ds(base, 2 * WINDOW)
        query_at = lax.broadcasted_iota(jnp.int32, (WINDOW, 2 * WINDOW), 0)
        key_at = lax.broadcasted_iota(jnp.int32, (WINDOW, 2 * WINDOW), 1)
        lane = lax.broadcasted_iota(jnp.int32, (WINDOW, 128), 1)
        low = lane < HEAD_DIM
        logs = jnp.zeros((WINDOW, 128), jnp.float32)
        lowest = jnp.where((chip == 0) & (block == 0), WINDOW, 0)
        allowed = (key_at > query_at) & (key_at <= query_at + WINDOW) & (key_at >= lowest)
        queries = []
        for head in range(heads):
            pair = head // 2 * 128
            query = qkv_ref[pl.ds(base, WINDOW), pair : pair + 128].astype(jnp.float32)
            query = jnp.where(low if head % 2 == 0 else jnp.logical_not(low), query, 0.0)
            queries.append((query * HEAD_DIM ** (-0.5)).astype(jnp.bfloat16))
        all_scores = lax.dot_general(
            jnp.concatenate(queries, axis=0),
            keys[window, :],
            (((1,), (1,)), ((), ())),
            preferred_element_type=jnp.float32,
        )
        weights = []
        for head in range(heads):
            scores = all_scores[head * WINDOW : (head + 1) * WINDOW]
            scores = jnp.where(allowed, scores, -jnp.inf)
            sums = jnp.sum(jnp.exp(scores), axis=1, keepdims=True)
            sink = jnp.full((WINDOW, 1), sinks_ref[core * heads + head], jnp.float32)
            log_total = jnp.log(sums + jnp.exp(sink))
            logs = jnp.where(lane == head, log_total, logs)
            weights.append(jnp.exp(scores - log_total).astype(jnp.bfloat16))
        attended = jnp.dot(
            jnp.concatenate(weights, axis=0), values[window, :], preferred_element_type=jnp.float32
        )
        parts = [attended[head * WINDOW : (head + 1) * WINDOW] for head in range(heads)]
        outs = [
            jnp.where(low, parts[head], parts[head + 1]).astype(jnp.bfloat16)
            for head in range(0, heads, 2)
        ]
        out = jnp.concatenate(outs, axis=1)
        logs_ref[:, pl.ds(base, WINDOW)] = logs.T[:heads]
        own = block // half_blocks == core
        to = pl.ds(pl.multiple_of((block % half_blocks) * WINDOW, WINDOW), WINDOW)

        @pl.when(own)
        def _():
            kept_ref[to, :] = out

        @pl.when(jnp.logical_not(own))
        def _():
            given_ref[to, :] = out


def output_kernel(steps, conv_ref, attn_ref, got_ref, own_ref, other_ref, *rest):
    out_refs, (x_ref, w_ref) = rest[:-2], rest[-2:]
    core, member = lax.axis_index("core"), lax.axis_index("tp")
    count = out_refs[0].shape[0]
    peers = conv_ref.shape[0] // count
    block = own_ref.shape[0] // CHIPS
    width = own_ref.shape[1]
    for index, away in enumerate(steps):
        to = jnp.bitwise_and(member + away, peers - 1)
        rows = pl.ds(pl.multiple_of(to * count, count), count)
        x_ref[index * count : (index + 1) * count, :] = jnp.concatenate(
            [conv_ref[rows, :], attn_ref[rows, :], got_ref[rows, :]], axis=1
        )

    @pl.loop(0, SIDE, unroll=4)
    def _(z):
        cols = pl.ds(pl.multiple_of(z * SIDE * block, TILE), SIDE * block)
        by_z, by_y = z * SIDE * block, z * block
        for source, at, along_z in ((own_ref, 0, core == 0), (other_ref, width, core == 1)):
            first = jnp.where(along_z, by_z, by_y)
            stride = jnp.where(along_z, block, SIDE * block)
            for y in range(SIDE):
                start = pl.multiple_of(first + y * stride, block)
                w_ref[y * block : (y + 1) * block, at : at + width] = source[pl.ds(start, block), :]
        total = lax.dot_general(
            x_ref[...], w_ref[...], (((1,), (1,)), ((), ())), preferred_element_type=jnp.float32
        )
        for index, out_ref in enumerate(out_refs):
            out_ref[:, cols] = total[index * count : (index + 1) * count].astype(jnp.bfloat16)


def layer(
    tokens,
    norm_gain,
    w_conv_value,
    w_conv_gate,
    w_query,
    w_key,
    w_value,
    conv_taps,
    ln_gain,
    sinks,
    out_conv,
    out_attn,
):
    core = lax.axis_index("core")
    chip = lax.axis_index("chip")
    own_rows, model = tokens.shape
    row_count = own_rows * CORES
    depth = w_conv_value.shape[0]
    channels = w_conv_value.shape[1] // CORES
    q_cols = w_query.shape[1] // CORES
    query_heads = q_cols // HEAD_DIM
    block = CORES * depth

    conv_cols = (0, 2 * channels)
    qkv_cols = (2 * channels, q_cols + 2 * HEAD_DIM)
    out_cols = (2 * channels + q_cols + 2 * HEAD_DIM, channels + q_cols)
    width = sum(out_cols)
    shards_in = (w_conv_value, w_conv_gate, w_query, w_key, w_value, out_conv.T, out_attn.T)
    kept, given = call(
        pack_kernel,
        (shape((depth, width)),) * 2,
        1 << 20,
        [HBM] * len(shards_in),
        shards_in,
        (
            *(pltpu.VMEM(w.shape, w.dtype) for w in shards_in),
            pltpu.SemaphoreType.DMA((len(shards_in),)),
        ),
    )
    got = lax.ppermute(given, SP, OTHER_CORE)
    sent = call(repeat_kernel, shape((SIDE, block, width)), 1 << 20, [VMEM, VMEM], (kept, got))
    own_line = lax.all_to_all(sent, SP, 0, 0, tiled=True, axis_index_groups=LINES)
    pieces = [own_line]
    ahead = behind = own_line
    for step in range(SIDE // 2):
        if step == SIDE // 2 - 1:
            ahead, behind = ahead[: SIDE // 2], behind[SIDE // 2 :]
        ahead = lax.ppermute(ahead, SP, AHEAD)
        behind = lax.ppermute(behind, SP, BEHIND)
        pieces += [ahead, behind]

    tokens_other = lax.ppermute(tokens, SP, OTHER_CORE)

    def rms_normed(rows):
        return call(
            norm_kernel, shape(rows.shape), 1 << 30, [VMEM, VMEM], (rows, norm_gain[None]), limit=12
        )

    normed = (rms_normed(tokens), rms_normed(tokens_other))

    positions = chip * row_count + jnp.arange(row_count, dtype=jnp.int32)
    half_dim = HEAD_DIM // 2
    inverse = ROPE_BASE ** (-jnp.arange(half_dim, dtype=jnp.float32) / half_dim)
    angles = positions.astype(jnp.float32)[:, None] * inverse[None, :]
    cosine, sine = jnp.cos(angles), jnp.sin(angles)
    cosines = jnp.concatenate([cosine] * 4, axis=1)
    sines = jnp.concatenate([-sine, sine] * 2, axis=1)

    in_cols = conv_cols[1] + qkv_cols[1]
    lines = SIDE * block

    def early(first, last, before):
        held = pieces[first:last]
        return call(
            functools.partial(early_kernel, first, len(held)),
            shape((row_count, in_cols), jnp.float32),
            2 * row_count * lines * len(held) * in_cols,
            [VMEM] * (2 + len(held) + len(before)),
            (*normed, *held, *before),
            (pltpu.VMEM((lines * len(held), in_cols), jnp.bfloat16),),
            limit=16,
        )

    total = early(0, 5, ())
    total = early(5, 7, (total,))
    glu, qkv, tail = call(
        functools.partial(late_kernel, 7),
        (shape((row_count, channels)), shape((row_count, qkv_cols[1])), shape((WINDOW + 64, 128))),
        2 * row_count * lines * in_cols,
        [VMEM] * 7,
        (*normed, cosines, sines, total, *pieces[7:]),
        (pltpu.VMEM((lines, in_cols), jnp.bfloat16),),
        limit=16,
    )
    before = lax.ppermute(tail, SP, NEXT_CHIP)
    out_own = call(
        functools.partial(join_kernel, out_cols[0]),
        shape((model, out_cols[1])),
        1 << 28,
        [VMEM] * len(pieces),
        pieces,
        limit=12,
    )
    out_other = lax.ppermute(out_own, SP, OTHER_CORE)

    members = CORES * lax.axis_size("tp")
    conv_out, sums = call(
        conv_kernel,
        (shape((row_count, channels), jnp.float32), shape((members, 2, row_count), jnp.float32)),
        1 << 32,
        [VMEM] * 3,
        (before, glu, conv_taps),
        (pltpu.VMEM((2, row_count + 32, 128), jnp.float32), pltpu.VMEM((2, 128, 128), jnp.float32)),
        limit=12,
    )
    everyones = lax.all_to_all(sums, CHIP, 0, 0, tiled=True)
    extended = pltpu.VMEM((row_count + WINDOW, 128), jnp.bfloat16)
    attn_kept, attn_given, log_rows = call(
        attention_kernel,
        (
            shape((own_rows, q_cols)),
            shape((own_rows, q_cols)),
            shape((query_heads, row_count), jnp.float32),
        ),
        1 << 32,
        [SMEM, VMEM, VMEM],
        (sinks, qkv, before),
        (extended,) * 2,
    )
    conv_kept, given = call(
        scaled_kernel,
        (shape((own_rows, channels)), shape((own_rows, channels + q_cols))),
        1 << 28,
        [VMEM] * 4,
        (conv_out, everyones, ln_gain[None], attn_given),
        limit=12,
    )
    rows_got = lax.ppermute(given, SP, OTHER_CORE)

    kept = lax.dynamic_slice_in_dim(log_rows, core * own_rows, own_rows, 1)
    given = lax.dynamic_slice_in_dim(log_rows, (1 - core) * own_rows, own_rows, 1)
    logs_got = lax.ppermute(given, SP, OTHER_CORE)
    log_sums = jnp.where(
        core == 0,
        jnp.concatenate([kept, logs_got], axis=0),
        jnp.concatenate([logs_got, kept], axis=0),
    )

    peers = lax.axis_size("tp")
    share = own_rows // peers

    def output(steps):
        return call(
            functools.partial(output_kernel, steps),
            (shape((share, model)),) * len(steps),
            2 * share * len(steps) * model * 2 * out_cols[1],
            [VMEM] * 5,
            (conv_kept, attn_kept, rows_got, out_own, out_other),
            (
                pltpu.VMEM((share * len(steps), 2 * out_cols[1]), jnp.bfloat16),
                pltpu.VMEM((TILE, 2 * out_cols[1]), jnp.bfloat16),
            ),
            limit=12,
        )

    def to_member(value, away):
        return lax.ppermute(value, "tp", [(i, (i + away) % peers) for i in range(peers)])

    far, up, down, mine = output((2, 1, 3, 0))
    far, up = to_member(far, 2), to_member(up, 1)
    down = to_member(down, 3)
    mixed = (
        mine.astype(jnp.float32)
        + far.astype(jnp.float32)
        + up.astype(jnp.float32)
        + down.astype(jnp.float32)
    )
    return (mixed.astype(jnp.bfloat16), log_sums)


def solution(mesh):
    split = Mesh(mesh.devices.reshape(-1, CORES, mesh.shape["tp"]), ("chip", "core", "tp"))
    in_specs = (
        P(SP, None),
        P(),
        P(SP, "tp"),
        P(SP, "tp"),
        P(SP, "tp"),
        P(SP, "tp"),
        P(SP, "tp"),
        P(None, "tp"),
        P("tp"),
        P("tp"),
        P("tp", SP),
        P("tp", SP),
    )
    out_specs = (P((*SP, "tp"), None), P("tp", SP))
    return jax.shard_map(layer, mesh=split, in_specs=in_specs, out_specs=out_specs, check_vma=False)
```
